32 devices in a mesh: grp: 2 (over y), sp: 4 (over z), tp: 4 (over x, core).
Axes of the slice: x: 2, y: 2, z: 4, core: 2. Of those that a mesh axis runs over, the one named last changes fastest.
Arguments:
- hidden_in: bfloat16 [2048, 2048], P(('grp', 'sp'), 'tp'), parts along dimension 0, may hold values from -40 to 40
- norm_gain: float32 [3, 2048], replicated, may hold values from 0.1 to 1.9
- query_weight: bfloat16 [3, 1024, 2048], P(None, 'tp'), may hold values from -6 to 6
- key_weight: bfloat16 [3, 1024, 2048], P(None, 'tp'), may hold values from -6 to 6
- value_weight: bfloat16 [3, 1024, 2048], P(None, 'tp'), may hold values from -0.125 to 0.125
- output_weight: bfloat16 [3, 1024, 2048], P(None, None, 'tp'), may hold values from -0.75 to 0.75
- offset_bias: float32 [3, 16, 15, 31], P(None, 'tp'), may hold values from -4 to 4
Outputs:
- hidden_out: bfloat16 [2048, 2048], P(('grp', 'sp'), 'tp'), parts along dimension 0
The draws below stay inside these ranges and needn't reach their ends.
There are 2 independent parts, one for each index of `grp`. The reference program is written for one: setup_inputs(seed, part) draws one part's arguments, and reference() takes and returns one part's arrays. A program takes and returns all parts, laid end to end along the dimension named above; an argument that names none is the same for every part. Nothing has to cross between parts.
All inputs are finite; a program needn't handle non-finite values.
Results may differ from the reference program's by a relative error of at most 0.028.
Values may be sent and summed in bfloat16 or wider, within the bound.
No kernel may reach another device: no remote copies, remote signals or barrier semaphores. Data moves between devices by JAX's collectives and lax.ppermute only.
A program may use at most 64 MiB of HBM per device.

```python
import jax
import jax.numpy as jnp
import numpy as np
from jax import lax

D = 2048
HEADS = 16
HEAD_DIM = 64
GRID_W = 64
ROW_SPAN = 8
COL_SPAN = 16
LAYERS = 3
TOKENS = 1024


def query_draw(key):
    drawn = jax.random.normal(jax.random.fold_in(key, 101), (LAYERS, HEADS * HEAD_DIM, D), jnp.float32)
    return drawn * D ** (-0.5)


def draw_hidden_in(key, part):
    subkeys = jax.random.split(jax.random.fold_in(key, 505), 3)
    normal_part = jax.random.normal(subkeys[0], (TOKENS, D), jnp.float32)
    col_pos = jnp.arange(D, dtype=jnp.float32) / D
    col_scale = jnp.exp(jnp.log(4.0) * col_pos + jax.random.uniform(subkeys[1], (D,), jnp.float32, -0.6, 0.6))
    row_scale = jnp.exp(jax.random.uniform(subkeys[2], (TOKENS, 1), jnp.float32, -1.0, 1.0))
    values = normal_part * col_scale[None, :] * row_scale * 0.6
    return jnp.clip(values, -40.0, 40.0).astype(jnp.bfloat16)


def draw_query_weight(key, part):
    return jnp.clip(query_draw(key), -6.0, 6.0).astype(jnp.bfloat16)


def draw_key_weight(key, part):
    values = jax.random.normal(jax.random.fold_in(key, 202), (LAYERS, HEADS * HEAD_DIM, D), jnp.float32) * D ** (-0.5)
    return jnp.clip(values, -6.0, 6.0).astype(jnp.bfloat16)


def block_levels(rng, shape, shards, low, top_value):
    level = 1.0
    for axis_at, parts in shards:
        heights = jax.random.uniform(jax.random.fold_in(jax.random.fold_in(rng, 6), axis_at), (parts,), jnp.float32, low / len(shards), top_value / len(shards))
        level = level * jnp.repeat(jnp.exp(heights), shape[axis_at] // parts).reshape((-1,) + (1,) * (len(shape) - 1 - axis_at))
    return level


def scatter_about(key, dims, scale, most, cuts=(), held_as=jnp.bfloat16):
    gain = block_levels(key, dims, cuts, -0.22, 0.18) if cuts else 1.0
    values = jax.random.normal(key, dims, jnp.float32) * scale * gain
    return jnp.minimum(jnp.maximum(values, -most), most).astype(held_as)


def setup_inputs(seed: int = 0, part: int = 0) -> dict:
    key_of = jax.random.split(jax.random.key(seed), 8)
    part_keys = jax.random.split(jax.random.fold_in(key_of[7], part), 8)
    return {
        "hidden_in": draw_hidden_in(jax.random.fold_in(jax.random.fold_in(key_of[7], part), 71), part),
        "norm_gain": jnp.clip(1.0 + 0.18 * jax.random.normal(key_of[1], (LAYERS, D), jnp.float32), 0.1, 1.9),
        "query_weight": draw_query_weight(jax.random.fold_in(key_of[7], 71), part),
        "key_weight": draw_key_weight(jax.random.fold_in(key_of[7], 71), part),
        "value_weight": scatter_about(key_of[4], (LAYERS, HEADS * HEAD_DIM, D), D ** -0.5, 0.125, ((1, 4),)),
        "output_weight": scatter_about(key_of[5], (LAYERS, HEADS * HEAD_DIM, D), (HEADS * HEAD_DIM // 16) ** -0.5, 0.75, ((2, 4),)),
        "offset_bias": scatter_about(key_of[6], (LAYERS, HEADS, 2 * ROW_SPAN - 1, 2 * COL_SPAN - 1), 1.0, 4.0, ((1, 4),), jnp.float32),
    }


EPS = 1e-06
NEG = -1e+30
QBLOCK = 16

def column_tables():
    nblocks = GRID_W // QBLOCK
    key_span = QBLOCK + COL_SPAN
    block_start = np.clip(np.arange(nblocks) * QBLOCK - COL_SPAN // 2, 0, GRID_W - key_span)
    key_cols = block_start[:, None] + np.arange(key_span)[None, :]
    query_cols = np.arange(nblocks)[:, None] * QBLOCK + np.arange(QBLOCK)[None, :]
    window_cols = np.clip(query_cols - COL_SPAN // 2, 0, GRID_W - COL_SPAN)
    inside = (key_cols[:, None, :] >= window_cols[:, :, None]) & (key_cols[:, None, :] < window_cols[:, :, None] + COL_SPAN)
    col_offset = np.clip(key_cols[:, None, :] - query_cols[:, :, None], 1 - COL_SPAN, COL_SPAN - 1) + COL_SPAN - 1
    return (block_start, inside, col_offset)

def block_firsts():
    nblocks = GRID_W // QBLOCK
    key_span = QBLOCK + COL_SPAN
    return [min(max(block * QBLOCK - COL_SPAN // 2, 0), GRID_W - key_span) for block in range(nblocks)]

def bias_rows(bias_table, row_offset):
    block_start, inside, col_offset = column_tables()
    nblocks = block_start.shape[0]
    key_span = QBLOCK + COL_SPAN
    rows_n = row_offset.shape[0]
    heads_n = bias_table.shape[0]
    by_row = bias_table[:, row_offset]
    chosen = by_row[:, :, :, jnp.asarray(col_offset, dtype=jnp.int32)]
    chosen = chosen.transpose(1, 0, 3, 4, 2, 5)
    return chosen.reshape(rows_n, heads_n, nblocks, QBLOCK, ROW_SPAN * key_span)

def attend_rows(queries, key_rows, value_rows, bias):
    block_start, inside, col_offset = column_tables()
    nblocks = block_start.shape[0]
    key_span = QBLOCK + COL_SPAN
    rows_n, heads_n, head_size = (queries.shape[0], queries.shape[2], queries.shape[3])

    def pick_blocks(tensor):
        pieces = [tensor[:, :, first_col:first_col + key_span] for first_col in block_firsts()]
        return jnp.stack(pieces, axis=1).reshape(rows_n, nblocks, ROW_SPAN * key_span, heads_n, head_size)
    key_blocks = pick_blocks(key_rows).astype(jnp.float32)
    value_blocks = pick_blocks(value_rows).astype(jnp.float32)
    query_blocks = queries.reshape(rows_n, nblocks, QBLOCK, heads_n, head_size).astype(jnp.float32)
    scores = jnp.einsum('rcqhd,rckhd->rhcqk', query_blocks, key_blocks) * head_size ** (-0.5) + bias
    allowed = np.broadcast_to(inside[:, :, None, :], (nblocks, QBLOCK, ROW_SPAN, key_span))
    allowed = allowed.reshape(nblocks, QBLOCK, ROW_SPAN * key_span)
    scores = jnp.where(jnp.asarray(allowed)[None, None], scores, NEG)
    row_peak = lax.optimization_barrier(jnp.max(scores, axis=-1, keepdims=True))
    lifted = jnp.exp(scores - row_peak)
    weights = (lifted / lax.optimization_barrier(jnp.sum(lifted, axis=-1, keepdims=True))).astype(jnp.bfloat16)
    attended = jnp.einsum('rhcqk,rckhd->rcqhd', weights.astype(jnp.float32), value_blocks)
    return attended.astype(jnp.bfloat16).reshape(rows_n, GRID_W, heads_n, head_size)

def reference(hidden_in, norm_gain, query_weight, key_weight, value_weight, output_weight, offset_bias):
    all_rows = hidden_in.shape[0] // GRID_W
    span_half = ROW_SPAN // 2
    channels = HEADS * HEAD_DIM
    stream = hidden_in
    for layer_idx in range(LAYERS):
        stream_wide = stream.astype(jnp.float32)
        row_scale = lax.rsqrt(lax.optimization_barrier(jnp.mean(stream_wide * stream_wide, axis=1, keepdims=True)) + EPS)
        normed = (stream_wide * row_scale * norm_gain[layer_idx][None, :]).astype(jnp.bfloat16)
        query_grid = jnp.dot(normed, query_weight[layer_idx].T, preferred_element_type=jnp.float32).astype(jnp.bfloat16)
        key_grid = jnp.dot(normed, key_weight[layer_idx].T, preferred_element_type=jnp.float32).astype(jnp.bfloat16)
        value_grid = jnp.dot(normed, value_weight[layer_idx].T, preferred_element_type=jnp.float32).astype(jnp.bfloat16)
        query_grid = query_grid.reshape(all_rows, GRID_W, HEADS, HEAD_DIM)
        key_grid = key_grid.reshape(all_rows, GRID_W, HEADS, HEAD_DIM)
        value_grid = value_grid.reshape(all_rows, GRID_W, HEADS, HEAD_DIM)
        bias_table = offset_bias[layer_idx]

        def one_row(row_idx):
            first_row = jnp.clip(row_idx - span_half, 0, all_rows - ROW_SPAN).astype(jnp.int32)
            key_rows = lax.dynamic_slice_in_dim(key_grid, first_row, ROW_SPAN, 0)[None]
            value_rows = lax.dynamic_slice_in_dim(value_grid, first_row, ROW_SPAN, 0)[None]
            query_row = lax.dynamic_slice_in_dim(query_grid, row_idx, 1, 0)
            row_offset = (first_row + jnp.arange(ROW_SPAN, dtype=jnp.int32) - row_idx + ROW_SPAN - 1).astype(jnp.int32)[None]
            bias = bias_rows(bias_table, row_offset)
            return attend_rows(query_row, key_rows, value_rows, bias)[0]
        attended = lax.map(one_row, jnp.arange(all_rows, dtype=jnp.int32)).reshape(all_rows * GRID_W, channels)
        projected = jnp.dot(attended, output_weight[layer_idx], preferred_element_type=jnp.float32)
        stream = (stream.astype(jnp.float32) + projected).astype(jnp.bfloat16)
    return stream
```

```python
from functools import partial

import jax
import jax.numpy as jnp
import numpy as np
from jax import lax
from jax.experimental import pallas as pl
from jax.experimental.pallas import tpu as pltpu
from jax.sharding import PartitionSpec as P

HEAD_DIM = 64
GRID_W = 64
ROW_SPAN = 8
COL_SPAN = 16
LAYERS = 3
HALF = ROW_SPAN // 2

EPS = 1e-06
NEG = -1e30
LANES = 128
F32 = jnp.float32
BF16 = jnp.bfloat16

VMEM = pl.BlockSpec(memory_space=pltpu.VMEM)
SMEM = pl.BlockSpec(memory_space=pltpu.SMEM)


def nt_dot(left, right):
    return lax.dot_general(left, right, (((1,), (1,)), ((), ())), preferred_element_type=F32)


def cost(flops, bytes_accessed, transcendentals=0):
    return pl.CostEstimate(
        flops=int(flops), bytes_accessed=int(bytes_accessed), transcendentals=int(transcendentals)
    )


def project_kernel(parts_n, first, last, full_width, where, *refs):
    sources = refs[:parts_n]
    refs = refs[parts_n:]
    gains, refs = refs[:parts_n], refs[parts_n:]
    weights, refs = refs[: 3 * parts_n], refs[3 * parts_n :]
    if not first:
        (acc_in, sq_in), refs = refs[:2], refs[2:]
    totals = [None, None, None]
    squares = None
    for at in range(parts_n):
        wide = sources[at][...].astype(F32)
        square = jnp.sum(wide * wide, axis=1, keepdims=True)
        squares = square if squares is None else squares + square
        scaled = (wide * gains[at][0]).astype(BF16)
        for kind in range(3):
            product = nt_dot(scaled, weights[3 * at + kind][0])
            totals[kind] = product if totals[kind] is None else totals[kind] + product
    if not first:
        squares = squares + sq_in[:, :1]
        totals = [totals[kind] + acc_in[kind] for kind in range(3)]
    if last:
        query_ref, pair_ref = refs
        row_scale = lax.rsqrt(squares * (1.0 / full_width) + EPS)
        query_ref[...] = (totals[0] * (row_scale * HEAD_DIM ** (-0.5))).astype(BF16)
        pair_ref[0] = (totals[1] * row_scale).astype(BF16)
        pair_ref[1] = (totals[2] * row_scale).astype(BF16)
    else:
        acc_out, sq_out = refs
        for kind in range(3):
            acc_out[kind] = totals[kind]
        sq_out[...] = jnp.broadcast_to(squares, sq_out.shape)


def project(parts, places, carried, last, layer, gain, weights):
    tok = parts[0].shape[0]
    width = parts[0].shape[1]
    channels = weights[0].shape[1]
    full = weights[0].shape[2]
    parts_n = len(parts)
    first = carried is None
    whole = lambda shape: pl.BlockSpec(shape, lambda i, s: (0,) * len(shape))
    in_specs = [whole(part.shape) for part in parts]
    in_specs += [
        pl.BlockSpec((1, 1, width), lambda i, s, at=at: (layer, 0, s[at])) for at in range(parts_n)
    ]
    operands = list(parts) + [gain] * parts_n
    for at in range(parts_n):
        for weight in weights:
            in_specs.append(
                pl.BlockSpec((1, channels, width), lambda i, s, at=at: (layer, 0, s[at]))
            )
            operands.append(weight)
    if not first:
        in_specs += [whole(part.shape) for part in carried]
        operands += list(carried)
    if last:
        out_shape = (
            jax.ShapeDtypeStruct((tok, channels), BF16),
            jax.ShapeDtypeStruct((2, tok, channels), BF16),
        )
    else:
        out_shape = (
            jax.ShapeDtypeStruct((3, tok, channels), F32),
            jax.ShapeDtypeStruct((tok, LANES), F32),
        )
    flops = 2 * tok * width * channels * 3 * parts_n
    return pl.pallas_call(
        partial(project_kernel, parts_n, first, last, full),
        out_shape=out_shape,
        grid_spec=pltpu.PrefetchScalarGridSpec(
            num_scalar_prefetch=1,
            grid=(1,),
            in_specs=in_specs,
            out_specs=[whole(shape.shape) for shape in out_shape],
        ),
        cost_estimate=cost(flops, parts_n * width * (channels * 6 + tok * 2) + 4 * tok * channels),
        name=f"project_{layer}_{parts_n}_{int(last)}",
    )(places, *operands)


def emit_kernel(parts_n, where, *refs):
    sources, refs = refs[:parts_n], refs[parts_n:]
    weights, refs = refs[:parts_n], refs[parts_n:]
    base_ref, out_ref = refs
    total = base_ref[...].astype(F32)
    for at in range(parts_n):
        total = total + jnp.dot(sources[at][...], weights[at][0], preferred_element_type=F32)
    out_ref[...] = total.astype(out_ref.dtype)


def emit(parts, places, base, out_type, layer, weight):
    tok, width = parts[0].shape
    cols = weight.shape[2]
    parts_n = len(parts)
    whole = lambda shape: pl.BlockSpec(shape, lambda i, s: (0,) * len(shape))
    in_specs = [whole(part.shape) for part in parts]
    in_specs += [
        pl.BlockSpec((1, width, cols), lambda i, s, at=at: (layer, s[at], 0)) for at in range(parts_n)
    ]
    in_specs.append(whole(base.shape))
    return pl.pallas_call(
        partial(emit_kernel, parts_n),
        out_shape=jax.ShapeDtypeStruct((tok, cols), out_type),
        grid_spec=pltpu.PrefetchScalarGridSpec(
            num_scalar_prefetch=1,
            grid=(1,),
            in_specs=in_specs,
            out_specs=whole((tok, cols)),
        ),
        cost_estimate=cost(
            2 * tok * width * cols * parts_n, parts_n * width * (cols + tok) * 2 + tok * cols * 6
        ),
        name=f"emit_{layer}_{parts_n}",
    )(places, *parts, *([weight] * parts_n), base)


def bias_kernel(rows_ref, out_ref):
    heads_n, spans = out_ref.shape[:2]
    shape = (GRID_W, LANES)
    query_col = lax.broadcasted_iota(jnp.int32, shape, 0)
    key_col = lax.broadcasted_iota(jnp.int32, shape, 1) % GRID_W
    first_col = jnp.clip(query_col - COL_SPAN // 2, 0, GRID_W - COL_SPAN)
    inside = (key_col >= first_col) & (key_col < first_col + COL_SPAN)
    for head in range(heads_n):
        for span in range(spans):
            row = jnp.broadcast_to(rows_ref[head, span : span + 1, :], shape)
            turned = pltpu.roll(row, LANES - (COL_SPAN - 1), axis=1, stride=1, stride_axis=0)
            out_ref[head, span] = jnp.where(inside, turned, NEG)


def expand_bias(table):
    heads_n, offsets, cols = table.shape
    padded = jnp.pad(table, ((0, 0), (0, 0), (0, GRID_W - cols)))
    rows = jnp.concatenate([padded[:, :-1], padded[:, 1:]], axis=2)
    spans = offsets - 1
    return pl.pallas_call(
        bias_kernel,
        out_shape=jax.ShapeDtypeStruct((heads_n, spans, GRID_W, LANES), F32),
        in_specs=[VMEM],
        out_specs=VMEM,
        cost_estimate=cost(heads_n * spans * GRID_W * LANES * 40, heads_n * spans * GRID_W * LANES * 4),
        name="expand_bias",
    )(rows)


def attend_kernel(
    rows_dev, where_ref, query_ref, own_ref, even_ref, odd_ref, bias_ref, out_ref, keys, values
):
    channels = query_ref.shape[1]
    group = min(LANES, channels)
    heads_in = group // HEAD_DIM
    span = ROW_SPAN * GRID_W
    low_slot, high_slot = 0, HALF + rows_dev
    even_slot = pl.multiple_of(where_ref[0] * GRID_W, GRID_W)
    odd_slot = pl.multiple_of(where_ref[1] * GRID_W, GRID_W)
    halo = HALF * GRID_W
    for scratch, kind in ((keys, 0), (values, 1)):
        scratch[HALF * GRID_W : (HALF + rows_dev) * GRID_W, :] = own_ref[kind]
        scratch[pl.ds(even_slot, halo), :] = even_ref[kind]
        scratch[pl.ds(odd_slot, halo), :] = odd_ref[kind]
    lane = lax.broadcasted_iota(jnp.int32, (GRID_W, group), 1)
    ones = jnp.ones((span, group), BF16)
    for row in range(rows_dev):
        first = pl.multiple_of(where_ref[2 + row] * GRID_W, GRID_W)
        offset = where_ref[2 + rows_dev + row]
        for pair in range(channels // group):
            cols = slice(pair * group, (pair + 1) * group)
            query = query_ref[row * GRID_W : (row + 1) * GRID_W, cols]
            if heads_in > 1:
                zero = jnp.zeros_like(query)
                query = jnp.concatenate(
                    [
                        jnp.where(lane // HEAD_DIM == head, query, zero)
                        for head in range(heads_in)
                    ],
                    axis=0,
                )
            scores = nt_dot(query, keys[pl.ds(first, span), cols])
            pieces = []
            for at in range(span // LANES):
                bias = jnp.concatenate(
                    [
                        bias_ref[pair * heads_in + head, offset + (LANES // GRID_W) * at]
                        for head in range(heads_in)
                    ],
                    axis=0,
                )
                pieces.append(scores[:, at * LANES : (at + 1) * LANES] + bias)
            peak = pieces[0]
            for piece in pieces[1:]:
                peak = jnp.maximum(peak, piece)
            peak = jnp.max(peak, axis=1, keepdims=True)
            lifted = jnp.concatenate([jnp.exp(piece - peak).astype(BF16) for piece in pieces], axis=1)
            mixed = jnp.dot(lifted, values[pl.ds(first, span), cols], preferred_element_type=F32)
            weight = jnp.dot(lifted, ones, preferred_element_type=F32)
            mixed = mixed / weight
            result = mixed[:GRID_W]
            for head in range(1, heads_in):
                result = jnp.where(
                    lane // HEAD_DIM == head, mixed[head * GRID_W : (head + 1) * GRID_W], result
                )
            out_ref[row * GRID_W : (row + 1) * GRID_W, cols] = result.astype(BF16)


def attend(where, query, own, even, odd, bias, rows_dev):
    tok, channels = query.shape
    padded = (rows_dev + 2 * HALF) * GRID_W
    scores = tok * (channels // HEAD_DIM) * ROW_SPAN * GRID_W
    return pl.pallas_call(
        partial(attend_kernel, rows_dev),
        out_shape=jax.ShapeDtypeStruct((tok, channels), BF16),
        in_specs=[SMEM] + [VMEM] * 5,
        out_specs=VMEM,
        scratch_shapes=[pltpu.VMEM((padded, channels), BF16)] * 2,
        cost_estimate=cost(scores * HEAD_DIM * 6, bias.size * 4 + tok * channels * 16, scores),
        name="attend",
    )(where, query, own, even, odd, bias)


def exchange(block, axis, pairs):
    return lax.ppermute(block, axis, [pair for one, two in pairs for pair in ((one, two), (two, one))])


def flip(block, axis, bit):
    count = lax.axis_size(axis)
    return lax.ppermute(block, axis, [(at, at ^ bit) for at in range(count)])


def body(hidden_in, norm_gain, query_weight, key_weight, value_weight, output_weight, offset_bias):
    tok_dev, width_local = hidden_in.shape
    rows_dev = tok_dev // GRID_W
    tp = lax.axis_size("tp")
    sp = lax.axis_size("sp")
    me = lax.axis_index("tp")
    mine = lax.axis_index("sp")
    all_rows = rows_dev * sp
    first_row = mine * rows_dev
    query_rows = first_row + jnp.arange(rows_dev, dtype=jnp.int32)
    window_first = jnp.clip(query_rows - HALF, 0, all_rows - ROW_SPAN)
    local_first = window_first - first_row + HALF
    offsets = window_first - query_rows + ROW_SPAN - 1
    is_odd = mine % 2
    high = HALF + rows_dev
    slots = jnp.stack([high * (1 - is_odd), high * is_odd])
    where = jnp.concatenate([slots, local_first, offsets]).astype(jnp.int32)
    gain = norm_gain[:, None, :]
    weights = (query_weight, key_weight, value_weight)
    near = jnp.stack([me, me ^ 1]).astype(jnp.int32)
    far = jnp.stack([me ^ 2]).astype(jnp.int32)
    last = jnp.stack([me ^ 3]).astype(jnp.int32)
    zero = jnp.zeros((1,), jnp.int32)
    even_pairs = [(at, at + 1) for at in range(0, sp - 1, 2)]
    odd_pairs = [(at, at + 1) for at in range(1, sp - 1, 2)]
    stream = hidden_in
    biases = [expand_bias(offset_bias[layer]) for layer in range(LAYERS)]
    for layer in range(LAYERS):
        step = partial(project, layer=layer, gain=gain, weights=weights)
        if tp == 4:
            across = flip(stream, "tp", 2)
            beside = flip(stream, "tp", 1)
            corner = flip(across, "tp", 1)
            carried = step([stream, beside], near, None, False)
            carried = step([across], far, carried, False)
            query, pair = step([corner], last, carried, True)
        else:
            gathered = lax.all_gather(stream, "tp", axis=1, tiled=True)
            query, pair = step([gathered], zero, None, True)
        if rows_dev == HALF:
            to_even = to_odd = pair
        else:
            low, top = pair[:, : HALF * GRID_W], pair[:, (rows_dev - HALF) * GRID_W :]
            to_even = jnp.where(is_odd == 0, top, low)
            to_odd = jnp.where(is_odd == 0, low, top)
        even = exchange(to_even, "sp", even_pairs)
        odd = exchange(to_odd, "sp", odd_pairs)
        attended = attend(where, query, pair, even, odd, biases[layer], rows_dev)
        if tp == 4:
            across = flip(attended, "tp", 2)
            beside = flip(attended, "tp", 1)
            corner = flip(across, "tp", 1)
            partly = emit([attended, beside], near, stream, F32, layer, output_weight)
            partly = emit([across], far, partly, F32, layer, output_weight)
            stream = emit([corner], last, partly, BF16, layer, output_weight)
        else:
            gathered = lax.all_gather(attended, "tp", axis=1, tiled=True)
            stream = emit([gathered], zero, stream, BF16, layer, output_weight)
    return stream


def solution(mesh):
    return jax.shard_map(
        body,
        mesh=mesh,
        in_specs=(
            P(("grp", "sp"), "tp"),
            P(),
            P(None, "tp", None),
            P(None, "tp", None),
            P(None, "tp", None),
            P(None, None, "tp"),
            P(None, "tp", None, None),
        ),
        out_specs=P(("grp", "sp"), "tp"),
        check_vma=False,
    )
```

```python
from functools import partial

import jax
import jax.numpy as jnp
from jax import lax
from jax.experimental import pallas as pl
from jax.experimental.pallas import tpu as pltpu
from jax.sharding import PartitionSpec as P


HEAD_DIM = 64
GRID_W = 64
ROW_SPAN = 8
COL_SPAN = 16
LAYERS = 3
HALF = ROW_SPAN // 2

EPS = 1e-06
NEG = -1e30
LANES = 128
F32 = jnp.float32
BF16 = jnp.bfloat16

PARAMS = pltpu.CompilerParams(vmem_limit_bytes=8 * 2**20)
VMEM = pl.BlockSpec(memory_space=pltpu.VMEM)
HBM = pl.BlockSpec(memory_space=pltpu.HBM)
SMEM = pl.BlockSpec(memory_space=pltpu.SMEM)


def nt_dot(left, right):
    return lax.dot_general(left, right, (((1,), (1,)), ((), ())), preferred_element_type=F32)


def cost(flops, bytes_accessed, transcendentals=0):
    return pl.CostEstimate(
        flops=int(flops), bytes_accessed=int(bytes_accessed), transcendentals=int(transcendentals)
    )


def project_kernel(parts_n, first, last, layer, where_ref, *refs):
    sources, refs = refs[:parts_n], refs[parts_n:]
    gain_ref, refs = refs[0], refs[1:]
    if first:
        stored, refs = refs[:3], refs[3:]
        *refs, held_ref, sems = refs
        copies = [
            pltpu.make_async_copy(stored[kind].at[layer], held_ref.at[kind], sems.at[kind])
            for kind in range(3)
        ]
        for copy in copies:
            copy.start()
    else:
        (held_ref, acc_in, sq_in), refs = refs[:3], refs[3:]
    full = gain_ref.shape[2]
    totals = [None, None, None]
    squares = None
    for at in range(parts_n):
        wide = sources[at][...].astype(F32)
        width = wide.shape[1]
        cols = pl.ds(pl.multiple_of(where_ref[at] * width, LANES), width)
        square = jnp.sum(wide * wide, axis=1, keepdims=True)
        squares = square if squares is None else squares + square
        scaled = (wide * gain_ref[layer, :, cols]).astype(BF16)
        for kind in range(3):
            if first and at == 0:
                copies[kind].wait()
            product = nt_dot(scaled, held_ref[kind, :, cols])
            totals[kind] = product if totals[kind] is None else totals[kind] + product
    if not first:
        squares = squares + sq_in[:, :1]
        totals = [totals[kind] + acc_in[kind] for kind in range(3)]
    if last:
        query_ref, pair_ref = refs
        row_scale = lax.rsqrt(squares * (1.0 / full) + EPS)
        query_ref[...] = (totals[0] * (row_scale * HEAD_DIM ** (-0.5))).astype(BF16)
        pair_ref[0] = (totals[1] * row_scale).astype(BF16)
        pair_ref[1] = (totals[2] * row_scale).astype(BF16)
    else:
        acc_out, sq_out = refs
        for kind in range(3):
            acc_out[kind] = totals[kind]
        sq_out[...] = jnp.broadcast_to(squares, sq_out.shape)


def project(parts, places, weights, carried, last, layer, gain):
    tok, width = parts[0].shape
    parts_n = len(parts)
    first = carried is None
    operands = [places, *parts, gain]
    specs = [SMEM] + [VMEM] * (parts_n + 1)
    if first:
        _, channels, full = weights[0].shape
        operands += weights
        specs += [HBM] * 3
    else:
        _, channels, full = weights.shape
        operands += [weights, *carried]
        specs += [VMEM] * 3
    if last:
        out_shape = [pltpu.VMEM((tok, channels), BF16), pltpu.VMEM((2, tok, channels), BF16)]
    else:
        out_shape = [pltpu.VMEM((3, tok, channels), F32), pltpu.VMEM((tok, LANES), F32)]
    scratch = []
    if first:
        out_shape.append(pltpu.VMEM((3, channels, full), BF16))
        scratch.append(pltpu.SemaphoreType.DMA((3,)))
    flops = 2 * tok * width * channels * 3 * parts_n
    return pl.pallas_call(
        partial(project_kernel, parts_n, first, last, layer),
        out_shape=out_shape,
        in_specs=specs,
        out_specs=[VMEM] * len(out_shape),
        scratch_shapes=scratch,
        cost_estimate=cost(flops, parts_n * width * (channels * 6 + tok * 2) + 4 * tok * channels),
        compiler_params=PARAMS,
    )(*operands)


def emit_kernel(parts_n, first, layer, where_ref, *refs):
    sources, refs = refs[:parts_n], refs[parts_n:]
    if first:
        stored_ref, base_ref, out_ref, held_ref, sem = refs
        copy = pltpu.make_async_copy(stored_ref.at[layer], held_ref, sem)
        copy.start()
    else:
        held_ref, base_ref, out_ref = refs
    total = base_ref[...].astype(F32)
    if first:
        copy.wait()
    for at in range(parts_n):
        width = sources[at].shape[1]
        rows = pl.ds(pl.multiple_of(where_ref[at] * width, HEAD_DIM), width)
        total = total + jnp.dot(sources[at][...], held_ref[rows, :], preferred_element_type=F32)
    out_ref[...] = total.astype(out_ref.dtype)


def emit(parts, places, weight, base, out_type, first, layer):
    tok, width = parts[0].shape
    cols = base.shape[1]
    parts_n = len(parts)
    out_shape = [pltpu.VMEM((tok, cols), out_type)]
    if out_type == BF16 and layer == LAYERS - 1:
        out_shape = [jax.ShapeDtypeStruct((tok, cols), out_type)]
    scratch = []
    if first:
        out_shape.append(pltpu.VMEM(weight.shape[1:], BF16))
        scratch.append(pltpu.SemaphoreType.DMA)
    return pl.pallas_call(
        partial(emit_kernel, parts_n, first, layer),
        out_shape=out_shape,
        in_specs=[SMEM] + [VMEM] * parts_n + [HBM if first else VMEM, VMEM],
        out_specs=[VMEM] * len(out_shape),
        scratch_shapes=scratch,
        cost_estimate=cost(
            2 * tok * width * cols * parts_n, parts_n * width * (cols + tok) * 2 + tok * cols * 6
        ),
        compiler_params=PARAMS,
    )(places, *parts, weight, base)


def bias_kernel(rows_ref, out_ref):
    heads_n, spans = out_ref.shape[:2]
    shape = (GRID_W, LANES)
    query_col = lax.broadcasted_iota(jnp.int32, shape, 0)
    key_col = lax.broadcasted_iota(jnp.int32, shape, 1) % GRID_W
    first_col = jnp.clip(query_col - COL_SPAN // 2, 0, GRID_W - COL_SPAN)
    inside = (key_col >= first_col) & (key_col < first_col + COL_SPAN)
    for head in range(heads_n):
        for span in range(spans):
            row = jnp.broadcast_to(rows_ref[head, span : span + 1, :], shape)
            turned = pltpu.roll(row, LANES - (COL_SPAN - 1), axis=1, stride=1, stride_axis=0)
            out_ref[head, span] = jnp.where(inside, turned, NEG)


def expand_bias(table):
    heads_n, offsets, cols = table.shape
    padded = jnp.pad(table, ((0, 0), (0, 0), (0, GRID_W - cols)))
    rows = jnp.concatenate([padded[:, :-1], padded[:, 1:]], axis=2)
    spans = offsets - 1
    return pl.pallas_call(
        bias_kernel,
        out_shape=pltpu.VMEM((heads_n, spans, GRID_W, LANES), F32),
        in_specs=[VMEM],
        out_specs=VMEM,
        cost_estimate=cost(heads_n * spans * GRID_W * LANES * 40, heads_n * spans * GRID_W * LANES * 4),
        compiler_params=PARAMS,
        name="expand_bias",
    )(rows)


def attend_kernel(
    rows_dev, where_ref, query_ref, own_ref, even_ref, odd_ref, bias_ref, out_ref, keys, values
):
    channels = query_ref.shape[1]
    group = min(LANES, channels)
    heads_in = group // HEAD_DIM
    span = ROW_SPAN * GRID_W
    even_slot = pl.multiple_of(where_ref[0] * GRID_W, GRID_W)
    odd_slot = pl.multiple_of(where_ref[1] * GRID_W, GRID_W)
    halo = HALF * GRID_W
    for scratch, kind in ((keys, 0), (values, 1)):
        scratch[HALF * GRID_W : (HALF + rows_dev) * GRID_W, :] = own_ref[kind]
        scratch[pl.ds(even_slot, halo), :] = even_ref[kind]
        scratch[pl.ds(odd_slot, halo), :] = odd_ref[kind]
    lane = lax.broadcasted_iota(jnp.int32, (GRID_W, group), 1)
    ones = jnp.ones((span, group), BF16)
    for row in range(rows_dev):
        first = pl.multiple_of(where_ref[2 + row] * GRID_W, GRID_W)
        offset = where_ref[2 + rows_dev + row]
        for pair in range(channels // group):
            cols = slice(pair * group, (pair + 1) * group)
            query = query_ref[row * GRID_W : (row + 1) * GRID_W, cols]
            if heads_in > 1:
                zero = jnp.zeros_like(query)
                query = jnp.concatenate(
                    [
                        jnp.where(lane // HEAD_DIM == head, query, zero)
                        for head in range(heads_in)
                    ],
                    axis=0,
                )
            scores = nt_dot(query, keys[pl.ds(first, span), cols])
            pieces = []
            for at in range(span // LANES):
                bias = jnp.concatenate(
                    [
                        bias_ref[pair * heads_in + head, offset + (LANES // GRID_W) * at]
                        for head in range(heads_in)
                    ],
                    axis=0,
                )
                pieces.append(scores[:, at * LANES : (at + 1) * LANES] + bias)
            peak = pieces[0]
            for piece in pieces[1:]:
                peak = jnp.maximum(peak, piece)
            peak = jnp.max(peak, axis=1, keepdims=True)
            lifted = jnp.concatenate([jnp.exp(piece - peak).astype(BF16) for piece in pieces], axis=1)
            mixed = jnp.dot(lifted, values[pl.ds(first, span), cols], preferred_element_type=F32)
            weight = jnp.dot(lifted, ones, preferred_element_type=F32)
            mixed = mixed / weight
            result = mixed[:GRID_W]
            for head in range(1, heads_in):
                result = jnp.where(
                    lane // HEAD_DIM == head, mixed[head * GRID_W : (head + 1) * GRID_W], result
                )
            out_ref[row * GRID_W : (row + 1) * GRID_W, cols] = result.astype(BF16)


def attend(where, query, own, even, odd, bias, rows_dev):
    tok, channels = query.shape
    padded = (rows_dev + 2 * HALF) * GRID_W
    scores = tok * (channels // HEAD_DIM) * ROW_SPAN * GRID_W
    return pl.pallas_call(
        partial(attend_kernel, rows_dev),
        out_shape=pltpu.VMEM((tok, channels), BF16),
        in_specs=[SMEM] + [VMEM] * 5,
        out_specs=VMEM,
        scratch_shapes=[pltpu.VMEM((padded, channels), BF16)] * 2,
        cost_estimate=cost(scores * HEAD_DIM * 6, bias.size * 4 + tok * channels * 16, scores),
        compiler_params=PARAMS,
        name="attend",
    )(where, query, own, even, odd, bias)


def exchange(block, pairs):
    sp, tp = lax.axis_size("sp"), lax.axis_size("tp")
    partner = {}
    for one, two in pairs:
        partner[one], partner[two] = two, one
    moves = []
    for row in range(sp):
        for col in range(tp):
            if row in partner:
                moves.append((row * tp + col, partner[row] * tp + col))
            elif tp % 2 == 0:
                moves.append((row * tp + col, row * tp + (col ^ 1)))
    return lax.ppermute(block, ("sp", "tp"), moves)


def flip(block, axis, bit):
    count = lax.axis_size(axis)
    return lax.ppermute(block, axis, [(at, at ^ bit) for at in range(count)])


def body(hidden_in, norm_gain, query_weight, key_weight, value_weight, output_weight, offset_bias):
    tok_dev, _ = hidden_in.shape
    rows_dev = tok_dev // GRID_W
    tp = lax.axis_size("tp")
    sp = lax.axis_size("sp")
    me = lax.axis_index("tp")
    mine = lax.axis_index("sp")
    all_rows = rows_dev * sp
    first_row = mine * rows_dev
    query_rows = first_row + jnp.arange(rows_dev, dtype=jnp.int32)
    window_first = jnp.clip(query_rows - HALF, 0, all_rows - ROW_SPAN)
    local_first = window_first - first_row + HALF
    offsets = window_first - query_rows + ROW_SPAN - 1
    is_odd = mine % 2
    high = HALF + rows_dev
    slots = jnp.stack([high * (1 - is_odd), high * is_odd])
    where = jnp.concatenate([slots, local_first, offsets]).astype(jnp.int32)
    gain = norm_gain[:, None, :]
    in_hbm = partial(pltpu.with_memory_space_constraint, memory_space=pltpu.HBM)
    weights = [in_hbm(weight) for weight in (query_weight, key_weight, value_weight)]
    output_weight = in_hbm(output_weight)
    near = jnp.stack([me]).astype(jnp.int32)
    far = jnp.stack([me ^ 1, me ^ 2]).astype(jnp.int32)
    last = jnp.stack([me ^ 3]).astype(jnp.int32)
    zero = jnp.zeros((1,), jnp.int32)
    even_pairs = [(at, at + 1) for at in range(0, sp - 1, 2)]
    odd_pairs = [(at, at + 1) for at in range(1, sp - 1, 2)]
    stream = hidden_in
    for layer in range(LAYERS):
        step = partial(project, layer=layer, gain=gain)
        if tp == 4:
            across = flip(stream, "tp", 2)
            beside = flip(stream, "tp", 1)
            corner = flip(across, "tp", 1)
            *carried, held = step([stream], near, weights, None, False)
            carried = step([beside, across], far, held, carried, False)
            query, pair = step([corner], last, held, carried, True)
        else:
            gathered = lax.all_gather(stream, "tp", axis=1, tiled=True)
            query, pair, _ = step([gathered], zero, weights, None, True)
        if rows_dev == HALF:
            to_even = to_odd = pair
        else:
            low, top = pair[:, : HALF * GRID_W], pair[:, (rows_dev - HALF) * GRID_W :]
            to_even = jnp.where(is_odd == 0, top, low)
            to_odd = jnp.where(is_odd == 0, low, top)
        even = exchange(to_even, even_pairs)
        odd = exchange(to_odd, odd_pairs)
        bias = expand_bias(offset_bias[layer])
        attended = attend(where, query, pair, even, odd, bias, rows_dev)
        step = partial(emit, layer=layer)
        if tp == 4:
            across = flip(attended, "tp", 2)
            beside = flip(attended, "tp", 1)
            corner = flip(across, "tp", 1)
            partly, held = step([attended], near, output_weight, stream, F32, True)
            (partly,) = step([beside, across], far, held, partly, F32, False)
            (stream,) = step([corner], last, held, partly, BF16, False)
        else:
            gathered = lax.all_gather(attended, "tp", axis=1, tiled=True)
            stream, _ = step([gathered], zero, output_weight, stream, BF16, True)
    return stream


def solution(mesh):
    return jax.shard_map(
        body,
        mesh=mesh,
        in_specs=(
            P(("grp", "sp"), "tp"),
            P(),
            P(None, "tp", None),
            P(None, "tp", None),
            P(None, "tp", None),
            P(None, None, "tp"),
            P(None, "tp", None, None),
        ),
        out_specs=P(("grp", "sp"), "tp"),
        check_vma=False,
    )
```

```python
from functools import partial

import jax
import jax.numpy as jnp
from jax import lax
from jax.experimental import pallas as pl
from jax.experimental.pallas import tpu as pltpu
from jax.sharding import PartitionSpec as P


HEAD_DIM = 64
GRID_W = 64
ROW_SPAN = 8
COL_SPAN = 16
LAYERS = 3
HALF = ROW_SPAN // 2

EPS = 1e-06
NEG = -1e30
LANES = 128
F32 = jnp.float32
BF16 = jnp.bfloat16

PARAMS = pltpu.CompilerParams(vmem_limit_bytes=8 * 2**20)
VMEM = pl.BlockSpec(memory_space=pltpu.VMEM)
HBM = pl.BlockSpec(memory_space=pltpu.HBM)


def nt_dot(left, right):
    return lax.dot_general(left, right, (((1,), (1,)), ((), ())), preferred_element_type=F32)


def in_vmem(array):
    return pltpu.with_memory_space_constraint(array, memory_space=pltpu.VMEM)


def in_hbm(array):
    return pltpu.with_memory_space_constraint(array, memory_space=pltpu.HBM)


def cost(flops, bytes_accessed, transcendentals=0):
    return pl.CostEstimate(
        flops=int(flops), bytes_accessed=int(bytes_accessed), transcendentals=int(transcendentals)
    )


def block_at(bit, width, unit):
    if bit is None:
        return slice(None)
    return pl.ds(pl.multiple_of((lax.axis_index("tp") ^ bit) * width, unit), width)


def window_at(row, rows_dev, sp):
    first_row = lax.axis_index("sp") * rows_dev
    first = jnp.minimum(jnp.maximum(first_row + row - HALF, 0), rows_dev * sp - ROW_SPAN)
    return first - first_row + HALF


def halo_slots(high):
    odd = lax.axis_index("sp") % 2
    return (
        pl.multiple_of((1 - odd) * (high * GRID_W), GRID_W),
        pl.multiple_of(odd * (high * GRID_W), GRID_W),
    )


def project_kernel(bits, first, kinds, layer, *refs):
    sources, refs = refs[: len(bits)], refs[len(bits) :]
    gain_ref, refs = refs[0], refs[1:]
    if first:
        stored, refs = refs[:3], refs[3:]
        *refs, held_ref, sems = refs
        copies = [
            pltpu.make_async_copy(stored[kind].at[layer], held_ref.at[kind], sems.at[kind])
            for kind in range(3)
        ]
        for copy in copies:
            copy.start()
    else:
        (held_ref, acc_in, sq_in), refs = refs[:3], refs[3:]
    full = gain_ref.shape[1]
    totals = [None, None, None]
    squares = None
    for at, bit in enumerate(bits):
        wide = sources[at][...].astype(F32)
        width = wide.shape[1]
        cols = block_at(bit, width, LANES)
        square = jnp.sum(wide * wide, axis=1, keepdims=True)
        squares = square if squares is None else squares + square
        scaled = (wide * gain_ref[layer : layer + 1, cols]).astype(BF16)
        for kind in kinds or range(3):
            if first and at == 0:
                copies[kind].wait()
            product = nt_dot(scaled, held_ref[kind, :, cols])
            totals[kind] = product if totals[kind] is None else totals[kind] + product
    if not first:
        squares = squares + sq_in[:, :1]
        for kind in kinds or range(3):
            totals[kind] = totals[kind] + acc_in[kind]
    if kinds:
        row_scale = lax.rsqrt(squares * (1.0 / full) + EPS)
        for at, kind in enumerate(kinds):
            scale = row_scale * HEAD_DIM ** (-0.5) if kind == 0 else row_scale
            refs[0][at] = (totals[kind] * scale).astype(BF16)
    else:
        acc_out, sq_out = refs
        for kind in range(3):
            acc_out[kind] = totals[kind]
        sq_out[...] = jnp.broadcast_to(squares, sq_out.shape)


def project(parts, bits, weights, carried, kinds, layer, gain):
    tok, width = parts[0].shape
    parts_n = len(parts)
    first = carried is None
    operands = [*parts, gain]
    specs = [VMEM] * (parts_n + 1)
    if first:
        _, channels, full = weights[0].shape
        operands += weights
        specs += [HBM] * 3
    else:
        _, channels, full = weights.shape
        operands += [in_vmem(weights), *map(in_vmem, carried)]
        specs += [VMEM] * 3
    if kinds:
        out_shape = [pltpu.VMEM((len(kinds), tok, channels), BF16)]
    else:
        out_shape = [pltpu.VMEM((3, tok, channels), F32), pltpu.VMEM((tok, LANES), F32)]
    scratch = []
    if first:
        out_shape.append(pltpu.VMEM((3, channels, full), BF16))
        scratch.append(pltpu.SemaphoreType.DMA((3,)))
    flops = 2 * tok * width * channels * len(kinds or range(3)) * parts_n
    return pl.pallas_call(
        partial(project_kernel, bits, first, kinds, layer),
        out_shape=out_shape,
        in_specs=specs,
        out_specs=[VMEM] * len(out_shape),
        scratch_shapes=scratch,
        cost_estimate=cost(flops, parts_n * width * (channels * 6 + tok * 2) + 4 * tok * channels),
        compiler_params=PARAMS,
    )(*operands)


def emit_kernel(bits, first, layer, *refs):
    sources, refs = refs[: len(bits)], refs[len(bits) :]
    if first:
        stored_ref, base_ref, out_ref, held_ref, sem = refs
        copy = pltpu.make_async_copy(stored_ref.at[layer], held_ref, sem)
        copy.start()
    else:
        held_ref, base_ref, out_ref = refs
    total = base_ref[...].astype(F32)
    if first:
        copy.wait()
    for at, bit in enumerate(bits):
        rows = block_at(bit, sources[at].shape[1], HEAD_DIM)
        total = total + jnp.dot(sources[at][...], held_ref[rows, :], preferred_element_type=F32)
    out_ref[...] = total.astype(out_ref.dtype)


def emit(parts, bits, weight, base, out_type, first, layer):
    tok, width = parts[0].shape
    cols = base.shape[1]
    parts_n = len(parts)
    out_shape = [pltpu.VMEM((tok, cols), out_type)]
    if out_type == BF16 and layer == LAYERS - 1:
        out_shape = [jax.ShapeDtypeStruct((tok, cols), out_type)]
    scratch = []
    if first:
        out_shape.append(pltpu.VMEM(weight.shape[1:], BF16))
        scratch.append(pltpu.SemaphoreType.DMA)
    return pl.pallas_call(
        partial(emit_kernel, bits, first, layer),
        out_shape=out_shape,
        in_specs=[VMEM] * parts_n + [HBM if first else VMEM, VMEM],
        out_specs=[VMEM] * len(out_shape),
        scratch_shapes=scratch,
        cost_estimate=cost(
            2 * tok * width * cols * parts_n, parts_n * width * (cols + tok) * 2 + tok * cols * 6
        ),
        compiler_params=PARAMS,
    )(*parts, weight if first else in_vmem(weight), base if first else in_vmem(base))


def bias_kernel(layer, sp, table_ref, out_ref, *refs):
    *halo_refs, rows_ref = refs
    heads_n, spans = out_ref.shape[:2]
    offsets, cols = table_ref.shape[2:]
    rows_ref[...] = jnp.zeros_like(rows_ref)
    for head in range(heads_n):
        rows_ref[head, :offsets, :cols] = table_ref[layer, head]
    shape = (GRID_W, LANES)
    query_col = lax.broadcasted_iota(jnp.int32, shape, 0)
    lane = lax.broadcasted_iota(jnp.int32, shape, 1)
    key_col = lane % GRID_W
    first_col = jnp.clip(query_col - COL_SPAN // 2, 0, GRID_W - COL_SPAN)
    inside = (key_col >= first_col) & (key_col < first_col + COL_SPAN)
    for head in range(heads_n):
        plain = rows_ref[head]
        after = pltpu.roll(pltpu.roll(plain, GRID_W, axis=1), rows_ref.shape[1] - 1, axis=0)
        at_lane = lax.broadcasted_iota(jnp.int32, plain.shape, 1)
        both = jnp.where(at_lane < GRID_W, plain, after)
        for span in range(spans):
            row = jnp.broadcast_to(both[span : span + 1, :], shape)
            turned = pltpu.roll(row, LANES - (COL_SPAN - 1), axis=1, stride=1, stride_axis=0)
            out_ref[head, span] = jnp.where(inside, turned, NEG)
    for halo_ref in halo_refs:
        for row in range(halo_ref.shape[0]):
            for at in range(halo_ref.shape[2]):
                one = window_at(row, halo_ref.shape[0], sp) + 2 * at
                low = one + jnp.where(one < HALF, HALF - 1, ROW_SPAN - 1) - row
                high = one + jnp.where(one + 1 < HALF, HALF - 1, ROW_SPAN - 1) - row
                for head in range(heads_n):
                    halo_ref[row, head, at] = jnp.where(
                        lane < GRID_W, out_ref[head, low], out_ref[head, high]
                    )


def expand_bias(table, layer, halo_rows):
    _, heads_n, offsets, _ = table.shape
    spans = offsets - 1
    out_shape = [pltpu.VMEM((heads_n, spans, GRID_W, LANES), F32)]
    if halo_rows:
        out_shape.append(pltpu.VMEM((halo_rows, heads_n, HALF // 2, GRID_W, LANES), F32))
    return pl.pallas_call(
        partial(bias_kernel, layer, lax.axis_size("sp")),
        out_shape=out_shape,
        in_specs=[VMEM],
        out_specs=[VMEM] * len(out_shape),
        scratch_shapes=[pltpu.VMEM((heads_n, 2 * ROW_SPAN, LANES), F32)],
        cost_estimate=cost(heads_n * spans * GRID_W * LANES * 40, heads_n * spans * GRID_W * LANES * 4),
        compiler_params=PARAMS,
        name="expand_bias",
    )(table)


def stacked_query(query, lane, heads_in):
    if heads_in == 1:
        return query
    zero = jnp.zeros_like(query)
    return jnp.concatenate(
        [jnp.where(lane // HEAD_DIM == head, query, zero) for head in range(heads_in)], axis=0
    )


def own_kernel(rows_dev, query_ref, pair_ref, bias_ref, mixed_ref, peak_ref):
    channels = query_ref.shape[2]
    group = min(LANES, channels)
    heads_in = group // HEAD_DIM
    tok = rows_dev * GRID_W
    stack = heads_in * GRID_W
    lane = lax.broadcasted_iota(jnp.int32, (GRID_W, group), 1)
    ones = jnp.ones((tok, LANES), BF16)
    for pair in range(channels // group):
        cols = slice(pair * group, (pair + 1) * group)
        query = jnp.concatenate(
            [
                stacked_query(query_ref[0, row * GRID_W : (row + 1) * GRID_W, cols], lane, heads_in)
                for row in range(rows_dev)
            ],
            axis=0,
        )
        scores = nt_dot(query, pair_ref[0, :, cols])
        values = jnp.concatenate([pair_ref[1, :, cols], ones], axis=1)
        for row in range(rows_dev):
            here = slice(row * stack, (row + 1) * stack)
            pieces = []
            for at in range(tok // LANES):
                offset = (LANES // GRID_W) * at - row + ROW_SPAN - 1
                bias = jnp.concatenate(
                    [bias_ref[pair * heads_in + head, offset] for head in range(heads_in)], axis=0
                )
                pieces.append(scores[here, at * LANES : (at + 1) * LANES] + bias)
            peak = pieces[0]
            for piece in pieces[1:]:
                peak = jnp.maximum(peak, piece)
            peak = jnp.max(peak, axis=1, keepdims=True)
            lifted = jnp.concatenate([jnp.exp(piece - peak).astype(BF16) for piece in pieces], axis=1)
            mixed_ref[pair, here, :] = jnp.dot(lifted, values, preferred_element_type=F32)
            peak_ref[pair, here, :] = jnp.broadcast_to(peak, (stack, LANES))


def attend_own(query, pair, bias, rows_dev):
    _, tok, channels = query.shape
    group = min(LANES, channels)
    pairs, rows = channels // group, tok * (group // HEAD_DIM)
    return pl.pallas_call(
        partial(own_kernel, rows_dev),
        out_shape=[
            pltpu.VMEM((pairs, rows, group + LANES), F32),
            pltpu.VMEM((pairs, rows, LANES), F32),
        ],
        in_specs=[VMEM] * 3,
        out_specs=[VMEM] * 2,
        cost_estimate=cost(pairs * rows * tok * 800, bias.size * 4, pairs * rows * tok),
        compiler_params=PARAMS,
        name="attend_own",
    )(*map(in_vmem, (query, pair, bias)))


def halo_kernel(
    rows_dev, sp, query_ref, even_ref, odd_ref, bias_ref, mixed_ref, peak_ref, out_ref, keys, values
):
    channels = query_ref.shape[2]
    group = min(LANES, channels)
    heads_in = group // HEAD_DIM
    span = HALF * GRID_W
    stack = heads_in * GRID_W
    even_slot, odd_slot = halo_slots(HALF)
    for scratch, kind in ((keys, 0), (values, 1)):
        scratch[pl.ds(even_slot, span), :] = even_ref[kind]
        scratch[pl.ds(odd_slot, span), :] = odd_ref[kind]
    lane = lax.broadcasted_iota(jnp.int32, (GRID_W, group), 1)
    ones = jnp.ones((span, LANES), BF16)
    for row in range(rows_dev):
        first = pl.multiple_of(window_at(row, rows_dev, sp) * GRID_W, GRID_W)
        here = slice(row * stack, (row + 1) * stack)
        for pair in range(channels // group):
            cols = slice(pair * group, (pair + 1) * group)
            query = stacked_query(query_ref[0, row * GRID_W : (row + 1) * GRID_W, cols], lane, heads_in)
            scores = nt_dot(query, keys[pl.ds(first, span), cols])
            pieces = []
            for at in range(span // LANES):
                bias = jnp.concatenate(
                    [bias_ref[row, pair * heads_in + head, at] for head in range(heads_in)], axis=0
                )
                pieces.append(scores[:, at * LANES : (at + 1) * LANES] + bias)
            peak = pieces[0]
            for piece in pieces[1:]:
                peak = jnp.maximum(peak, piece)
            before = peak_ref[pair, here, :]
            peak = jnp.maximum(jnp.max(peak, axis=1, keepdims=True), before)
            lifted = jnp.concatenate([jnp.exp(piece - peak).astype(BF16) for piece in pieces], axis=1)
            wide = jnp.concatenate([values[pl.ds(first, span), cols], ones], axis=1)
            mixed = jnp.dot(lifted, wide, preferred_element_type=F32)
            fade = jnp.exp(before - peak)
            top = mixed_ref[pair, here, :group] * fade[:, :group] + mixed[:, :group]
            weight = mixed_ref[pair, here, group:] * fade + mixed[:, group:]
            result, total = top[:GRID_W], weight[:GRID_W, :group]
            for head in range(1, heads_in):
                mine = lane // HEAD_DIM == head
                below = slice(head * GRID_W, (head + 1) * GRID_W)
                result = jnp.where(mine, top[below], result)
                total = jnp.where(mine, weight[below, :group], total)
            out_ref[row * GRID_W : (row + 1) * GRID_W, cols] = (result / total).astype(BF16)


def attend_halo(query, even, odd, bias, mixed, peak, rows_dev):
    _, tok, channels = query.shape
    scores = tok * (channels // HEAD_DIM) * HALF * GRID_W
    return pl.pallas_call(
        partial(halo_kernel, rows_dev, lax.axis_size("sp")),
        out_shape=pltpu.VMEM((tok, channels), BF16),
        in_specs=[VMEM] * 6,
        out_specs=VMEM,
        scratch_shapes=[pltpu.VMEM((ROW_SPAN * GRID_W, channels), BF16)] * 2,
        cost_estimate=cost(scores * HEAD_DIM * 6, bias.size * 4 + tok * channels * 16, scores),
        compiler_params=PARAMS,
        name="attend_halo",
    )(*map(in_vmem, (query, even, odd, bias, mixed, peak)))


def attend_kernel(
    rows_dev, sp, query_ref, own_ref, even_ref, odd_ref, bias_ref, out_ref, keys, values
):
    channels = query_ref.shape[2]
    group = min(LANES, channels)
    heads_in = group // HEAD_DIM
    span = ROW_SPAN * GRID_W
    even_slot, odd_slot = halo_slots(HALF + rows_dev)
    halo = HALF * GRID_W
    for scratch, kind in ((keys, 0), (values, 1)):
        scratch[HALF * GRID_W : (HALF + rows_dev) * GRID_W, :] = own_ref[kind]
        scratch[pl.ds(even_slot, halo), :] = even_ref[kind]
        scratch[pl.ds(odd_slot, halo), :] = odd_ref[kind]
    lane = lax.broadcasted_iota(jnp.int32, (GRID_W, group), 1)
    ones = jnp.ones((span, group), BF16)
    for row in range(rows_dev):
        window = window_at(row, rows_dev, sp)
        first = pl.multiple_of(window * GRID_W, GRID_W)
        offset = window - row + HALF - 1
        for pair in range(channels // group):
            cols = slice(pair * group, (pair + 1) * group)
            query = query_ref[0, row * GRID_W : (row + 1) * GRID_W, cols]
            query = stacked_query(query, lane, heads_in)
            scores = nt_dot(query, keys[pl.ds(first, span), cols])
            pieces = []
            for at in range(span // LANES):
                bias = jnp.concatenate(
                    [
                        bias_ref[pair * heads_in + head, offset + (LANES // GRID_W) * at]
                        for head in range(heads_in)
                    ],
                    axis=0,
                )
                pieces.append(scores[:, at * LANES : (at + 1) * LANES] + bias)
            peak = pieces[0]
            for piece in pieces[1:]:
                peak = jnp.maximum(peak, piece)
            peak = jnp.max(peak, axis=1, keepdims=True)
            lifted = jnp.concatenate([jnp.exp(piece - peak).astype(BF16) for piece in pieces], axis=1)
            mixed = jnp.dot(lifted, values[pl.ds(first, span), cols], preferred_element_type=F32)
            weight = jnp.dot(lifted, ones, preferred_element_type=F32)
            mixed = mixed / weight
            result = mixed[:GRID_W]
            for head in range(1, heads_in):
                result = jnp.where(
                    lane // HEAD_DIM == head, mixed[head * GRID_W : (head + 1) * GRID_W], result
                )
            out_ref[row * GRID_W : (row + 1) * GRID_W, cols] = result.astype(BF16)


def attend(query, own, even, odd, bias, rows_dev):
    _, tok, channels = query.shape
    padded = (rows_dev + 2 * HALF) * GRID_W
    scores = tok * (channels // HEAD_DIM) * ROW_SPAN * GRID_W
    return pl.pallas_call(
        partial(attend_kernel, rows_dev, lax.axis_size("sp")),
        out_shape=pltpu.VMEM((tok, channels), BF16),
        in_specs=[VMEM] * 5,
        out_specs=VMEM,
        scratch_shapes=[pltpu.VMEM((padded, channels), BF16)] * 2,
        cost_estimate=cost(scores * HEAD_DIM * 6, bias.size * 4 + tok * channels * 16, scores),
        compiler_params=PARAMS,
        name="attend",
    )(query, own, even, odd, bias)


def exchange(block, pairs):
    sp, tp = lax.axis_size("sp"), lax.axis_size("tp")
    partner = {}
    for one, two in pairs:
        partner[one], partner[two] = two, one
    moves = []
    for row in range(sp):
        for col in range(tp):
            if row in partner:
                moves.append((row * tp + col, partner[row] * tp + col))
            elif tp % 2 == 0:
                moves.append((row * tp + col, row * tp + (col ^ 1)))
    return lax.ppermute(block, ("sp", "tp"), moves)


def flip(block, axis, bit):
    count = lax.axis_size(axis)
    return lax.ppermute(block, axis, [(at, at ^ bit) for at in range(count)])


def body(hidden_in, norm_gain, query_weight, key_weight, value_weight, output_weight, offset_bias):
    tok_dev, _ = hidden_in.shape
    rows_dev = tok_dev // GRID_W
    tp = lax.axis_size("tp")
    sp = lax.axis_size("sp")
    is_odd = lax.axis_index("sp") % 2
    split = rows_dev == HALF
    weights = [in_hbm(weight) for weight in (query_weight, key_weight, value_weight)]
    output_weight = in_hbm(output_weight)
    even_pairs = [(at, at + 1) for at in range(0, sp - 1, 2)]
    odd_pairs = [(at, at + 1) for at in range(1, sp - 1, 2)]
    stream = hidden_in
    for layer in range(LAYERS):
        step = partial(project, layer=layer, gain=norm_gain)
        if tp == 4:
            across = flip(stream, "tp", 2)
            beside = flip(stream, "tp", 1)
            corner = flip(across, "tp", 1)
            *carried, held = step([stream], (0,), weights, None, None)
            carried = step([beside], (1,), held, carried, None)
            carried = step([across], (2,), held, carried, None)
            (pair,) = step([corner], (3,), held, carried, (1, 2))
            (query,) = step([corner], (3,), held, carried, (0,))
        else:
            gathered = lax.all_gather(stream, "tp", axis=1, tiled=True)
            *carried, held = step([gathered], (None,), weights, None, (0, 1, 2))
            query, pair = carried[0][:1], carried[0][1:]
        if split:
            to_even = to_odd = pair
        else:
            low, top = pair[:, : HALF * GRID_W], pair[:, (rows_dev - HALF) * GRID_W :]
            to_even = jnp.where(is_odd == 0, top, low)
            to_odd = jnp.where(is_odd == 0, low, top)
        even = exchange(to_even, even_pairs)
        odd = exchange(to_odd, odd_pairs)
        bias, *halo_bias = expand_bias(offset_bias, layer, rows_dev if split else 0)
        if split:
            mixed, peak = attend_own(query, pair, bias, rows_dev)
            attended = attend_halo(
                query, even, odd, halo_bias[0], mixed, peak, rows_dev
            )
        else:
            attended = attend(query, pair, even, odd, bias, rows_dev)
        step = partial(emit, layer=layer)
        if tp == 4:
            across = flip(attended, "tp", 2)
            beside = flip(attended, "tp", 1)
            corner = flip(across, "tp", 1)
            partly, held = step([attended], (0,), output_weight, stream, F32, True)
            (partly,) = step([beside], (1,), held, partly, F32, False)
            (partly,) = step([across], (2,), held, partly, F32, False)
            (stream,) = step([corner], (3,), held, partly, BF16, False)
        else:
            gathered = lax.all_gather(attended, "tp", axis=1, tiled=True)
            stream, _ = step([gathered], (None,), output_weight, stream, BF16, True)
    return stream


def solution(mesh):
    return jax.shard_map(
        body,
        mesh=mesh,
        in_specs=(
            P(("grp", "sp"), "tp"),
            P(),
            P(None, "tp", None),
            P(None, "tp", None),
            P(None, "tp", None),
            P(None, None, "tp"),
            P(None, "tp", None, None),
        ),
        out_specs=P(("grp", "sp"), "tp"),
        check_vma=False,
    )
```

```python
from functools import partial

import jax
import jax.numpy as jnp
from jax import lax
from jax.experimental import pallas as pl
from jax.experimental.pallas import tpu as pltpu
from jax.sharding import PartitionSpec as P


HEAD_DIM = 64
GRID_W = 64
ROW_SPAN = 8
COL_SPAN = 16
LAYERS = 3
HALF = ROW_SPAN // 2

EPS = 1e-06
NEG = -1e30
LANES = 128
F32 = jnp.float32
BF16 = jnp.bfloat16

PARAMS = pltpu.CompilerParams(vmem_limit_bytes=8 * 2**20)
VMEM = pl.BlockSpec(memory_space=pltpu.VMEM)
HBM = pl.BlockSpec(memory_space=pltpu.HBM)


def nt_dot(left, right):
    return lax.dot_general(left, right, (((1,), (1,)), ((), ())), preferred_element_type=F32)


def in_vmem(array):
    return pltpu.with_memory_space_constraint(array, memory_space=pltpu.VMEM)


def in_hbm(array):
    return pltpu.with_memory_space_constraint(array, memory_space=pltpu.HBM)


def cost(flops, bytes_accessed, transcendentals=0):
    return pl.CostEstimate(
        flops=int(flops), bytes_accessed=int(bytes_accessed), transcendentals=int(transcendentals)
    )


def block_at(bit, width, unit):
    if bit is None:
        return slice(None)
    return pl.ds(pl.multiple_of((lax.axis_index("tp") ^ bit) * width, unit), width)


def window_at(row, rows_dev, sp):
    first_row = lax.axis_index("sp") * rows_dev
    first = jnp.minimum(jnp.maximum(first_row + row - HALF, 0), rows_dev * sp - ROW_SPAN)
    return first - first_row + HALF


def halo_slots(high):
    odd = lax.axis_index("sp") % 2
    return (
        pl.multiple_of((1 - odd) * (high * GRID_W), GRID_W),
        pl.multiple_of(odd * (high * GRID_W), GRID_W),
    )


def project_kernel(bits, load, first, kinds, layer, *refs):
    sources, refs = refs[: len(bits)], refs[len(bits) :]
    gain_ref, refs = refs[0], refs[1:]
    if load:
        stored, refs = refs[:3], refs[3:]
        *refs, held_ref, sems = refs
        copies = [
            pltpu.make_async_copy(stored[kind].at[layer], held_ref.at[kind], sems.at[kind])
            for kind in range(3)
        ]
        for copy in copies:
            copy.start()
    else:
        held_ref, refs = refs[0], refs[1:]
    if not first:
        (acc_in, sq_in), refs = refs[:2], refs[2:]
    full = gain_ref.shape[1]
    totals = [None, None, None]
    squares = None
    for at, bit in enumerate(bits):
        wide = sources[at][...].astype(F32)
        width = wide.shape[1]
        cols = block_at(bit, width, LANES)
        square = jnp.sum(wide * wide, axis=1, keepdims=True)
        squares = square if squares is None else squares + square
        scaled = (wide * gain_ref[layer : layer + 1, cols]).astype(BF16)
        for kind in kinds or range(3):
            if load and at == 0:
                copies[kind].wait()
            product = nt_dot(scaled, held_ref[kind, :, cols])
            totals[kind] = product if totals[kind] is None else totals[kind] + product
    if not first:
        squares = squares + sq_in[:, :1]
        for kind in kinds or range(3):
            totals[kind] = totals[kind] + acc_in[kind]
    if kinds:
        row_scale = lax.rsqrt(squares * (1.0 / full) + EPS)
        for at, kind in enumerate(kinds):
            scale = row_scale * HEAD_DIM ** (-0.5) if kind == 0 else row_scale
            refs[0][at] = (totals[kind] * scale).astype(BF16)
    else:
        acc_out, sq_out = refs
        for kind in range(3):
            acc_out[kind] = totals[kind]
        sq_out[...] = jnp.broadcast_to(squares, sq_out.shape)


def project(parts, bits, weights, carried, kinds, layer, gain):
    tok, width = parts[0].shape
    parts_n = len(parts)
    first = carried is None
    operands = [*parts, gain]
    specs = [VMEM] * (parts_n + 1)
    load = isinstance(weights, list)
    if load:
        _, channels, full = weights[0].shape
        operands += weights
        specs += [HBM] * 3
    else:
        _, channels, full = weights.shape
        operands.append(in_vmem(weights))
        specs.append(VMEM)
    if not first:
        operands += map(in_vmem, carried)
        specs += [VMEM] * 2
    if kinds:
        out_shape = [pltpu.VMEM((len(kinds), tok, channels), BF16)]
    else:
        out_shape = [pltpu.VMEM((3, tok, channels), F32), pltpu.VMEM((tok, LANES), F32)]
    scratch = []
    if load:
        out_shape.append(pltpu.VMEM((3, channels, full), BF16))
        scratch.append(pltpu.SemaphoreType.DMA((3,)))
    flops = 2 * tok * width * channels * len(kinds or range(3)) * parts_n
    return pl.pallas_call(
        partial(project_kernel, bits, load, first, kinds, layer),
        out_shape=out_shape,
        in_specs=specs,
        out_specs=[VMEM] * len(out_shape),
        scratch_shapes=scratch,
        cost_estimate=cost(flops, parts_n * width * (channels * 6 + tok * 2) + 4 * tok * channels),
        compiler_params=PARAMS,
    )(*operands)


def emit_kernel(bits, first, layer, *refs):
    sources, refs = refs[: len(bits)], refs[len(bits) :]
    if first:
        stored_ref, base_ref, out_ref, held_ref, sem = refs
        copy = pltpu.make_async_copy(stored_ref.at[layer], held_ref, sem)
        copy.start()
    else:
        held_ref, base_ref, out_ref = refs
    total = base_ref[...].astype(F32)
    if first:
        copy.wait()
    for at, bit in enumerate(bits):
        rows = block_at(bit, sources[at].shape[1], HEAD_DIM)
        total = total + jnp.dot(sources[at][...], held_ref[rows, :], preferred_element_type=F32)
    out_ref[...] = total.astype(out_ref.dtype)


def emit(parts, bits, weight, base, out_type, first, layer):
    tok, width = parts[0].shape
    cols = base.shape[1]
    parts_n = len(parts)
    out_shape = [pltpu.VMEM((tok, cols), out_type)]
    if out_type == BF16 and layer == LAYERS - 1:
        out_shape = [jax.ShapeDtypeStruct((tok, cols), out_type)]
    scratch = []
    if first:
        out_shape.append(pltpu.VMEM(weight.shape[1:], BF16))
        scratch.append(pltpu.SemaphoreType.DMA)
    return pl.pallas_call(
        partial(emit_kernel, bits, first, layer),
        out_shape=out_shape,
        in_specs=[VMEM] * parts_n + [HBM if first else VMEM, VMEM],
        out_specs=[VMEM] * len(out_shape),
        scratch_shapes=scratch,
        cost_estimate=cost(
            2 * tok * width * cols * parts_n, parts_n * width * (cols + tok) * 2 + tok * cols * 6
        ),
        compiler_params=PARAMS,
    )(*parts, weight if first else in_vmem(weight), base if first else in_vmem(base))


def fetch_kernel(pick, count, *refs):
    sources, targets, sems = refs[:count], refs[count:-1], refs[-1]
    copies = [
        pltpu.make_async_copy(source, target, sems.at[at])
        for at, (source, target) in enumerate(pick(sources, targets))
    ]
    for copy in copies:
        copy.start()
    for copy in copies:
        copy.wait()


def fetch(arrays, shapes, pick, copies):
    return pl.pallas_call(
        partial(fetch_kernel, pick, len(arrays)),
        out_shape=[pltpu.VMEM(shape, BF16) for shape in shapes],
        in_specs=[HBM] * len(arrays),
        out_specs=[VMEM] * len(shapes),
        scratch_shapes=[pltpu.SemaphoreType.DMA((copies,))],
        cost_estimate=cost(10**6, 10**6),
        compiler_params=PARAMS,
    )(*arrays)


def load_weights(weights, layer):
    _, channels, full = weights[0].shape

    def pick(sources, targets):
        return [(source.at[layer], targets[0].at[kind]) for kind, source in enumerate(sources)]

    return fetch(weights, [(3, channels, full)], pick, 3)[0]


def cut_weight(weight, layer):
    _, rows, cols = weight.shape
    half = rows // 2
    widths = (cols // 2, cols // 4, cols // 4)

    def pick(sources, targets):
        here = pl.ds(pl.multiple_of(lax.axis_index("grp") * half, half), half)
        firsts = (0, cols // 2, 3 * cols // 4)
        return [
            (sources[0].at[layer, here, pl.ds(first, width)], target)
            for first, width, target in zip(firsts, widths, targets)
        ]

    return fetch([weight], [(half, width) for width in widths], pick, 3)


def far_kernel(pieces, own_ref, beside_ref, across_ref, corner_ref, base_ref, *refs):
    near, side, out_ref = refs[:pieces], refs[pieces:-1], refs[-1]
    me = lax.axis_index("tp")
    even = me % 2 == 0
    aligned = me // 2 == lax.axis_index("grp")
    own, beside, across, corner = own_ref[...], beside_ref[...], across_ref[...], corner_ref[...]
    mine = jnp.concatenate([jnp.where(even, own, beside), jnp.where(even, beside, own)], axis=1)
    other = jnp.concatenate(
        [jnp.where(even, across, corner), jnp.where(even, corner, across)], axis=1
    )
    with_near = jnp.where(aligned, mine, other)
    with_side = jnp.where(aligned, other, mine)
    done = 0
    for at in range(pieces):
        cols = slice(done, done + near[at].shape[1])
        done = cols.stop
        total = base_ref[:, cols].astype(F32)
        total = total + jnp.dot(with_near, near[at][...], preferred_element_type=F32)
        total = total + jnp.dot(with_side, side[at][...], preferred_element_type=F32)
        out_ref[:, cols] = total.astype(BF16)


def emit_far(parts, base, near, side):
    tok, cols = base.shape
    operands = [*parts, base, *near, *side]
    return pl.pallas_call(
        partial(far_kernel, len(near)),
        out_shape=pltpu.VMEM((tok, cols), BF16),
        in_specs=[VMEM] * len(operands),
        out_specs=VMEM,
        cost_estimate=cost(2 * tok * cols * 4 * parts[0].shape[1], 10**6),
        compiler_params=PARAMS,
        name="lent",
    )(*map(in_vmem, operands))


def bias_kernel(layer, sp, table_ref, out_ref, *refs):
    *halo_refs, rows_ref = refs
    heads_n, spans = out_ref.shape[:2]
    offsets, cols = table_ref.shape[2:]
    rows_ref[...] = jnp.zeros_like(rows_ref)
    for head in range(heads_n):
        rows_ref[head, :offsets, :cols] = table_ref[layer, head]
    shape = (GRID_W, LANES)
    query_col = lax.broadcasted_iota(jnp.int32, shape, 0)
    lane = lax.broadcasted_iota(jnp.int32, shape, 1)
    key_col = lane % GRID_W
    first_col = jnp.clip(query_col - COL_SPAN // 2, 0, GRID_W - COL_SPAN)
    inside = (key_col >= first_col) & (key_col < first_col + COL_SPAN)
    for head in range(heads_n):
        plain = rows_ref[head]
        after = pltpu.roll(pltpu.roll(plain, GRID_W, axis=1), rows_ref.shape[1] - 1, axis=0)
        at_lane = lax.broadcasted_iota(jnp.int32, plain.shape, 1)
        both = jnp.where(at_lane < GRID_W, plain, after)
        for span in range(spans):
            row = jnp.broadcast_to(both[span : span + 1, :], shape)
            turned = pltpu.roll(row, LANES - (COL_SPAN - 1), axis=1, stride=1, stride_axis=0)
            out_ref[head, span] = jnp.where(inside, turned, NEG)
    for halo_ref in halo_refs:
        for row in range(halo_ref.shape[0]):
            for at in range(halo_ref.shape[2]):
                one = window_at(row, halo_ref.shape[0], sp) + 2 * at
                low = one + jnp.where(one < HALF, HALF - 1, ROW_SPAN - 1) - row
                high = one + jnp.where(one + 1 < HALF, HALF - 1, ROW_SPAN - 1) - row
                for head in range(heads_n):
                    halo_ref[row, head, at] = jnp.where(
                        lane < GRID_W, out_ref[head, low], out_ref[head, high]
                    )


def expand_bias(table, layer, halo_rows):
    _, heads_n, offsets, _ = table.shape
    spans = offsets - 1
    out_shape = [pltpu.VMEM((heads_n, spans, GRID_W, LANES), F32)]
    if halo_rows:
        out_shape.append(pltpu.VMEM((halo_rows, heads_n, HALF // 2, GRID_W, LANES), F32))
    return pl.pallas_call(
        partial(bias_kernel, layer, lax.axis_size("sp")),
        out_shape=out_shape,
        in_specs=[VMEM],
        out_specs=[VMEM] * len(out_shape),
        scratch_shapes=[pltpu.VMEM((heads_n, 2 * ROW_SPAN, LANES), F32)],
        cost_estimate=cost(heads_n * spans * GRID_W * LANES * 40, heads_n * spans * GRID_W * LANES * 4),
        compiler_params=PARAMS,
        name="expand_bias",
    )(table)


def stacked_query(query, lane, heads_in):
    if heads_in == 1:
        return query
    zero = jnp.zeros_like(query)
    return jnp.concatenate(
        [jnp.where(lane // HEAD_DIM == head, query, zero) for head in range(heads_in)], axis=0
    )


def own_kernel(rows_dev, query_ref, pair_ref, bias_ref, mixed_ref, peak_ref):
    channels = query_ref.shape[2]
    group = min(LANES, channels)
    heads_in = group // HEAD_DIM
    tok = rows_dev * GRID_W
    stack = heads_in * GRID_W
    lane = lax.broadcasted_iota(jnp.int32, (GRID_W, group), 1)
    ones = jnp.ones((tok, LANES), BF16)
    for pair in range(channels // group):
        cols = slice(pair * group, (pair + 1) * group)
        query = jnp.concatenate(
            [
                stacked_query(query_ref[0, row * GRID_W : (row + 1) * GRID_W, cols], lane, heads_in)
                for row in range(rows_dev)
            ],
            axis=0,
        )
        scores = nt_dot(query, pair_ref[0, :, cols])
        values = jnp.concatenate([pair_ref[1, :, cols], ones], axis=1)
        for row in range(rows_dev):
            here = slice(row * stack, (row + 1) * stack)
            pieces = []
            for at in range(tok // LANES):
                offset = (LANES // GRID_W) * at - row + ROW_SPAN - 1
                bias = jnp.concatenate(
                    [bias_ref[pair * heads_in + head, offset] for head in range(heads_in)], axis=0
                )
                pieces.append(scores[here, at * LANES : (at + 1) * LANES] + bias)
            peak = pieces[0]
            for piece in pieces[1:]:
                peak = jnp.maximum(peak, piece)
            peak = jnp.max(peak, axis=1, keepdims=True)
            lifted = jnp.concatenate([jnp.exp(piece - peak).astype(BF16) for piece in pieces], axis=1)
            mixed_ref[pair, here, :] = jnp.dot(lifted, values, preferred_element_type=F32)
            peak_ref[pair, here, :] = jnp.broadcast_to(peak, (stack, LANES))


def attend_own(query, pair, bias, rows_dev):
    _, tok, channels = query.shape
    group = min(LANES, channels)
    pairs, rows = channels // group, tok * (group // HEAD_DIM)
    return pl.pallas_call(
        partial(own_kernel, rows_dev),
        out_shape=[
            pltpu.VMEM((pairs, rows, group + LANES), F32),
            pltpu.VMEM((pairs, rows, LANES), F32),
        ],
        in_specs=[VMEM] * 3,
        out_specs=[VMEM] * 2,
        cost_estimate=cost(pairs * rows * tok * 800, bias.size * 4, pairs * rows * tok),
        compiler_params=PARAMS,
        name="attend_own",
    )(*map(in_vmem, (query, pair, bias)))


def halo_kernel(
    rows_dev, sp, query_ref, even_ref, odd_ref, bias_ref, mixed_ref, peak_ref, out_ref, keys, values
):
    channels = query_ref.shape[2]
    group = min(LANES, channels)
    heads_in = group // HEAD_DIM
    span = HALF * GRID_W
    stack = heads_in * GRID_W
    even_slot, odd_slot = halo_slots(HALF)
    for scratch, kind in ((keys, 0), (values, 1)):
        scratch[pl.ds(even_slot, span), :] = even_ref[kind]
        scratch[pl.ds(odd_slot, span), :] = odd_ref[kind]
    lane = lax.broadcasted_iota(jnp.int32, (GRID_W, group), 1)
    ones = jnp.ones((span, LANES), BF16)
    for row in range(rows_dev):
        first = pl.multiple_of(window_at(row, rows_dev, sp) * GRID_W, GRID_W)
        here = slice(row * stack, (row + 1) * stack)
        for pair in range(channels // group):
            cols = slice(pair * group, (pair + 1) * group)
            query = stacked_query(query_ref[0, row * GRID_W : (row + 1) * GRID_W, cols], lane, heads_in)
            scores = nt_dot(query, keys[pl.ds(first, span), cols])
            pieces = []
            for at in range(span // LANES):
                bias = jnp.concatenate(
                    [bias_ref[row, pair * heads_in + head, at] for head in range(heads_in)], axis=0
                )
                pieces.append(scores[:, at * LANES : (at + 1) * LANES] + bias)
            peak = pieces[0]
            for piece in pieces[1:]:
                peak = jnp.maximum(peak, piece)
            before = peak_ref[pair, here, :]
            peak = jnp.maximum(jnp.max(peak, axis=1, keepdims=True), before)
            lifted = jnp.concatenate([jnp.exp(piece - peak).astype(BF16) for piece in pieces], axis=1)
            wide = jnp.concatenate([values[pl.ds(first, span), cols], ones], axis=1)
            mixed = jnp.dot(lifted, wide, preferred_element_type=F32)
            fade = jnp.exp(before - peak)
            top = mixed_ref[pair, here, :group] * fade[:, :group] + mixed[:, :group]
            weight = mixed_ref[pair, here, group:] * fade + mixed[:, group:]
            result, total = top[:GRID_W], weight[:GRID_W, :group]
            for head in range(1, heads_in):
                mine = lane // HEAD_DIM == head
                below = slice(head * GRID_W, (head + 1) * GRID_W)
                result = jnp.where(mine, top[below], result)
                total = jnp.where(mine, weight[below, :group], total)
            out_ref[row * GRID_W : (row + 1) * GRID_W, cols] = (result / total).astype(BF16)


def attend_halo(query, even, odd, bias, mixed, peak, rows_dev):
    _, tok, channels = query.shape
    scores = tok * (channels // HEAD_DIM) * HALF * GRID_W
    return pl.pallas_call(
        partial(halo_kernel, rows_dev, lax.axis_size("sp")),
        out_shape=pltpu.VMEM((tok, channels), BF16),
        in_specs=[VMEM] * 6,
        out_specs=VMEM,
        scratch_shapes=[pltpu.VMEM((ROW_SPAN * GRID_W, channels), BF16)] * 2,
        cost_estimate=cost(scores * HEAD_DIM * 6, bias.size * 4 + tok * channels * 16, scores),
        compiler_params=PARAMS,
        name="attend_halo",
    )(*map(in_vmem, (query, even, odd, bias, mixed, peak)))


def attend_kernel(
    rows_dev, sp, query_ref, own_ref, even_ref, odd_ref, bias_ref, out_ref, keys, values
):
    channels = query_ref.shape[2]
    group = min(LANES, channels)
    heads_in = group // HEAD_DIM
    span = ROW_SPAN * GRID_W
    even_slot, odd_slot = halo_slots(HALF + rows_dev)
    halo = HALF * GRID_W
    for scratch, kind in ((keys, 0), (values, 1)):
        scratch[HALF * GRID_W : (HALF + rows_dev) * GRID_W, :] = own_ref[kind]
        scratch[pl.ds(even_slot, halo), :] = even_ref[kind]
        scratch[pl.ds(odd_slot, halo), :] = odd_ref[kind]
    lane = lax.broadcasted_iota(jnp.int32, (GRID_W, group), 1)
    ones = jnp.ones((span, group), BF16)
    for row in range(rows_dev):
        window = window_at(row, rows_dev, sp)
        first = pl.multiple_of(window * GRID_W, GRID_W)
        offset = window - row + HALF - 1
        for pair in range(channels // group):
            cols = slice(pair * group, (pair + 1) * group)
            query = query_ref[0, row * GRID_W : (row + 1) * GRID_W, cols]
            query = stacked_query(query, lane, heads_in)
            scores = nt_dot(query, keys[pl.ds(first, span), cols])
            pieces = []
            for at in range(span // LANES):
                bias = jnp.concatenate(
                    [
                        bias_ref[pair * heads_in + head, offset + (LANES // GRID_W) * at]
                        for head in range(heads_in)
                    ],
                    axis=0,
                )
                pieces.append(scores[:, at * LANES : (at + 1) * LANES] + bias)
            peak = pieces[0]
            for piece in pieces[1:]:
                peak = jnp.maximum(peak, piece)
            peak = jnp.max(peak, axis=1, keepdims=True)
            lifted = jnp.concatenate([jnp.exp(piece - peak).astype(BF16) for piece in pieces], axis=1)
            mixed = jnp.dot(lifted, values[pl.ds(first, span), cols], preferred_element_type=F32)
            weight = jnp.dot(lifted, ones, preferred_element_type=F32)
            mixed = mixed / weight
            result = mixed[:GRID_W]
            for head in range(1, heads_in):
                result = jnp.where(
                    lane // HEAD_DIM == head, mixed[head * GRID_W : (head + 1) * GRID_W], result
                )
            out_ref[row * GRID_W : (row + 1) * GRID_W, cols] = result.astype(BF16)


def attend(query, own, even, odd, bias, rows_dev):
    _, tok, channels = query.shape
    padded = (rows_dev + 2 * HALF) * GRID_W
    scores = tok * (channels // HEAD_DIM) * ROW_SPAN * GRID_W
    return pl.pallas_call(
        partial(attend_kernel, rows_dev, lax.axis_size("sp")),
        out_shape=pltpu.VMEM((tok, channels), BF16),
        in_specs=[VMEM] * 5,
        out_specs=VMEM,
        scratch_shapes=[pltpu.VMEM((padded, channels), BF16)] * 2,
        cost_estimate=cost(scores * HEAD_DIM * 6, bias.size * 4 + tok * channels * 16, scores),
        compiler_params=PARAMS,
        name="attend",
    )(query, own, even, odd, bias)


def exchange(block, pairs):
    sp, tp = lax.axis_size("sp"), lax.axis_size("tp")
    partner = {}
    for one, two in pairs:
        partner[one], partner[two] = two, one
    moves = []
    for row in range(sp):
        for col in range(tp):
            if row in partner:
                moves.append((row * tp + col, partner[row] * tp + col))
            elif tp % 2 == 0:
                moves.append((row * tp + col, row * tp + (col ^ 1)))
    return lax.ppermute(block, ("sp", "tp"), moves)


def flip(block, axis, bit):
    count = lax.axis_size(axis)
    return lax.ppermute(block, axis, [(at, at ^ bit) for at in range(count)])


def send_weight(weight, layer):
    cuts = cut_weight(weight, layer)
    near = []
    for cut in cuts:
        near.append(flip(cut, "tp", 2))
    return near


def body(hidden_in, norm_gain, query_weight, key_weight, value_weight, output_weight, offset_bias):
    tok_dev, _ = hidden_in.shape
    rows_dev = tok_dev // GRID_W
    tp = lax.axis_size("tp")
    sp = lax.axis_size("sp")
    is_odd = lax.axis_index("sp") % 2
    split = rows_dev == HALF
    weights = [in_hbm(weight) for weight in (query_weight, key_weight, value_weight)]
    output_weight = in_hbm(output_weight)
    even_pairs = [(at, at + 1) for at in range(0, sp - 1, 2)]
    odd_pairs = [(at, at + 1) for at in range(1, sp - 1, 2)]
    stream = hidden_in
    lend = split and tp == 4 and lax.axis_size("grp") == 2
    carry = None
    for layer in range(LAYERS):
        step = partial(project, layer=layer, gain=norm_gain)
        if carry is not None:
            parts, base, held = carry
            beside = flip(stream, "tp", 1)
            across = emit_far(parts, base, *last_lent)
            corner = flip(across, "tp", 1)
            carried = step([stream, across], (0, 2), held, None, None)
            carried = step([beside], (1,), held, carried, None)
        elif tp == 4:
            across = flip(stream, "tp", 2)
            beside = flip(stream, "tp", 1)
            corner = flip(across, "tp", 1)
            *carried, held = step([stream], (0,), weights, None, None)
            carried = step([beside], (1,), held, carried, None)
            carried = step([across], (2,), held, carried, None)
        if tp == 4:
            across_stream = across
            (pair,) = step([corner], (3,), held, carried, (1, 2))
            (query,) = step([corner], (3,), held, carried, (0,))
        else:
            gathered = lax.all_gather(stream, "tp", axis=1, tiled=True)
            *carried, held = step([gathered], (None,), weights, None, (0, 1, 2))
            query, pair = carried[0][:1], carried[0][1:]
        if lend and layer < LAYERS - 1:
            if layer == 0:
                near = send_weight(output_weight, layer)
            side = []
            for piece in near:
                side.append(flip(piece, "grp", 1))
            lent = (near, side)
        else:
            lent = None
        if split:
            to_even = to_odd = pair
        else:
            low, top = pair[:, : HALF * GRID_W], pair[:, (rows_dev - HALF) * GRID_W :]
            to_even = jnp.where(is_odd == 0, top, low)
            to_odd = jnp.where(is_odd == 0, low, top)
        even = exchange(to_even, even_pairs)
        odd = exchange(to_odd, odd_pairs)
        bias, *halo_bias = expand_bias(offset_bias, layer, rows_dev if split else 0)
        if split:
            mixed, peak = attend_own(query, pair, bias, rows_dev)
            attended = attend_halo(
                query, even, odd, halo_bias[0], mixed, peak, rows_dev
            )
        else:
            attended = attend(query, pair, even, odd, bias, rows_dev)
        step = partial(emit, layer=layer)
        carry = None
        if lent:
            last_lent = lent
            carry = load_weights(weights, layer + 1)
        if tp == 4:
            across = flip(attended, "tp", 2)
            beside = flip(attended, "tp", 1)
            corner = flip(across, "tp", 1)
            if lent and layer + 1 < LAYERS - 1:
                near = send_weight(output_weight, layer + 1)
            partly, held = step([attended], (0,), output_weight, stream, F32, True)
            (partly,) = step([beside], (1,), held, partly, F32, False)
            (partly,) = step([across], (2,), held, partly, F32, False)
            old = across_stream
            (stream,) = step([corner], (3,), held, partly, BF16, False)
            if carry is not None:
                carry = ([attended, beside, across, corner], old, carry)
        else:
            gathered = lax.all_gather(attended, "tp", axis=1, tiled=True)
            stream, _ = step([gathered], (None,), output_weight, stream, BF16, True)
    return stream


def solution(mesh):
    return jax.shard_map(
        body,
        mesh=mesh,
        in_specs=(
            P(("grp", "sp"), "tp"),
            P(),
            P(None, "tp", None),
            P(None, "tp", None),
            P(None, "tp", None),
            P(None, None, "tp"),
            P(None, "tp", None, None),
        ),
        out_specs=P(("grp", "sp"), "tp"),
        check_vma=False,
    )
```

```python
from functools import partial

import jax
import jax.numpy as jnp
from jax import lax
from jax.experimental import pallas as pl
from jax.experimental.pallas import tpu as pltpu
from jax.sharding import PartitionSpec as P


HEAD_DIM = 64
GRID_W = 64
ROW_SPAN = 8
COL_SPAN = 16
LAYERS = 3
HALF = ROW_SPAN // 2
PARTS = ((1, 2, 1), (2, 2))

EPS = 1e-06
NEG = -1e30
LANES = 128
F32 = jnp.float32
BF16 = jnp.bfloat16

PARAMS = pltpu.CompilerParams(vmem_limit_bytes=8 * 2**20)
VMEM = pl.BlockSpec(memory_space=pltpu.VMEM)
HBM = pl.BlockSpec(memory_space=pltpu.HBM)


def nt_dot(left, right):
    return lax.dot_general(left, right, (((1,), (1,)), ((), ())), preferred_element_type=F32)


def in_vmem(array):
    return pltpu.with_memory_space_constraint(array, memory_space=pltpu.VMEM)


def in_hbm(array):
    return pltpu.with_memory_space_constraint(array, memory_space=pltpu.HBM)


def cost(flops, bytes_accessed, transcendentals=0):
    return pl.CostEstimate(
        flops=int(flops), bytes_accessed=int(bytes_accessed), transcendentals=int(transcendentals)
    )


def call(kernel, operands, in_specs, out_shape, estimate, scratch=(), rider=None):
    taken, given = len(operands), len(out_shape)
    arrays, shapes, pick, count = rider or ((), (), None, 0)

    def carrying(*refs):
        ends = taken, taken + len(arrays), taken + len(arrays) + given
        last = ends[2] + len(shapes)
        copies = [
            pltpu.make_async_copy(source, target, refs[-1].at[at])
            for at, (source, target) in enumerate(
                pick(refs[ends[0] : ends[1]], refs[ends[2] : last])
            )
        ]
        for copy in copies:
            copy.start()
        kernel(*refs[: ends[0]], *refs[ends[1] : ends[2]], *refs[last:-1])
        for copy in copies:
            copy.wait()

    sems = [pltpu.SemaphoreType.DMA((count,))] if rider else []
    return pl.pallas_call(
        carrying if rider else kernel,
        out_shape=[*out_shape, *(pltpu.VMEM(shape, BF16) for shape in shapes)],
        in_specs=[*in_specs, *[HBM] * len(arrays)],
        out_specs=[VMEM] * (given + len(shapes)),
        scratch_shapes=[*scratch, *sems],
        cost_estimate=estimate,
        compiler_params=PARAMS,
    )(*operands, *arrays)


def block_at(bit, width, unit):
    if bit is None:
        return slice(None)
    return pl.ds(pl.multiple_of((lax.axis_index("tp") ^ bit) * width, unit), width)


def window_at(row, rows_dev, sp):
    first_row = lax.axis_index("sp") * rows_dev
    first = jnp.minimum(jnp.maximum(first_row + row - HALF, 0), rows_dev * sp - ROW_SPAN)
    return first - first_row + HALF


def halo_slots(high):
    odd = lax.axis_index("sp") % 2
    return (
        pl.multiple_of((1 - odd) * (high * GRID_W), GRID_W),
        pl.multiple_of(odd * (high * GRID_W), GRID_W),
    )


def project_kernel(bits, load, shared, first, kinds, layer, *refs):
    sources, refs = refs[: len(bits)], refs[len(bits) :]
    gain_ref, refs = refs[0], refs[1:]
    if load:
        stored, refs = refs[:3], refs[3:]
        *refs, held_ref, sems = refs
        copies = [
            pltpu.make_async_copy(stored[kind].at[layer], held_ref.at[kind], sems.at[kind])
            for kind in range(3)
        ]
        for copy in copies:
            copy.start()
    elif shared:
        stored, refs = refs[:3], refs[3:]
    else:
        held_ref, refs = refs[0], refs[1:]
    if not first:
        (acc_in, sq_in), refs = refs[:2], refs[2:]
    full = gain_ref.shape[1]
    totals = [None, None, None]
    squares = None
    for at, bit in enumerate(bits):
        wide = sources[at][...].astype(F32)
        width = wide.shape[1]
        cols = block_at(bit, width, LANES)
        square = jnp.sum(wide * wide, axis=1, keepdims=True)
        squares = square if squares is None else squares + square
        scaled = (wide * gain_ref[layer : layer + 1, cols]).astype(BF16)
        for kind in kinds or range(3):
            if load and at == 0:
                copies[kind].wait()
            held = stored[kind][layer, :, cols] if shared else held_ref[kind, :, cols]
            product = nt_dot(scaled, held)
            totals[kind] = product if totals[kind] is None else totals[kind] + product
    if not first:
        squares = squares + sq_in[:, :1]
        for kind in kinds or range(3):
            totals[kind] = totals[kind] + acc_in[kind]
    if kinds:
        row_scale = lax.rsqrt(squares * (1.0 / full) + EPS)
        for at, kind in enumerate(kinds):
            scale = row_scale * HEAD_DIM ** (-0.5) if kind == 0 else row_scale
            refs[0][at] = (totals[kind] * scale).astype(BF16)
    else:
        acc_out, sq_out = refs
        for kind in range(3):
            acc_out[kind] = totals[kind]
        sq_out[...] = jnp.broadcast_to(squares, sq_out.shape)


def project(parts, bits, weights, carried, kinds, layer, gain):
    tok, width = parts[0].shape
    parts_n = len(parts)
    first = carried is None
    operands = [*parts, gain]
    specs = [VMEM] * (parts_n + 1)
    load, shared = isinstance(weights, list), isinstance(weights, tuple)
    if load:
        _, channels, full = weights[0].shape
        operands += weights
        specs += [HBM] * 3
    elif shared:
        _, channels, full = weights[0].shape
        operands += weights
        specs += [VMEM] * 3
    else:
        _, channels, full = weights.shape
        operands.append(in_vmem(weights))
        specs.append(VMEM)
    if not first:
        operands += map(in_vmem, carried)
        specs += [VMEM] * 2
    if kinds:
        out_shape = [pltpu.VMEM((len(kinds), tok, channels), BF16)]
    else:
        out_shape = [pltpu.VMEM((3, tok, channels), F32), pltpu.VMEM((tok, LANES), F32)]
    scratch = []
    if load:
        out_shape.append(pltpu.VMEM((3, channels, full), BF16))
        scratch.append(pltpu.SemaphoreType.DMA((3,)))
    flops = 2 * tok * width * channels * len(kinds or range(3)) * parts_n
    return call(
        partial(project_kernel, bits, load, shared, first, kinds, layer),
        operands,
        specs,
        out_shape,
        cost(flops, parts_n * width * (channels * 6 + tok * 2) + 4 * tok * channels),
        scratch,
    )


def emit_kernel(bits, load, layer, *refs):
    sources, refs = refs[: len(bits)], refs[len(bits) :]
    held_ref, base_ref, out_ref, *rest = refs
    if load:
        stored_ref, (held_ref, sem) = held_ref, rest
        copy = pltpu.make_async_copy(stored_ref.at[layer], held_ref, sem)
        copy.start()
    total = base_ref[...].astype(F32)
    if load:
        copy.wait()
    for at, bit in enumerate(bits):
        rows = block_at(bit, sources[at].shape[1], HEAD_DIM)
        held = held_ref[rows, :] if load else held_ref[layer, rows, :]
        total = total + jnp.dot(sources[at][...], held, preferred_element_type=F32)
    out_ref[...] = total.astype(out_ref.dtype)


def emit(parts, bits, weight, base, out_type, load, layer):
    tok, width = parts[0].shape
    cols = base.shape[1]
    out_shape = [pltpu.VMEM((tok, cols), out_type)]
    if out_type == BF16 and layer == LAYERS - 1:
        out_shape = [jax.ShapeDtypeStruct((tok, cols), out_type)]
    scratch = []
    if load:
        scratch = [pltpu.VMEM(weight.shape[1:], BF16), pltpu.SemaphoreType.DMA]
    return call(
        partial(emit_kernel, bits, load, layer),
        [*parts, weight, base],
        [VMEM] * len(parts) + [HBM if load else VMEM, VMEM],
        out_shape,
        cost(2 * tok * width * cols * len(bits), 10**6),
        scratch,
    )


def cut_weight(weight):
    _, rows, cols = weight.shape
    half = rows // 2
    slabs = []
    for layer, parts in enumerate(PARTS):
        unit = cols // sum(parts)
        for at, part in enumerate(parts):
            slabs.append((layer, unit * sum(parts[:at]), unit * part))

    def pick(sources, targets):
        here = pl.ds(pl.multiple_of(lax.axis_index("grp") * half, half), half)
        return [
            (sources[0].at[layer, here, pl.ds(first, width)], target)
            for (layer, first, width), target in zip(slabs, targets)
        ]

    shapes = [(half, width) for _, _, width in slabs]
    rider = [weight], shapes, pick, len(slabs)
    cuts = call(lambda *refs: None, [], [], [], cost(10**6, 10**6), rider=rider)
    return [
        [cut for cut, slab in zip(cuts, slabs) if slab[0] == layer] for layer in range(len(PARTS))
    ]


def far_kernel(pieces, own_ref, beside_ref, across_ref, corner_ref, base_ref, *refs):
    near, side, out_ref = refs[:pieces], refs[pieces:-1], refs[-1]
    me = lax.axis_index("tp")
    even = me % 2 == 0
    aligned = me // 2 == lax.axis_index("grp")
    own, beside, across, corner = own_ref[...], beside_ref[...], across_ref[...], corner_ref[...]
    mine = jnp.concatenate([jnp.where(even, own, beside), jnp.where(even, beside, own)], axis=1)
    other = jnp.concatenate(
        [jnp.where(even, across, corner), jnp.where(even, corner, across)], axis=1
    )
    with_near = jnp.where(aligned, mine, other)
    with_side = jnp.where(aligned, other, mine)
    done = 0
    for at in range(pieces):
        cols = slice(done, done + near[at].shape[1])
        done = cols.stop
        total = base_ref[:, cols].astype(F32)
        total = total + jnp.dot(with_near, near[at][...], preferred_element_type=F32)
        total = total + jnp.dot(with_side, side[at][...], preferred_element_type=F32)
        out_ref[:, cols] = total.astype(BF16)


def emit_far(parts, base, near, side):
    tok, cols = base.shape
    operands = [*parts, base, *near, *side]
    return pl.pallas_call(
        partial(far_kernel, len(near)),
        out_shape=pltpu.VMEM((tok, cols), BF16),
        in_specs=[VMEM] * len(operands),
        out_specs=VMEM,
        cost_estimate=cost(2 * tok * cols * 4 * parts[0].shape[1], 10**6),
        compiler_params=PARAMS,
        name="lent",
    )(*map(in_vmem, operands))


def bias_kernel(layer, sp, table_ref, out_ref, *refs):
    *halo_refs, rows_ref = refs
    heads_n, spans = out_ref.shape[:2]
    offsets, cols = table_ref.shape[2:]
    rows_ref[...] = jnp.zeros_like(rows_ref)
    for head in range(heads_n):
        rows_ref[head, :offsets, :cols] = table_ref[layer, head]
    shape = (GRID_W, LANES)
    query_col = lax.broadcasted_iota(jnp.int32, shape, 0)
    lane = lax.broadcasted_iota(jnp.int32, shape, 1)
    key_col = lane % GRID_W
    first_col = jnp.clip(query_col - COL_SPAN // 2, 0, GRID_W - COL_SPAN)
    inside = (key_col >= first_col) & (key_col < first_col + COL_SPAN)
    for head in range(heads_n):
        plain = rows_ref[head]
        after = pltpu.roll(pltpu.roll(plain, GRID_W, axis=1), rows_ref.shape[1] - 1, axis=0)
        at_lane = lax.broadcasted_iota(jnp.int32, plain.shape, 1)
        both = jnp.where(at_lane < GRID_W, plain, after)
        for span in range(spans):
            row = jnp.broadcast_to(both[span : span + 1, :], shape)
            turned = pltpu.roll(row, LANES - (COL_SPAN - 1), axis=1, stride=1, stride_axis=0)
            out_ref[head, span] = jnp.where(inside, turned, NEG)
    for halo_ref in halo_refs:
        for row in range(halo_ref.shape[0]):
            for at in range(halo_ref.shape[2]):
                one = window_at(row, halo_ref.shape[0], sp) + 2 * at
                low = one + jnp.where(one < HALF, HALF - 1, ROW_SPAN - 1) - row
                high = one + jnp.where(one + 1 < HALF, HALF - 1, ROW_SPAN - 1) - row
                for head in range(heads_n):
                    halo_ref[row, head, at] = jnp.where(
                        lane < GRID_W, out_ref[head, low], out_ref[head, high]
                    )


def expand_bias(table, layer, halo_rows):
    _, heads_n, offsets, _ = table.shape
    spans = offsets - 1
    out_shape = [pltpu.VMEM((heads_n, spans, GRID_W, LANES), F32)]
    if halo_rows:
        out_shape.append(pltpu.VMEM((halo_rows, heads_n, HALF // 2, GRID_W, LANES), F32))
    return call(
        partial(bias_kernel, layer, lax.axis_size("sp")),
        [table],
        [VMEM],
        out_shape,
        cost(heads_n * spans * GRID_W * LANES * 40, heads_n * spans * GRID_W * LANES * 4),
        [pltpu.VMEM((heads_n, 2 * ROW_SPAN, LANES), F32)],
    )


def stacked_query(query, lane, heads_in):
    if heads_in == 1:
        return query
    zero = jnp.zeros_like(query)
    return jnp.concatenate(
        [jnp.where(lane // HEAD_DIM == head, query, zero) for head in range(heads_in)], axis=0
    )


def own_kernel(rows_dev, query_ref, pair_ref, bias_ref, mixed_ref, peak_ref):
    channels = query_ref.shape[2]
    group = min(LANES, channels)
    heads_in = group // HEAD_DIM
    tok = rows_dev * GRID_W
    stack = heads_in * GRID_W
    lane = lax.broadcasted_iota(jnp.int32, (GRID_W, group), 1)
    ones = jnp.ones((tok, LANES), BF16)
    for pair in range(channels // group):
        cols = slice(pair * group, (pair + 1) * group)
        query = jnp.concatenate(
            [
                stacked_query(query_ref[0, row * GRID_W : (row + 1) * GRID_W, cols], lane, heads_in)
                for row in range(rows_dev)
            ],
            axis=0,
        )
        scores = nt_dot(query, pair_ref[0, :, cols])
        values = jnp.concatenate([pair_ref[1, :, cols], ones], axis=1)
        for row in range(rows_dev):
            here = slice(row * stack, (row + 1) * stack)
            pieces = []
            for at in range(tok // LANES):
                offset = (LANES // GRID_W) * at - row + ROW_SPAN - 1
                bias = jnp.concatenate(
                    [bias_ref[pair * heads_in + head, offset] for head in range(heads_in)], axis=0
                )
                pieces.append(scores[here, at * LANES : (at + 1) * LANES] + bias)
            peak = pieces[0]
            for piece in pieces[1:]:
                peak = jnp.maximum(peak, piece)
            peak = jnp.max(peak, axis=1, keepdims=True)
            lifted = jnp.concatenate([jnp.exp(piece - peak).astype(BF16) for piece in pieces], axis=1)
            mixed_ref[pair, here, :] = jnp.dot(lifted, values, preferred_element_type=F32)
            peak_ref[pair, here, :] = jnp.broadcast_to(peak, (stack, LANES))


def attend_own(query, pair, bias, rows_dev):
    _, tok, channels = query.shape
    group = min(LANES, channels)
    pairs, rows = channels // group, tok * (group // HEAD_DIM)
    return call(
        partial(own_kernel, rows_dev),
        [*map(in_vmem, (query, pair, bias))],
        [VMEM] * 3,
        [
            pltpu.VMEM((pairs, rows, group + LANES), F32),
            pltpu.VMEM((pairs, rows, LANES), F32),
        ],
        cost(pairs * rows * tok * 800, bias.size * 4, pairs * rows * tok),
    )


def halo_kernel(
    rows_dev, sp, query_ref, even_ref, odd_ref, bias_ref, mixed_ref, peak_ref, out_ref, keys, values
):
    channels = query_ref.shape[2]
    group = min(LANES, channels)
    heads_in = group // HEAD_DIM
    span = HALF * GRID_W
    stack = heads_in * GRID_W
    even_slot, odd_slot = halo_slots(HALF)
    for scratch, kind in ((keys, 0), (values, 1)):
        scratch[pl.ds(even_slot, span), :] = even_ref[kind]
        scratch[pl.ds(odd_slot, span), :] = odd_ref[kind]
    lane = lax.broadcasted_iota(jnp.int32, (GRID_W, group), 1)
    ones = jnp.ones((span, LANES), BF16)
    for row in range(rows_dev):
        first = pl.multiple_of(window_at(row, rows_dev, sp) * GRID_W, GRID_W)
        here = slice(row * stack, (row + 1) * stack)
        for pair in range(channels // group):
            cols = slice(pair * group, (pair + 1) * group)
            query = stacked_query(query_ref[0, row * GRID_W : (row + 1) * GRID_W, cols], lane, heads_in)
            scores = nt_dot(query, keys[pl.ds(first, span), cols])
            pieces = []
            for at in range(span // LANES):
                bias = jnp.concatenate(
                    [bias_ref[row, pair * heads_in + head, at] for head in range(heads_in)], axis=0
                )
                pieces.append(scores[:, at * LANES : (at + 1) * LANES] + bias)
            peak = pieces[0]
            for piece in pieces[1:]:
                peak = jnp.maximum(peak, piece)
            before = peak_ref[pair, here, :]
            peak = jnp.maximum(jnp.max(peak, axis=1, keepdims=True), before)
            lifted = jnp.concatenate([jnp.exp(piece - peak).astype(BF16) for piece in pieces], axis=1)
            wide = jnp.concatenate([values[pl.ds(first, span), cols], ones], axis=1)
            mixed = jnp.dot(lifted, wide, preferred_element_type=F32)
            fade = jnp.exp(before - peak)
            top = mixed_ref[pair, here, :group] * fade[:, :group] + mixed[:, :group]
            weight = mixed_ref[pair, here, group:] * fade + mixed[:, group:]
            result, total = top[:GRID_W], weight[:GRID_W, :group]
            for head in range(1, heads_in):
                mine = lane // HEAD_DIM == head
                below = slice(head * GRID_W, (head + 1) * GRID_W)
                result = jnp.where(mine, top[below], result)
                total = jnp.where(mine, weight[below, :group], total)
            out_ref[row * GRID_W : (row + 1) * GRID_W, cols] = (result / total).astype(BF16)


def attend_halo(query, even, odd, bias, mixed, peak, rows_dev):
    _, tok, channels = query.shape
    scores = tok * (channels // HEAD_DIM) * HALF * GRID_W
    return pl.pallas_call(
        partial(halo_kernel, rows_dev, lax.axis_size("sp")),
        out_shape=pltpu.VMEM((tok, channels), BF16),
        in_specs=[VMEM] * 6,
        out_specs=VMEM,
        scratch_shapes=[pltpu.VMEM((ROW_SPAN * GRID_W, channels), BF16)] * 2,
        cost_estimate=cost(scores * HEAD_DIM * 6, bias.size * 4 + tok * channels * 16, scores),
        compiler_params=PARAMS,
        name="halo",
    )(*map(in_vmem, (query, even, odd, bias, mixed, peak)))


def attend_kernel(
    rows_dev, sp, query_ref, own_ref, even_ref, odd_ref, bias_ref, out_ref, keys, values
):
    channels = query_ref.shape[2]
    group = min(LANES, channels)
    heads_in = group // HEAD_DIM
    span = ROW_SPAN * GRID_W
    even_slot, odd_slot = halo_slots(HALF + rows_dev)
    halo = HALF * GRID_W
    for scratch, kind in ((keys, 0), (values, 1)):
        scratch[HALF * GRID_W : (HALF + rows_dev) * GRID_W, :] = own_ref[kind]
        scratch[pl.ds(even_slot, halo), :] = even_ref[kind]
        scratch[pl.ds(odd_slot, halo), :] = odd_ref[kind]
    lane = lax.broadcasted_iota(jnp.int32, (GRID_W, group), 1)
    ones = jnp.ones((span, group), BF16)
    for row in range(rows_dev):
        window = window_at(row, rows_dev, sp)
        first = pl.multiple_of(window * GRID_W, GRID_W)
        offset = window - row + HALF - 1
        for pair in range(channels // group):
            cols = slice(pair * group, (pair + 1) * group)
            query = query_ref[0, row * GRID_W : (row + 1) * GRID_W, cols]
            query = stacked_query(query, lane, heads_in)
            scores = nt_dot(query, keys[pl.ds(first, span), cols])
            pieces = []
            for at in range(span // LANES):
                bias = jnp.concatenate(
                    [
                        bias_ref[pair * heads_in + head, offset + (LANES // GRID_W) * at]
                        for head in range(heads_in)
                    ],
                    axis=0,
                )
                pieces.append(scores[:, at * LANES : (at + 1) * LANES] + bias)
            peak = pieces[0]
            for piece in pieces[1:]:
                peak = jnp.maximum(peak, piece)
            peak = jnp.max(peak, axis=1, keepdims=True)
            lifted = jnp.concatenate([jnp.exp(piece - peak).astype(BF16) for piece in pieces], axis=1)
            mixed = jnp.dot(lifted, values[pl.ds(first, span), cols], preferred_element_type=F32)
            weight = jnp.dot(lifted, ones, preferred_element_type=F32)
            mixed = mixed / weight
            result = mixed[:GRID_W]
            for head in range(1, heads_in):
                result = jnp.where(
                    lane // HEAD_DIM == head, mixed[head * GRID_W : (head + 1) * GRID_W], result
                )
            out_ref[row * GRID_W : (row + 1) * GRID_W, cols] = result.astype(BF16)


def attend(query, own, even, odd, bias, rows_dev):
    _, tok, channels = query.shape
    padded = (rows_dev + 2 * HALF) * GRID_W
    scores = tok * (channels // HEAD_DIM) * ROW_SPAN * GRID_W
    return pl.pallas_call(
        partial(attend_kernel, rows_dev, lax.axis_size("sp")),
        out_shape=pltpu.VMEM((tok, channels), BF16),
        in_specs=[VMEM] * 5,
        out_specs=VMEM,
        scratch_shapes=[pltpu.VMEM((padded, channels), BF16)] * 2,
        cost_estimate=cost(scores * HEAD_DIM * 6, bias.size * 4 + tok * channels * 16, scores),
        compiler_params=PARAMS,
        name="attend",
    )(query, own, even, odd, bias)


def exchange(block, pairs):
    sp, tp = lax.axis_size("sp"), lax.axis_size("tp")
    partner = {}
    for one, two in pairs:
        partner[one], partner[two] = two, one
    moves = []
    for row in range(sp):
        for col in range(tp):
            if row in partner:
                moves.append((row * tp + col, partner[row] * tp + col))
            elif tp % 2 == 0:
                moves.append((row * tp + col, row * tp + (col ^ 1)))
    return lax.ppermute(block, ("sp", "tp"), moves)


def flip(block, axis, bit):
    count = lax.axis_size(axis)
    return lax.ppermute(block, axis, [(at, at ^ bit) for at in range(count)])


def body(hidden_in, norm_gain, query_weight, key_weight, value_weight, output_weight, offset_bias):
    tok_dev, _ = hidden_in.shape
    rows_dev = tok_dev // GRID_W
    tp = lax.axis_size("tp")
    sp = lax.axis_size("sp")
    is_odd = lax.axis_index("sp") % 2
    split = rows_dev == HALF
    weights = [in_hbm(weight) for weight in (query_weight, key_weight, value_weight)]
    even_pairs = [(at, at + 1) for at in range(0, sp - 1, 2)]
    odd_pairs = [(at, at + 1) for at in range(1, sp - 1, 2)]
    stream = hidden_in
    lend = split and tp == 4 and lax.axis_size("grp") == 2 and len(PARTS) == LAYERS - 1
    lent = None
    near = {}
    shared = query_weight, key_weight, value_weight

    def send(cuts, layer, first, end):
        for at in range(first, end):
            near.setdefault(layer, []).append(flip(cuts[layer][at], "tp", 2))

    for layer in range(LAYERS):
        step = partial(project, layer=layer, gain=norm_gain)
        if lent:
            parts, base, held = carry
            beside = flip(stream, "tp", 1)
            across = emit_far(parts, base, near[layer - 1], side)
            corner = flip(across, "tp", 1)
            carried = step([stream, across], (0, 2), held, None, None)
            carried = step([beside], (1,), held, carried, None)
        elif tp == 4:
            across = flip(stream, "tp", 2)
            beside = flip(stream, "tp", 1)
            corner = flip(across, "tp", 1)
            *carried, held = step([stream], (0,), weights, None, None)
            carried = step([beside], (1,), held, carried, None)
            if lend:
                cuts = cut_weight(in_hbm(output_weight))
                send(cuts, layer, 0, len(cuts[layer]))
            carried = step([across], (2,), held, carried, None)
        if tp == 4:
            old = across
            (pair,) = step([corner], (3,), held, carried, (1, 2))
            (query,) = step([corner], (3,), shared if lend else held, carried, (0,))
        else:
            gathered = lax.all_gather(stream, "tp", axis=1, tiled=True)
            *carried, held = step([gathered], (None,), weights, None, (0, 1, 2))
            query, pair = carried[0][:1], carried[0][1:]
        if split:
            to_even = to_odd = pair
        else:
            low, top = pair[:, : HALF * GRID_W], pair[:, (rows_dev - HALF) * GRID_W :]
            to_even = jnp.where(is_odd == 0, top, low)
            to_odd = jnp.where(is_odd == 0, low, top)
        even = exchange(to_even, even_pairs)
        odd = exchange(to_odd, odd_pairs)
        lent = lend and layer < LAYERS - 1
        more = lend and layer < LAYERS - 2
        bias, *halo_bias = expand_bias(offset_bias, layer, rows_dev if split else 0)
        if lent:
            side = []
            for piece in near[layer]:
                side.append(flip(piece, "grp", 1))
        if split:
            mixed, peak = attend_own(query, pair, bias, rows_dev)
            attended = attend_halo(
                query, even, odd, halo_bias[0], mixed, peak, rows_dev
            )
        else:
            attended = attend(query, pair, even, odd, bias, rows_dev)
        step = partial(emit, layer=layer)
        if tp == 4:
            across = flip(attended, "tp", 2)
            beside = flip(attended, "tp", 1)
            corner = flip(across, "tp", 1)
            (partly,) = step([attended], (0,), output_weight, stream, F32, False)
            (partly,) = step([beside], (1,), output_weight, partly, F32, False)
            (partly,) = step([across], (2,), output_weight, partly, F32, False)
            if more:
                send(cuts, layer + 1, 0, len(cuts[layer + 1]))
            (stream,) = step([corner], (3,), output_weight, partly, BF16, False)
            if lent:
                carry = ([attended, beside, across, corner], old, shared)
        else:
            gathered = lax.all_gather(attended, "tp", axis=1, tiled=True)
            (stream,) = step([gathered], (None,), in_hbm(output_weight), stream, BF16, True)
    return stream


def solution(mesh):
    return jax.shard_map(
        body,
        mesh=mesh,
        in_specs=(
            P(("grp", "sp"), "tp"),
            P(),
            P(None, "tp", None),
            P(None, "tp", None),
            P(None, "tp", None),
            P(None, None, "tp"),
            P(None, "tp", None, None),
        ),
        out_specs=P(("grp", "sp"), "tp"),
        check_vma=False,
    )
```

```python
from functools import partial

import jax
import jax.numpy as jnp
from jax import lax
from jax.experimental import pallas as pl
from jax.experimental.pallas import tpu as pltpu
from jax.sharding import PartitionSpec as P


HEAD_DIM = 64
GRID_W = 64
ROW_SPAN = 8
COL_SPAN = 16
LAYERS = 3
HALF = ROW_SPAN // 2
PARTS = ((1, 2, 1), (2, 2))

EPS = 1e-06
NEG = -1e30
LANES = 128
F32 = jnp.float32
BF16 = jnp.bfloat16

PARAMS = pltpu.CompilerParams(vmem_limit_bytes=8 * 2**20)
VMEM = pl.BlockSpec(memory_space=pltpu.VMEM)
HBM = pl.BlockSpec(memory_space=pltpu.HBM)


def nt_dot(left, right):
    return lax.dot_general(left, right, (((1,), (1,)), ((), ())), preferred_element_type=F32)


def in_vmem(array):
    return pltpu.with_memory_space_constraint(array, memory_space=pltpu.VMEM)


def in_hbm(array):
    return pltpu.with_memory_space_constraint(array, memory_space=pltpu.HBM)


def cost(flops, bytes_accessed, transcendentals=0):
    return pl.CostEstimate(
        flops=int(flops), bytes_accessed=int(bytes_accessed), transcendentals=int(transcendentals)
    )


def call(kernel, operands, in_specs, out_shape, estimate, scratch=(), rider=None):
    taken, given = len(operands), len(out_shape)
    arrays, shapes, pick, count = rider or ((), (), None, 0)

    def carrying(*refs):
        ends = taken, taken + len(arrays), taken + len(arrays) + given
        last = ends[2] + len(shapes)
        copies = [
            pltpu.make_async_copy(source, target, refs[-1].at[at])
            for at, (source, target) in enumerate(
                pick(refs[ends[0] : ends[1]], refs[ends[2] : last])
            )
        ]
        for copy in copies:
            copy.start()
        kernel(*refs[: ends[0]], *refs[ends[1] : ends[2]], *refs[last:-1])
        for copy in copies:
            copy.wait()

    sems = [pltpu.SemaphoreType.DMA((count,))] if rider else []
    return pl.pallas_call(
        carrying if rider else kernel,
        out_shape=[*out_shape, *(pltpu.VMEM(shape, BF16) for shape in shapes)],
        in_specs=[*in_specs, *[HBM] * len(arrays)],
        out_specs=[VMEM] * (given + len(shapes)),
        scratch_shapes=[*scratch, *sems],
        cost_estimate=estimate,
        compiler_params=PARAMS,
    )(*operands, *arrays)


def block_at(bit, width, unit, sub=0, subs=1):
    if bit is None:
        return slice(None)
    first = (lax.axis_index("tp") ^ bit) * (width * subs) + sub * width
    return pl.ds(pl.multiple_of(first, unit), width)


def window_at(row, rows_dev, sp):
    first_row = lax.axis_index("sp") * rows_dev
    first = jnp.minimum(jnp.maximum(first_row + row - HALF, 0), rows_dev * sp - ROW_SPAN)
    return first - first_row + HALF


def halo_slots(high):
    odd = lax.axis_index("sp") % 2
    return (
        pl.multiple_of((1 - odd) * (high * GRID_W), GRID_W),
        pl.multiple_of(odd * (high * GRID_W), GRID_W),
    )


def project_kernel(bits, load, shared, first, kinds, layer, *refs):
    sources, refs = refs[: len(bits)], refs[len(bits) :]
    gain_ref, refs = refs[0], refs[1:]
    if load:
        stored, refs = refs[:3], refs[3:]
        *refs, held_ref, sems = refs
        copies = [
            pltpu.make_async_copy(stored[kind].at[layer], held_ref.at[kind], sems.at[kind])
            for kind in range(3)
        ]
        for copy in copies:
            copy.start()
    elif shared:
        stored, refs = refs[:3], refs[3:]
    else:
        held_ref, refs = refs[0], refs[1:]
    if not first:
        (acc_in, sq_in), refs = refs[:2], refs[2:]
    full = gain_ref.shape[1]
    totals = [None, None, None]
    squares = None
    for at, bit in enumerate(bits):
        wide = sources[at][...].astype(F32)
        width = wide.shape[1]
        cols = block_at(bit, width, LANES)
        square = jnp.sum(wide * wide, axis=1, keepdims=True)
        squares = square if squares is None else squares + square
        scaled = (wide * gain_ref[layer : layer + 1, cols]).astype(BF16)
        for kind in kinds or range(3):
            if load and at == 0:
                copies[kind].wait()
            held = stored[kind][layer, :, cols] if shared else held_ref[kind, :, cols]
            product = nt_dot(scaled, held)
            totals[kind] = product if totals[kind] is None else totals[kind] + product
    if not first:
        squares = squares + sq_in[:, :1]
        for kind in kinds or range(3):
            totals[kind] = totals[kind] + acc_in[kind]
    if kinds:
        row_scale = lax.rsqrt(squares * (1.0 / full) + EPS)
        for at, kind in enumerate(kinds):
            scale = row_scale * HEAD_DIM ** (-0.5) if kind == 0 else row_scale
            made = (totals[kind] * scale).astype(BF16)
            for group, out_ref in enumerate(refs):
                width = out_ref.shape[2]
                out_ref[at] = made[:, group * width : (group + 1) * width]
    else:
        acc_out, sq_out = refs
        for kind in range(3):
            acc_out[kind] = totals[kind]
        sq_out[...] = jnp.broadcast_to(squares, sq_out.shape)


def project(parts, bits, weights, carried, kinds, layer, gain, groups=1):
    tok, width = parts[0].shape
    parts_n = len(parts)
    first = carried is None
    operands = [*parts, gain]
    specs = [VMEM] * (parts_n + 1)
    load, shared = isinstance(weights, list), isinstance(weights, tuple)
    if load:
        _, channels, full = weights[0].shape
        operands += weights
        specs += [HBM] * 3
    elif shared:
        _, channels, full = weights[0].shape
        operands += weights
        specs += [VMEM] * 3
    else:
        _, channels, full = weights.shape
        operands.append(in_vmem(weights))
        specs.append(VMEM)
    if not first:
        operands += map(in_vmem, carried)
        specs += [VMEM] * 2
    if kinds:
        out_shape = [pltpu.VMEM((len(kinds), tok, channels // groups), BF16)] * groups
    else:
        out_shape = [pltpu.VMEM((3, tok, channels), F32), pltpu.VMEM((tok, LANES), F32)]
    scratch = []
    if load:
        out_shape.append(pltpu.VMEM((3, channels, full), BF16))
        scratch.append(pltpu.SemaphoreType.DMA((3,)))
    flops = 2 * tok * width * channels * len(kinds or range(3)) * parts_n
    return call(
        partial(project_kernel, bits, load, shared, first, kinds, layer),
        operands,
        specs,
        out_shape,
        cost(flops, parts_n * width * (channels * 6 + tok * 2) + 4 * tok * channels),
        scratch,
    )


def emit_kernel(bits, load, layer, sub, subs, *refs):
    sources, refs = refs[: len(bits)], refs[len(bits) :]
    held_ref, base_ref, out_ref, *rest = refs
    if load:
        stored_ref, (held_ref, sem) = held_ref, rest
        copy = pltpu.make_async_copy(stored_ref.at[layer], held_ref, sem)
        copy.start()
    total = base_ref[...].astype(F32)
    if load:
        copy.wait()
    for at, bit in enumerate(bits):
        rows = block_at(bit, sources[at].shape[1], HEAD_DIM, sub, subs)
        held = held_ref[rows, :] if load else held_ref[layer, rows, :]
        total = total + jnp.dot(sources[at][...], held, preferred_element_type=F32)
    out_ref[...] = total.astype(out_ref.dtype)


def emit(parts, bits, weight, base, out_type, load, layer, sub=0, subs=1):
    tok, width = parts[0].shape
    cols = base.shape[1]
    out_shape = [pltpu.VMEM((tok, cols), out_type)]
    if out_type == BF16 and layer == LAYERS - 1:
        out_shape = [jax.ShapeDtypeStruct((tok, cols), out_type)]
    scratch = []
    if load:
        scratch = [pltpu.VMEM(weight.shape[1:], BF16), pltpu.SemaphoreType.DMA]
    return call(
        partial(emit_kernel, bits, load, layer, sub, subs),
        [*parts, weight, base],
        [VMEM] * len(parts) + [HBM if load else VMEM, VMEM],
        out_shape,
        cost(2 * tok * width * cols * len(bits), 10**6),
        scratch,
    )


def cut_weight(weight):
    _, rows, cols = weight.shape
    half = rows // 2
    slabs = []
    for layer, parts in enumerate(PARTS):
        unit = cols // sum(parts)
        for at, part in enumerate(parts):
            slabs.append((layer, unit * sum(parts[:at]), unit * part))

    def pick(sources, targets):
        here = pl.ds(pl.multiple_of(lax.axis_index("grp") * half, half), half)
        return [
            (sources[0].at[layer, here, pl.ds(first, width)], target)
            for (layer, first, width), target in zip(slabs, targets)
        ]

    shapes = [(half, width) for _, _, width in slabs]
    rider = [weight], shapes, pick, len(slabs)
    cuts = call(lambda *refs: None, [], [], [], cost(10**6, 10**6), rider=rider)
    return [
        [cut for cut, slab in zip(cuts, slabs) if slab[0] == layer] for layer in range(len(PARTS))
    ]


def far_kernel(pieces, own_ref, beside_ref, across_ref, corner_ref, base_ref, *refs):
    near, side, out_ref = refs[:pieces], refs[pieces:-1], refs[-1]
    me = lax.axis_index("tp")
    even = me % 2 == 0
    aligned = me // 2 == lax.axis_index("grp")
    own, beside, across, corner = own_ref[...], beside_ref[...], across_ref[...], corner_ref[...]
    mine = jnp.concatenate([jnp.where(even, own, beside), jnp.where(even, beside, own)], axis=1)
    other = jnp.concatenate(
        [jnp.where(even, across, corner), jnp.where(even, corner, across)], axis=1
    )
    with_near = jnp.where(aligned, mine, other)
    with_side = jnp.where(aligned, other, mine)
    done = 0
    for at in range(pieces):
        cols = slice(done, done + near[at].shape[1])
        done = cols.stop
        total = base_ref[:, cols].astype(F32)
        total = total + jnp.dot(with_near, near[at][...], preferred_element_type=F32)
        total = total + jnp.dot(with_side, side[at][...], preferred_element_type=F32)
        out_ref[:, cols] = total.astype(BF16)


def emit_far(parts, base, near, side):
    tok, cols = base.shape
    operands = [*parts, base, *near, *side]
    return pl.pallas_call(
        partial(far_kernel, len(near)),
        out_shape=pltpu.VMEM((tok, cols), BF16),
        in_specs=[VMEM] * len(operands),
        out_specs=VMEM,
        cost_estimate=cost(2 * tok * cols * 4 * parts[0].shape[1], 10**6),
        compiler_params=PARAMS,
        name="lent",
    )(*map(in_vmem, operands))


def bias_kernel(layer, sp, table_ref, out_ref, *refs):
    *halo_refs, rows_ref = refs
    heads_n, spans = out_ref.shape[:2]
    offsets, cols = table_ref.shape[2:]
    rows_ref[...] = jnp.zeros_like(rows_ref)
    for head in range(heads_n):
        rows_ref[head, :offsets, :cols] = table_ref[layer, head]
    shape = (GRID_W, LANES)
    query_col = lax.broadcasted_iota(jnp.int32, shape, 0)
    lane = lax.broadcasted_iota(jnp.int32, shape, 1)
    key_col = lane % GRID_W
    first_col = jnp.clip(query_col - COL_SPAN // 2, 0, GRID_W - COL_SPAN)
    inside = (key_col >= first_col) & (key_col < first_col + COL_SPAN)
    for head in range(heads_n):
        plain = rows_ref[head]
        after = pltpu.roll(pltpu.roll(plain, GRID_W, axis=1), rows_ref.shape[1] - 1, axis=0)
        at_lane = lax.broadcasted_iota(jnp.int32, plain.shape, 1)
        both = jnp.where(at_lane < GRID_W, plain, after)
        for span in range(spans):
            row = jnp.broadcast_to(both[span : span + 1, :], shape)
            turned = pltpu.roll(row, LANES - (COL_SPAN - 1), axis=1, stride=1, stride_axis=0)
            out_ref[head, span] = jnp.where(inside, turned, NEG)
    for halo_ref in halo_refs:
        for row in range(halo_ref.shape[0]):
            for at in range(halo_ref.shape[2]):
                one = window_at(row, halo_ref.shape[0], sp) + 2 * at
                low = one + jnp.where(one < HALF, HALF - 1, ROW_SPAN - 1) - row
                high = one + jnp.where(one + 1 < HALF, HALF - 1, ROW_SPAN - 1) - row
                for head in range(heads_n):
                    halo_ref[row, head, at] = jnp.where(
                        lane < GRID_W, out_ref[head, low], out_ref[head, high]
                    )


def expand_bias(table, layer, halo_rows):
    _, heads_n, offsets, _ = table.shape
    spans = offsets - 1
    out_shape = [pltpu.VMEM((heads_n, spans, GRID_W, LANES), F32)]
    if halo_rows:
        out_shape.append(pltpu.VMEM((halo_rows, heads_n, HALF // 2, GRID_W, LANES), F32))
    return call(
        partial(bias_kernel, layer, lax.axis_size("sp")),
        [table],
        [VMEM],
        out_shape,
        cost(heads_n * spans * GRID_W * LANES * 40, heads_n * spans * GRID_W * LANES * 4),
        [pltpu.VMEM((heads_n, 2 * ROW_SPAN, LANES), F32)],
    )


def stacked_query(query, lane, heads_in):
    if heads_in == 1:
        return query
    zero = jnp.zeros_like(query)
    return jnp.concatenate(
        [jnp.where(lane // HEAD_DIM == head, query, zero) for head in range(heads_in)], axis=0
    )


def own_kernel(rows_dev, head0, query_ref, pair_ref, bias_ref, mixed_ref, peak_ref):
    channels = query_ref.shape[2]
    group = min(LANES, channels)
    heads_in = group // HEAD_DIM
    tok = rows_dev * GRID_W
    stack = heads_in * GRID_W
    lane = lax.broadcasted_iota(jnp.int32, (GRID_W, group), 1)
    ones = jnp.ones((tok, LANES), BF16)
    for pair in range(channels // group):
        cols = slice(pair * group, (pair + 1) * group)
        query = jnp.concatenate(
            [
                stacked_query(query_ref[0, row * GRID_W : (row + 1) * GRID_W, cols], lane, heads_in)
                for row in range(rows_dev)
            ],
            axis=0,
        )
        scores = nt_dot(query, pair_ref[0, :, cols])
        values = jnp.concatenate([pair_ref[1, :, cols], ones], axis=1)
        for row in range(rows_dev):
            here = slice(row * stack, (row + 1) * stack)
            pieces = []
            for at in range(tok // LANES):
                offset = (LANES // GRID_W) * at - row + ROW_SPAN - 1
                bias = jnp.concatenate(
                    [bias_ref[head0 + pair * heads_in + head, offset] for head in range(heads_in)],
                    axis=0,
                )
                pieces.append(scores[here, at * LANES : (at + 1) * LANES] + bias)
            peak = pieces[0]
            for piece in pieces[1:]:
                peak = jnp.maximum(peak, piece)
            peak = jnp.max(peak, axis=1, keepdims=True)
            lifted = jnp.concatenate([jnp.exp(piece - peak).astype(BF16) for piece in pieces], axis=1)
            mixed_ref[pair, here, :] = jnp.dot(lifted, values, preferred_element_type=F32)
            peak_ref[pair, here, :] = jnp.broadcast_to(peak, (stack, LANES))


def attend_own(query, pair, bias, rows_dev, head0=0):
    _, tok, channels = query.shape
    group = min(LANES, channels)
    pairs, rows = channels // group, tok * (group // HEAD_DIM)
    return call(
        partial(own_kernel, rows_dev, head0),
        [*map(in_vmem, (query, pair, bias))],
        [VMEM] * 3,
        [
            pltpu.VMEM((pairs, rows, group + LANES), F32),
            pltpu.VMEM((pairs, rows, LANES), F32),
        ],
        cost(pairs * rows * tok * 800, bias.size * 4, pairs * rows * tok),
    )


def halo_kernel(
    rows_dev, sp, head0, query_ref, even_ref, odd_ref, bias_ref, mixed_ref, peak_ref, out_ref, keys, values
):
    channels = query_ref.shape[2]
    group = min(LANES, channels)
    heads_in = group // HEAD_DIM
    span = HALF * GRID_W
    stack = heads_in * GRID_W
    even_slot, odd_slot = halo_slots(HALF)
    for scratch, kind in ((keys, 0), (values, 1)):
        scratch[pl.ds(even_slot, span), :] = even_ref[kind]
        scratch[pl.ds(odd_slot, span), :] = odd_ref[kind]
    lane = lax.broadcasted_iota(jnp.int32, (GRID_W, group), 1)
    ones = jnp.ones((span, LANES), BF16)
    for row in range(rows_dev):
        first = pl.multiple_of(window_at(row, rows_dev, sp) * GRID_W, GRID_W)
        here = slice(row * stack, (row + 1) * stack)
        for pair in range(channels // group):
            cols = slice(pair * group, (pair + 1) * group)
            query = stacked_query(query_ref[0, row * GRID_W : (row + 1) * GRID_W, cols], lane, heads_in)
            scores = nt_dot(query, keys[pl.ds(first, span), cols])
            pieces = []
            for at in range(span // LANES):
                bias = jnp.concatenate(
                    [bias_ref[row, head0 + pair * heads_in + head, at] for head in range(heads_in)],
                    axis=0,
                )
                pieces.append(scores[:, at * LANES : (at + 1) * LANES] + bias)
            peak = pieces[0]
            for piece in pieces[1:]:
                peak = jnp.maximum(peak, piece)
            before = peak_ref[pair, here, :]
            peak = jnp.maximum(jnp.max(peak, axis=1, keepdims=True), before)
            lifted = jnp.concatenate([jnp.exp(piece - peak).astype(BF16) for piece in pieces], axis=1)
            wide = jnp.concatenate([values[pl.ds(first, span), cols], ones], axis=1)
            mixed = jnp.dot(lifted, wide, preferred_element_type=F32)
            fade = jnp.exp(before - peak)
            top = mixed_ref[pair, here, :group] * fade[:, :group] + mixed[:, :group]
            weight = mixed_ref[pair, here, group:] * fade + mixed[:, group:]
            result, total = top[:GRID_W], weight[:GRID_W, :group]
            for head in range(1, heads_in):
                mine = lane // HEAD_DIM == head
                below = slice(head * GRID_W, (head + 1) * GRID_W)
                result = jnp.where(mine, top[below], result)
                total = jnp.where(mine, weight[below, :group], total)
            out_ref[row * GRID_W : (row + 1) * GRID_W, cols] = (result / total).astype(BF16)


def attend_halo(query, even, odd, bias, mixed, peak, rows_dev, head0=0):
    _, tok, channels = query.shape
    scores = tok * (channels // HEAD_DIM) * HALF * GRID_W
    return pl.pallas_call(
        partial(halo_kernel, rows_dev, lax.axis_size("sp"), head0),
        out_shape=pltpu.VMEM((tok, channels), BF16),
        in_specs=[VMEM] * 6,
        out_specs=VMEM,
        scratch_shapes=[pltpu.VMEM((ROW_SPAN * GRID_W, channels), BF16)] * 2,
        cost_estimate=cost(scores * HEAD_DIM * 6, bias.size * 4 + tok * channels * 16, scores),
        compiler_params=PARAMS,
        name="halo",
    )(*map(in_vmem, (query, even, odd, bias, mixed, peak)))


def attend_kernel(
    rows_dev, sp, query_ref, own_ref, even_ref, odd_ref, bias_ref, out_ref, keys, values
):
    channels = query_ref.shape[2]
    group = min(LANES, channels)
    heads_in = group // HEAD_DIM
    span = ROW_SPAN * GRID_W
    even_slot, odd_slot = halo_slots(HALF + rows_dev)
    halo = HALF * GRID_W
    for scratch, kind in ((keys, 0), (values, 1)):
        scratch[HALF * GRID_W : (HALF + rows_dev) * GRID_W, :] = own_ref[kind]
        scratch[pl.ds(even_slot, halo), :] = even_ref[kind]
        scratch[pl.ds(odd_slot, halo), :] = odd_ref[kind]
    lane = lax.broadcasted_iota(jnp.int32, (GRID_W, group), 1)
    ones = jnp.ones((span, group), BF16)
    for row in range(rows_dev):
        window = window_at(row, rows_dev, sp)
        first = pl.multiple_of(window * GRID_W, GRID_W)
        offset = window - row + HALF - 1
        for pair in range(channels // group):
            cols = slice(pair * group, (pair + 1) * group)
            query = query_ref[0, row * GRID_W : (row + 1) * GRID_W, cols]
            query = stacked_query(query, lane, heads_in)
            scores = nt_dot(query, keys[pl.ds(first, span), cols])
            pieces = []
            for at in range(span // LANES):
                bias = jnp.concatenate(
                    [
                        bias_ref[pair * heads_in + head, offset + (LANES // GRID_W) * at]
                        for head in range(heads_in)
                    ],
                    axis=0,
                )
                pieces.append(scores[:, at * LANES : (at + 1) * LANES] + bias)
            peak = pieces[0]
            for piece in pieces[1:]:
                peak = jnp.maximum(peak, piece)
            peak = jnp.max(peak, axis=1, keepdims=True)
            lifted = jnp.concatenate([jnp.exp(piece - peak).astype(BF16) for piece in pieces], axis=1)
            mixed = jnp.dot(lifted, values[pl.ds(first, span), cols], preferred_element_type=F32)
            weight = jnp.dot(lifted, ones, preferred_element_type=F32)
            mixed = mixed / weight
            result = mixed[:GRID_W]
            for head in range(1, heads_in):
                result = jnp.where(
                    lane // HEAD_DIM == head, mixed[head * GRID_W : (head + 1) * GRID_W], result
                )
            out_ref[row * GRID_W : (row + 1) * GRID_W, cols] = result.astype(BF16)


def attend(query, own, even, odd, bias, rows_dev):
    _, tok, channels = query.shape
    padded = (rows_dev + 2 * HALF) * GRID_W
    scores = tok * (channels // HEAD_DIM) * ROW_SPAN * GRID_W
    return pl.pallas_call(
        partial(attend_kernel, rows_dev, lax.axis_size("sp")),
        out_shape=pltpu.VMEM((tok, channels), BF16),
        in_specs=[VMEM] * 5,
        out_specs=VMEM,
        scratch_shapes=[pltpu.VMEM((padded, channels), BF16)] * 2,
        cost_estimate=cost(scores * HEAD_DIM * 6, bias.size * 4 + tok * channels * 16, scores),
        compiler_params=PARAMS,
        name="attend",
    )(query, own, even, odd, bias)


def exchange(block, pairs):
    sp, tp = lax.axis_size("sp"), lax.axis_size("tp")
    partner = {}
    for one, two in pairs:
        partner[one], partner[two] = two, one
    moves = []
    for row in range(sp):
        for col in range(tp):
            if row in partner:
                moves.append((row * tp + col, partner[row] * tp + col))
            elif tp % 2 == 0:
                moves.append((row * tp + col, row * tp + (col ^ 1)))
    return lax.ppermute(block, ("sp", "tp"), moves)


def flip(block, axis, bit):
    count = lax.axis_size(axis)
    return lax.ppermute(block, axis, [(at, at ^ bit) for at in range(count)])


def body(hidden_in, norm_gain, query_weight, key_weight, value_weight, output_weight, offset_bias):
    tok_dev, _ = hidden_in.shape
    rows_dev = tok_dev // GRID_W
    tp = lax.axis_size("tp")
    sp = lax.axis_size("sp")
    is_odd = lax.axis_index("sp") % 2
    split = rows_dev == HALF
    weights = [in_hbm(weight) for weight in (query_weight, key_weight, value_weight)]
    even_pairs = [(at, at + 1) for at in range(0, sp - 1, 2)]
    odd_pairs = [(at, at + 1) for at in range(1, sp - 1, 2)]
    stream = hidden_in
    lend = split and tp == 4 and lax.axis_size("grp") == 2 and len(PARTS) == LAYERS - 1
    lent = None
    near = {}
    shared = query_weight, key_weight, value_weight

    def send(cuts, layer, first, end):
        for at in range(first, end):
            near.setdefault(layer, []).append(flip(cuts[layer][at], "tp", 2))

    for layer in range(LAYERS):
        step = partial(project, layer=layer, gain=norm_gain)
        if lent:
            parts, base, held = carry
            beside = flip(stream, "tp", 1)
            across = emit_far(parts, base, near[layer - 1], side)
            corner = flip(across, "tp", 1)
            carried = step([stream, across], (0, 2), held, None, None)
            carried = step([beside], (1,), held, carried, None)
        elif tp == 4:
            across = flip(stream, "tp", 2)
            beside = flip(stream, "tp", 1)
            corner = flip(across, "tp", 1)
            *carried, held = step([stream], (0,), weights, None, None)
            carried = step([beside], (1,), held, carried, None)
            if lend:
                cuts = cut_weight(in_hbm(output_weight))
                send(cuts, layer, 0, len(cuts[layer]))
            carried = step([across], (2,), held, carried, None)
        groups = query_weight.shape[1] // LANES
        if lend and layer == LAYERS - 1 and groups == 2:
            pairs, queries, swaps, attended = [], [], [], []
            pairs = step([corner], (3,), held, carried, (1, 2), groups=groups)
            queries = step([corner], (3,), held, carried, (0,), groups=groups)
            for pair in pairs:
                swaps.append(exchange(pair, even_pairs))
                swaps.append(exchange(pair, odd_pairs))
            bias, halo_bias = expand_bias(offset_bias, layer, rows_dev)
            beside, across, corner = [], [], []
            for group in range(groups):
                head0 = group * (LANES // HEAD_DIM)
                mixed, peak = attend_own(queries[group], pairs[group], bias, rows_dev, head0)
                halo = swaps[2 * group : 2 * group + 2]
                done = attend_halo(queries[group], *halo, halo_bias, mixed, peak, rows_dev, head0)
                attended.append(done)
                across.append(flip(done, "tp", 2))
                beside.append(flip(done, "tp", 1))
                corner.append(flip(across[-1], "tp", 1))
            turns = [(attended, 0), (beside, 1), (across, 2), (corner, 3)]
            for group in range(groups):
                for part, bit in turns:
                    final = group == groups - 1 and bit == 3
                    (stream,) = emit(
                        [part[group]],
                        (bit,),
                        output_weight,
                        stream,
                        BF16 if final else F32,
                        False,
                        layer,
                        group,
                        groups,
                    )
            return stream
        if tp == 4:
            old = across
            (pair,) = step([corner], (3,), held, carried, (1, 2))
            (query,) = step([corner], (3,), shared if lend else held, carried, (0,))
        else:
            gathered = lax.all_gather(stream, "tp", axis=1, tiled=True)
            *carried, held = step([gathered], (None,), weights, None, (0, 1, 2))
            query, pair = carried[0][:1], carried[0][1:]
        if split:
            to_even = to_odd = pair
        else:
            low, top = pair[:, : HALF * GRID_W], pair[:, (rows_dev - HALF) * GRID_W :]
            to_even = jnp.where(is_odd == 0, top, low)
            to_odd = jnp.where(is_odd == 0, low, top)
        even = exchange(to_even, even_pairs)
        odd = exchange(to_odd, odd_pairs)
        lent = lend and layer < LAYERS - 1
        more = lend and layer < LAYERS - 2
        bias, *halo_bias = expand_bias(offset_bias, layer, rows_dev if split else 0)
        if lent:
            side = []
            for piece in near[layer]:
                side.append(flip(piece, "grp", 1))
        if split:
            mixed, peak = attend_own(query, pair, bias, rows_dev)
            attended = attend_halo(
                query, even, odd, halo_bias[0], mixed, peak, rows_dev
            )
        else:
            attended = attend(query, pair, even, odd, bias, rows_dev)
        step = partial(emit, layer=layer)
        if tp == 4:
            across = flip(attended, "tp", 2)
            beside = flip(attended, "tp", 1)
            corner = flip(across, "tp", 1)
            (partly,) = step([attended], (0,), output_weight, stream, F32, False)
            (partly,) = step([beside], (1,), output_weight, partly, F32, False)
            (partly,) = step([across], (2,), output_weight, partly, F32, False)
            if more:
                send(cuts, layer + 1, 0, len(cuts[layer + 1]))
            (stream,) = step([corner], (3,), output_weight, partly, BF16, False)
            if lent:
                carry = ([attended, beside, across, corner], old, shared)
        else:
            gathered = lax.all_gather(attended, "tp", axis=1, tiled=True)
            (stream,) = step([gathered], (None,), in_hbm(output_weight), stream, BF16, True)
    return stream


def solution(mesh):
    return jax.shard_map(
        body,
        mesh=mesh,
        in_specs=(
            P(("grp", "sp"), "tp"),
            P(),
            P(None, "tp", None),
            P(None, "tp", None),
            P(None, "tp", None),
            P(None, None, "tp"),
            P(None, "tp", None, None),
        ),
        out_specs=P(("grp", "sp"), "tp"),
        check_vma=False,
    )
```

```python
from functools import partial

import jax
import jax.numpy as jnp
from jax import lax
from jax.experimental import pallas as pl
from jax.experimental.pallas import tpu as pltpu
from jax.sharding import PartitionSpec as P


HEAD_DIM = 64
GRID_W = 64
ROW_SPAN = 8
COL_SPAN = 16
LAYERS = 3
HALF = ROW_SPAN // 2
PARTS = ((2, 1, 1), (2, 2))

EPS = 1e-06
NEG = -1e30
LANES = 128
F32 = jnp.float32
BF16 = jnp.bfloat16

PARAMS = pltpu.CompilerParams(vmem_limit_bytes=8 * 2**20)
VMEM = pl.BlockSpec(memory_space=pltpu.VMEM)
HBM = pl.BlockSpec(memory_space=pltpu.HBM)


def nt_dot(left, right):
    return lax.dot_general(left, right, (((1,), (1,)), ((), ())), preferred_element_type=F32)


def in_vmem(array):
    return pltpu.with_memory_space_constraint(array, memory_space=pltpu.VMEM)


def in_hbm(array):
    return pltpu.with_memory_space_constraint(array, memory_space=pltpu.HBM)


def cost(flops, bytes_accessed, transcendentals=0):
    return pl.CostEstimate(
        flops=int(flops), bytes_accessed=int(bytes_accessed), transcendentals=int(transcendentals)
    )


def block_at(bit, width, unit):
    if bit is None:
        return slice(None)
    return pl.ds(pl.multiple_of((lax.axis_index("tp") ^ bit) * width, unit), width)


def window_at(row, rows_dev, sp):
    first_row = lax.axis_index("sp") * rows_dev
    first = jnp.minimum(jnp.maximum(first_row + row - HALF, 0), rows_dev * sp - ROW_SPAN)
    return first - first_row + HALF


def halo_slots(high):
    odd = lax.axis_index("sp") % 2
    return (
        pl.multiple_of((1 - odd) * (high * GRID_W), GRID_W),
        pl.multiple_of(odd * (high * GRID_W), GRID_W),
    )


def project_kernel(bits, load, first, kinds, layer, *refs):
    sources, refs = refs[: len(bits)], refs[len(bits) :]
    gain_ref, refs = refs[0], refs[1:]
    if load:
        stored, refs = refs[:3], refs[3:]
        *refs, held_ref, sems = refs
        copies = [
            pltpu.make_async_copy(stored[kind].at[layer], held_ref.at[kind], sems.at[kind])
            for kind in range(3)
        ]
        for copy in copies:
            copy.start()
    else:
        held_ref, refs = refs[0], refs[1:]
    if not first:
        (acc_in, sq_in), refs = refs[:2], refs[2:]
    full = gain_ref.shape[1]
    totals = [None, None, None]
    squares = None
    for at, bit in enumerate(bits):
        wide = sources[at][...].astype(F32)
        width = wide.shape[1]
        cols = block_at(bit, width, LANES)
        square = jnp.sum(wide * wide, axis=1, keepdims=True)
        squares = square if squares is None else squares + square
        scaled = (wide * gain_ref[layer : layer + 1, cols]).astype(BF16)
        for kind in kinds or range(3):
            if load and at == 0:
                copies[kind].wait()
            product = nt_dot(scaled, held_ref[kind, :, cols])
            totals[kind] = product if totals[kind] is None else totals[kind] + product
    if not first:
        squares = squares + sq_in[:, :1]
        for kind in kinds or range(3):
            totals[kind] = totals[kind] + acc_in[kind]
    if kinds:
        row_scale = lax.rsqrt(squares * (1.0 / full) + EPS)
        for at, kind in enumerate(kinds):
            scale = row_scale * HEAD_DIM ** (-0.5) if kind == 0 else row_scale
            refs[0][at] = (totals[kind] * scale).astype(BF16)
    else:
        acc_out, sq_out = refs
        for kind in range(3):
            acc_out[kind] = totals[kind]
        sq_out[...] = jnp.broadcast_to(squares, sq_out.shape)


def project(parts, bits, weights, carried, kinds, layer, gain):
    tok, width = parts[0].shape
    parts_n = len(parts)
    first = carried is None
    operands = [*parts, gain]
    specs = [VMEM] * (parts_n + 1)
    load = isinstance(weights, list)
    if load:
        _, channels, full = weights[0].shape
        operands += weights
        specs += [HBM] * 3
    else:
        _, channels, full = weights.shape
        operands.append(in_vmem(weights))
        specs.append(VMEM)
    if not first:
        operands += map(in_vmem, carried)
        specs += [VMEM] * 2
    if kinds:
        out_shape = [pltpu.VMEM((len(kinds), tok, channels), BF16)]
    else:
        out_shape = [pltpu.VMEM((3, tok, channels), F32), pltpu.VMEM((tok, LANES), F32)]
    scratch = []
    if load:
        out_shape.append(pltpu.VMEM((3, channels, full), BF16))
        scratch.append(pltpu.SemaphoreType.DMA((3,)))
    flops = 2 * tok * width * channels * len(kinds or range(3)) * parts_n
    return pl.pallas_call(
        partial(project_kernel, bits, load, first, kinds, layer),
        out_shape=out_shape,
        in_specs=specs,
        out_specs=[VMEM] * len(out_shape),
        scratch_shapes=scratch,
        cost_estimate=cost(flops, parts_n * width * (channels * 6 + tok * 2) + 4 * tok * channels),
        compiler_params=PARAMS,
        name="project",
    )(*operands)


def emit_kernel(bits, first, layer, *refs):
    sources, refs = refs[: len(bits)], refs[len(bits) :]
    if first:
        stored_ref, base_ref, out_ref, held_ref, sem = refs
        copy = pltpu.make_async_copy(stored_ref.at[layer], held_ref, sem)
        copy.start()
    else:
        held_ref, base_ref, out_ref = refs
    total = base_ref[...].astype(F32)
    if first:
        copy.wait()
    for at, bit in enumerate(bits):
        rows = block_at(bit, sources[at].shape[1], HEAD_DIM)
        total = total + jnp.dot(sources[at][...], held_ref[rows, :], preferred_element_type=F32)
    out_ref[...] = total.astype(out_ref.dtype)


def emit(parts, bits, weight, base, out_type, first, layer):
    tok, width = parts[0].shape
    cols = base.shape[1]
    parts_n = len(parts)
    out_shape = [pltpu.VMEM((tok, cols), out_type)]
    if out_type == BF16 and layer == LAYERS - 1:
        out_shape = [jax.ShapeDtypeStruct((tok, cols), out_type)]
    scratch = []
    if first:
        out_shape.append(pltpu.VMEM(weight.shape[1:], BF16))
        scratch.append(pltpu.SemaphoreType.DMA)
    return pl.pallas_call(
        partial(emit_kernel, bits, first, layer),
        out_shape=out_shape,
        in_specs=[VMEM] * parts_n + [HBM if first else VMEM, VMEM],
        out_specs=[VMEM] * len(out_shape),
        scratch_shapes=scratch,
        cost_estimate=cost(
            2 * tok * width * cols * parts_n, parts_n * width * (cols + tok) * 2 + tok * cols * 6
        ),
        compiler_params=PARAMS,
        name="emit",
    )(*parts, weight if first else in_vmem(weight), base if first else in_vmem(base))


def fetch_kernel(pick, count, *refs):
    sources, targets, sems = refs[:count], refs[count:-1], refs[-1]
    copies = [
        pltpu.make_async_copy(source, target, sems.at[at])
        for at, (source, target) in enumerate(pick(sources, targets))
    ]
    for copy in copies:
        copy.start()
    for copy in copies:
        copy.wait()


def fetch(arrays, shapes, pick, copies):
    return pl.pallas_call(
        partial(fetch_kernel, pick, len(arrays)),
        out_shape=[pltpu.VMEM(shape, BF16) for shape in shapes],
        in_specs=[HBM] * len(arrays),
        out_specs=[VMEM] * len(shapes),
        scratch_shapes=[pltpu.SemaphoreType.DMA((copies,))],
        cost_estimate=cost(10**6, 10**6),
        compiler_params=PARAMS,
    )(*arrays)


def cut_weight(weight):
    _, rows, cols = weight.shape
    half, unit = rows // 2, cols // 4
    slabs = []
    for layer, parts in enumerate(PARTS):
        first = 0
        for part in parts:
            slabs.append((layer, first * unit, part * unit))
            first += part

    def pick(sources, targets):
        here = pl.ds(pl.multiple_of(lax.axis_index("grp") * half, half), half)
        return [
            (sources[0].at[layer, here, pl.ds(first, width)], target)
            for (layer, first, width), target in zip(slabs, targets)
        ]

    cuts = fetch([weight], [(half, width) for _, _, width in slabs], pick, len(slabs))
    return [
        [cut for cut, slab in zip(cuts, slabs) if slab[0] == layer] for layer in range(len(PARTS))
    ]


def far_kernel(pieces, own_ref, beside_ref, across_ref, corner_ref, base_ref, *refs):
    near, side, out_ref = refs[:pieces], refs[pieces:-1], refs[-1]
    me = lax.axis_index("tp")
    even = me % 2 == 0
    aligned = me // 2 == lax.axis_index("grp")
    own, beside, across, corner = own_ref[...], beside_ref[...], across_ref[...], corner_ref[...]
    mine = jnp.concatenate([jnp.where(even, own, beside), jnp.where(even, beside, own)], axis=1)
    other = jnp.concatenate(
        [jnp.where(even, across, corner), jnp.where(even, corner, across)], axis=1
    )
    with_near = jnp.where(aligned, mine, other)
    with_side = jnp.where(aligned, other, mine)
    done = 0
    for at in range(pieces):
        cols = slice(done, done + near[at].shape[1])
        done = cols.stop
        total = base_ref[:, cols].astype(F32)
        total = total + jnp.dot(with_near, near[at][...], preferred_element_type=F32)
        total = total + jnp.dot(with_side, side[at][...], preferred_element_type=F32)
        out_ref[:, cols] = total.astype(BF16)


def emit_far(parts, base, near, side):
    tok, cols = base.shape
    operands = [*parts, base, *near, *side]
    return pl.pallas_call(
        partial(far_kernel, len(near)),
        out_shape=pltpu.VMEM((tok, cols), BF16),
        in_specs=[VMEM] * len(operands),
        out_specs=VMEM,
        cost_estimate=cost(2 * tok * cols * 4 * parts[0].shape[1], 10**6),
        compiler_params=PARAMS,
        name="lent",
    )(*map(in_vmem, operands))


def bias_kernel(layer, sp, table_ref, out_ref, *refs):
    *halo_refs, rows_ref = refs
    heads_n, spans = out_ref.shape[:2]
    offsets, cols = table_ref.shape[2:]
    rows_ref[...] = jnp.zeros_like(rows_ref)
    for head in range(heads_n):
        rows_ref[head, :offsets, :cols] = table_ref[layer, head]
    shape = (GRID_W, LANES)
    query_col = lax.broadcasted_iota(jnp.int32, shape, 0)
    lane = lax.broadcasted_iota(jnp.int32, shape, 1)
    key_col = lane % GRID_W
    first_col = jnp.clip(query_col - COL_SPAN // 2, 0, GRID_W - COL_SPAN)
    inside = (key_col >= first_col) & (key_col < first_col + COL_SPAN)
    for head in range(heads_n):
        plain = rows_ref[head]
        after = pltpu.roll(pltpu.roll(plain, GRID_W, axis=1), rows_ref.shape[1] - 1, axis=0)
        at_lane = lax.broadcasted_iota(jnp.int32, plain.shape, 1)
        both = jnp.where(at_lane < GRID_W, plain, after)
        for span in range(spans):
            row = jnp.broadcast_to(both[span : span + 1, :], shape)
            turned = pltpu.roll(row, LANES - (COL_SPAN - 1), axis=1, stride=1, stride_axis=0)
            out_ref[head, span] = jnp.where(inside, turned, NEG)
    for halo_ref in halo_refs:
        for row in range(halo_ref.shape[0]):
            for at in range(halo_ref.shape[2]):
                one = window_at(row, halo_ref.shape[0], sp) + 2 * at
                low = one + jnp.where(one < HALF, HALF - 1, ROW_SPAN - 1) - row
                high = one + jnp.where(one + 1 < HALF, HALF - 1, ROW_SPAN - 1) - row
                for head in range(heads_n):
                    halo_ref[row, head, at] = jnp.where(
                        lane < GRID_W, out_ref[head, low], out_ref[head, high]
                    )


def expand_bias(table, layer, halo_rows):
    _, heads_n, offsets, _ = table.shape
    spans = offsets - 1
    out_shape = [pltpu.VMEM((heads_n, spans, GRID_W, LANES), F32)]
    if halo_rows:
        out_shape.append(pltpu.VMEM((halo_rows, heads_n, HALF // 2, GRID_W, LANES), F32))
    return pl.pallas_call(
        partial(bias_kernel, layer, lax.axis_size("sp")),
        out_shape=out_shape,
        in_specs=[VMEM],
        out_specs=[VMEM] * len(out_shape),
        scratch_shapes=[pltpu.VMEM((heads_n, 2 * ROW_SPAN, LANES), F32)],
        cost_estimate=cost(heads_n * spans * GRID_W * LANES * 40, heads_n * spans * GRID_W * LANES * 4),
        compiler_params=PARAMS,
        name="bias",
    )(table)


def stacked_query(query, lane, heads_in):
    if heads_in == 1:
        return query
    zero = jnp.zeros_like(query)
    return jnp.concatenate(
        [jnp.where(lane // HEAD_DIM == head, query, zero) for head in range(heads_in)], axis=0
    )


def own_kernel(rows_dev, layer, query_ref, pair_ref, bias_ref, *refs):
    if layer is None:
        mixed_ref, peak_ref = refs
        copies = []
    else:
        *stored, mixed_ref, peak_ref, held_ref, sems = refs
        copies = [
            pltpu.make_async_copy(source.at[layer], held_ref.at[kind], sems.at[kind])
            for kind, source in enumerate(stored)
        ]
    for copy in copies:
        copy.start()
    channels = query_ref.shape[2]
    group = min(LANES, channels)
    heads_in = group // HEAD_DIM
    tok = rows_dev * GRID_W
    stack = heads_in * GRID_W
    lane = lax.broadcasted_iota(jnp.int32, (GRID_W, group), 1)
    ones = jnp.ones((tok, LANES), BF16)
    for pair in range(channels // group):
        cols = slice(pair * group, (pair + 1) * group)
        query = jnp.concatenate(
            [
                stacked_query(query_ref[0, row * GRID_W : (row + 1) * GRID_W, cols], lane, heads_in)
                for row in range(rows_dev)
            ],
            axis=0,
        )
        scores = nt_dot(query, pair_ref[0, :, cols])
        values = jnp.concatenate([pair_ref[1, :, cols], ones], axis=1)
        for row in range(rows_dev):
            here = slice(row * stack, (row + 1) * stack)
            pieces = []
            for at in range(tok // LANES):
                offset = (LANES // GRID_W) * at - row + ROW_SPAN - 1
                bias = jnp.concatenate(
                    [bias_ref[pair * heads_in + head, offset] for head in range(heads_in)], axis=0
                )
                pieces.append(scores[here, at * LANES : (at + 1) * LANES] + bias)
            peak = pieces[0]
            for piece in pieces[1:]:
                peak = jnp.maximum(peak, piece)
            peak = jnp.max(peak, axis=1, keepdims=True)
            lifted = jnp.concatenate([jnp.exp(piece - peak).astype(BF16) for piece in pieces], axis=1)
            mixed_ref[pair, here, :] = jnp.dot(lifted, values, preferred_element_type=F32)
            peak_ref[pair, here, :] = jnp.broadcast_to(peak, (stack, LANES))
    for copy in copies:
        copy.wait()


def attend_own(query, pair, bias, rows_dev, weights, layer):
    _, tok, channels = query.shape
    group = min(LANES, channels)
    pairs, rows = channels // group, tok * (group // HEAD_DIM)
    out_shape = [
        pltpu.VMEM((pairs, rows, group + LANES), F32),
        pltpu.VMEM((pairs, rows, LANES), F32),
    ]
    scratch = []
    if layer is not None:
        out_shape.append(pltpu.VMEM((3, *weights[0].shape[1:]), BF16))
        scratch.append(pltpu.SemaphoreType.DMA((3,)))
    else:
        weights = []
    return pl.pallas_call(
        partial(own_kernel, rows_dev, layer),
        out_shape=out_shape,
        in_specs=[VMEM] * 3 + [HBM] * len(weights),
        out_specs=[VMEM] * len(out_shape),
        scratch_shapes=scratch,
        cost_estimate=cost(pairs * rows * tok * 800, bias.size * 4, pairs * rows * tok),
        compiler_params=PARAMS,
        name="own",
    )(*map(in_vmem, (query, pair, bias)), *weights)


def halo_kernel(
    rows_dev, sp, query_ref, even_ref, odd_ref, bias_ref, mixed_ref, peak_ref, out_ref, keys, values
):
    channels = query_ref.shape[2]
    group = min(LANES, channels)
    heads_in = group // HEAD_DIM
    span = HALF * GRID_W
    stack = heads_in * GRID_W
    even_slot, odd_slot = halo_slots(HALF)
    for scratch, kind in ((keys, 0), (values, 1)):
        scratch[pl.ds(even_slot, span), :] = even_ref[kind]
        scratch[pl.ds(odd_slot, span), :] = odd_ref[kind]
    lane = lax.broadcasted_iota(jnp.int32, (GRID_W, group), 1)
    ones = jnp.ones((span, LANES), BF16)
    for row in range(rows_dev):
        first = pl.multiple_of(window_at(row, rows_dev, sp) * GRID_W, GRID_W)
        here = slice(row * stack, (row + 1) * stack)
        for pair in range(channels // group):
            cols = slice(pair * group, (pair + 1) * group)
            query = stacked_query(query_ref[0, row * GRID_W : (row + 1) * GRID_W, cols], lane, heads_in)
            scores = nt_dot(query, keys[pl.ds(first, span), cols])
            pieces = []
            for at in range(span // LANES):
                bias = jnp.concatenate(
                    [bias_ref[row, pair * heads_in + head, at] for head in range(heads_in)], axis=0
                )
                pieces.append(scores[:, at * LANES : (at + 1) * LANES] + bias)
            peak = pieces[0]
            for piece in pieces[1:]:
                peak = jnp.maximum(peak, piece)
            before = peak_ref[pair, here, :]
            peak = jnp.maximum(jnp.max(peak, axis=1, keepdims=True), before)
            lifted = jnp.concatenate([jnp.exp(piece - peak).astype(BF16) for piece in pieces], axis=1)
            wide = jnp.concatenate([values[pl.ds(first, span), cols], ones], axis=1)
            mixed = jnp.dot(lifted, wide, preferred_element_type=F32)
            fade = jnp.exp(before - peak)
            top = mixed_ref[pair, here, :group] * fade[:, :group] + mixed[:, :group]
            weight = mixed_ref[pair, here, group:] * fade + mixed[:, group:]
            result, total = top[:GRID_W], weight[:GRID_W, :group]
            for head in range(1, heads_in):
                mine = lane // HEAD_DIM == head
                below = slice(head * GRID_W, (head + 1) * GRID_W)
                result = jnp.where(mine, top[below], result)
                total = jnp.where(mine, weight[below, :group], total)
            out_ref[row * GRID_W : (row + 1) * GRID_W, cols] = (result / total).astype(BF16)


def attend_halo(query, even, odd, bias, mixed, peak, rows_dev):
    _, tok, channels = query.shape
    scores = tok * (channels // HEAD_DIM) * HALF * GRID_W
    return pl.pallas_call(
        partial(halo_kernel, rows_dev, lax.axis_size("sp")),
        out_shape=pltpu.VMEM((tok, channels), BF16),
        in_specs=[VMEM] * 6,
        out_specs=VMEM,
        scratch_shapes=[pltpu.VMEM((ROW_SPAN * GRID_W, channels), BF16)] * 2,
        cost_estimate=cost(scores * HEAD_DIM * 6, bias.size * 4 + tok * channels * 16, scores),
        compiler_params=PARAMS,
        name="halo",
    )(*map(in_vmem, (query, even, odd, bias, mixed, peak)))


def attend_kernel(
    rows_dev, sp, query_ref, own_ref, even_ref, odd_ref, bias_ref, out_ref, keys, values
):
    channels = query_ref.shape[2]
    group = min(LANES, channels)
    heads_in = group // HEAD_DIM
    span = ROW_SPAN * GRID_W
    even_slot, odd_slot = halo_slots(HALF + rows_dev)
    halo = HALF * GRID_W
    for scratch, kind in ((keys, 0), (values, 1)):
        scratch[HALF * GRID_W : (HALF + rows_dev) * GRID_W, :] = own_ref[kind]
        scratch[pl.ds(even_slot, halo), :] = even_ref[kind]
        scratch[pl.ds(odd_slot, halo), :] = odd_ref[kind]
    lane = lax.broadcasted_iota(jnp.int32, (GRID_W, group), 1)
    ones = jnp.ones((span, group), BF16)
    for row in range(rows_dev):
        window = window_at(row, rows_dev, sp)
        first = pl.multiple_of(window * GRID_W, GRID_W)
        offset = window - row + HALF - 1
        for pair in range(channels // group):
            cols = slice(pair * group, (pair + 1) * group)
            query = query_ref[0, row * GRID_W : (row + 1) * GRID_W, cols]
            query = stacked_query(query, lane, heads_in)
            scores = nt_dot(query, keys[pl.ds(first, span), cols])
            pieces = []
            for at in range(span // LANES):
                bias = jnp.concatenate(
                    [
                        bias_ref[pair * heads_in + head, offset + (LANES // GRID_W) * at]
                        for head in range(heads_in)
                    ],
                    axis=0,
                )
                pieces.append(scores[:, at * LANES : (at + 1) * LANES] + bias)
            peak = pieces[0]
            for piece in pieces[1:]:
                peak = jnp.maximum(peak, piece)
            peak = jnp.max(peak, axis=1, keepdims=True)
            lifted = jnp.concatenate([jnp.exp(piece - peak).astype(BF16) for piece in pieces], axis=1)
            mixed = jnp.dot(lifted, values[pl.ds(first, span), cols], preferred_element_type=F32)
            weight = jnp.dot(lifted, ones, preferred_element_type=F32)
            mixed = mixed / weight
            result = mixed[:GRID_W]
            for head in range(1, heads_in):
                result = jnp.where(
                    lane // HEAD_DIM == head, mixed[head * GRID_W : (head + 1) * GRID_W], result
                )
            out_ref[row * GRID_W : (row + 1) * GRID_W, cols] = result.astype(BF16)


def attend(query, own, even, odd, bias, rows_dev):
    _, tok, channels = query.shape
    padded = (rows_dev + 2 * HALF) * GRID_W
    scores = tok * (channels // HEAD_DIM) * ROW_SPAN * GRID_W
    return pl.pallas_call(
        partial(attend_kernel, rows_dev, lax.axis_size("sp")),
        out_shape=pltpu.VMEM((tok, channels), BF16),
        in_specs=[VMEM] * 5,
        out_specs=VMEM,
        scratch_shapes=[pltpu.VMEM((padded, channels), BF16)] * 2,
        cost_estimate=cost(scores * HEAD_DIM * 6, bias.size * 4 + tok * channels * 16, scores),
        compiler_params=PARAMS,
        name="attend",
    )(query, own, even, odd, bias)


def exchange(block, pairs):
    sp, tp = lax.axis_size("sp"), lax.axis_size("tp")
    partner = {}
    for one, two in pairs:
        partner[one], partner[two] = two, one
    moves = []
    for row in range(sp):
        for col in range(tp):
            if row in partner:
                moves.append((row * tp + col, partner[row] * tp + col))
            elif tp % 2 == 0:
                moves.append((row * tp + col, row * tp + (col ^ 1)))
    return lax.ppermute(block, ("sp", "tp"), moves)


def flip(block, axis, bit):
    count = lax.axis_size(axis)
    return lax.ppermute(block, axis, [(at, at ^ bit) for at in range(count)])


def send_weight(cuts, layer):
    near = []
    for cut in cuts[layer]:
        near.append(flip(cut, "tp", 2))
    return near


def body(hidden_in, norm_gain, query_weight, key_weight, value_weight, output_weight, offset_bias):
    tok_dev, _ = hidden_in.shape
    rows_dev = tok_dev // GRID_W
    tp = lax.axis_size("tp")
    sp = lax.axis_size("sp")
    is_odd = lax.axis_index("sp") % 2
    split = rows_dev == HALF
    weights = [in_hbm(weight) for weight in (query_weight, key_weight, value_weight)]
    output_weight = in_hbm(output_weight)
    even_pairs = [(at, at + 1) for at in range(0, sp - 1, 2)]
    odd_pairs = [(at, at + 1) for at in range(1, sp - 1, 2)]
    stream = hidden_in
    lend = split and tp == 4 and lax.axis_size("grp") == 2 and len(PARTS) == LAYERS - 1
    carry = None
    for layer in range(LAYERS):
        step = partial(project, layer=layer, gain=norm_gain)
        if carry is not None:
            parts, base, last_lent, held = carry
            beside = flip(stream, "tp", 1)
            across = emit_far(parts, base, *last_lent)
            corner = flip(across, "tp", 1)
            carried = step([stream, across], (0, 2), held, None, None)
            carried = step([beside], (1,), held, carried, None)
        elif tp == 4:
            across = flip(stream, "tp", 2)
            beside = flip(stream, "tp", 1)
            corner = flip(across, "tp", 1)
            *carried, held = step([stream], (0,), weights, None, None)
            carried = step([beside], (1,), held, carried, None)
            carried = step([across], (2,), held, carried, None)
        if tp == 4:
            across_stream = across
            (pair,) = step([corner], (3,), held, carried, (1, 2))
            (query,) = step([corner], (3,), held, carried, (0,))
        else:
            gathered = lax.all_gather(stream, "tp", axis=1, tiled=True)
            *carried, held = step([gathered], (None,), weights, None, (0, 1, 2))
            query, pair = carried[0][:1], carried[0][1:]
        if lend and layer < LAYERS - 1:
            if layer == 0:
                cuts = cut_weight(output_weight)
                near = send_weight(cuts, layer)
            side = []
            for piece in near:
                side.append(flip(piece, "grp", 1))
            lent = (near, side)
        else:
            lent = None
        if split:
            to_even = to_odd = pair
        else:
            low, top = pair[:, : HALF * GRID_W], pair[:, (rows_dev - HALF) * GRID_W :]
            to_even = jnp.where(is_odd == 0, top, low)
            to_odd = jnp.where(is_odd == 0, low, top)
        even = exchange(to_even, even_pairs)
        odd = exchange(to_odd, odd_pairs)
        bias, *halo_bias = expand_bias(offset_bias, layer, rows_dev if split else 0)
        if split:
            mixed, peak, *held_next = attend_own(
                query, pair, bias, rows_dev, weights, layer + 1 if lent else None
            )
            attended = attend_halo(
                query, even, odd, halo_bias[0], mixed, peak, rows_dev
            )
        else:
            attended = attend(query, pair, even, odd, bias, rows_dev)
        step = partial(emit, layer=layer)
        carry = None
        if tp == 4:
            across = flip(attended, "tp", 2)
            beside = flip(attended, "tp", 1)
            corner = flip(across, "tp", 1)
            if lent and layer + 1 < LAYERS - 1:
                near = send_weight(cuts, layer + 1)
            partly, held = step([attended], (0,), output_weight, stream, F32, True)
            (partly,) = step([beside], (1,), held, partly, F32, False)
            (partly,) = step([across], (2,), held, partly, F32, False)
            old = across_stream
            (stream,) = step([corner], (3,), held, partly, BF16, False)
            if lent:
                carry = ([attended, beside, across, corner], old, lent, held_next[0])
        else:
            gathered = lax.all_gather(attended, "tp", axis=1, tiled=True)
            stream, _ = step([gathered], (None,), output_weight, stream, BF16, True)
    return stream


def solution(mesh):
    return jax.shard_map(
        body,
        mesh=mesh,
        in_specs=(
            P(("grp", "sp"), "tp"),
            P(),
            P(None, "tp", None),
            P(None, "tp", None),
            P(None, "tp", None),
            P(None, None, "tp"),
            P(None, "tp", None, None),
        ),
        out_specs=P(("grp", "sp"), "tp"),
        check_vma=False,
    )
```

```python
from functools import partial

import jax
import jax.numpy as jnp
from jax import lax
from jax.experimental import pallas as pl
from jax.experimental.pallas import tpu as pltpu
from jax.sharding import PartitionSpec as P


HEAD_DIM = 64
GRID_W = 64
ROW_SPAN = 8
COL_SPAN = 16
LAYERS = 3
HALF = ROW_SPAN // 2
ALL, KEYED = (0, 1, 2), (1, 2)
PARTS = ((1, 2, 1), (2, 2))

EPS = 1e-06
NEG = -1e30
LANES = 128
F32 = jnp.float32
BF16 = jnp.bfloat16

PARAMS = pltpu.CompilerParams(vmem_limit_bytes=8 * 2**20)
VMEM = pl.BlockSpec(memory_space=pltpu.VMEM)
HBM = pl.BlockSpec(memory_space=pltpu.HBM)


def nt_dot(left, right):
    return lax.dot_general(left, right, (((1,), (1,)), ((), ())), preferred_element_type=F32)


def in_vmem(array):
    return pltpu.with_memory_space_constraint(array, memory_space=pltpu.VMEM)


def in_hbm(array):
    return pltpu.with_memory_space_constraint(array, memory_space=pltpu.HBM)


def cost(flops, bytes_accessed, transcendentals=0):
    return pl.CostEstimate(
        flops=int(flops), bytes_accessed=int(bytes_accessed), transcendentals=int(transcendentals)
    )


def call(kernel, operands, in_specs, out_shape, estimate, scratch=(), rider=None):
    taken, given = len(operands), len(out_shape)
    arrays, shapes, pick, count = rider or ((), (), None, 0)

    def carrying(*refs):
        ends = taken, taken + len(arrays), taken + len(arrays) + given
        last = ends[2] + len(shapes)
        copies = [
            pltpu.make_async_copy(source, target, refs[-1].at[at])
            for at, (source, target) in enumerate(
                pick(refs[ends[0] : ends[1]], refs[ends[2] : last])
            )
        ]
        for copy in copies:
            copy.start()
        kernel(*refs[: ends[0]], *refs[ends[1] : ends[2]], *refs[last:-1])
        for copy in copies:
            copy.wait()

    sems = [pltpu.SemaphoreType.DMA((count,))] if rider else []
    return pl.pallas_call(
        carrying if rider else kernel,
        out_shape=[*out_shape, *(pltpu.VMEM(shape, BF16) for shape in shapes)],
        in_specs=[*in_specs, *[HBM] * len(arrays)],
        out_specs=[VMEM] * (given + len(shapes)),
        scratch_shapes=[*scratch, *sems],
        cost_estimate=estimate,
        compiler_params=PARAMS,
    )(*operands, *arrays)


def block_at(bit, width, unit, sub=0, subs=1):
    if bit is None:
        return slice(None)
    first = (lax.axis_index("tp") ^ bit) * (width * subs) + sub * width
    return pl.ds(pl.multiple_of(first, unit), width)


def window_at(row, rows_dev, sp):
    first_row = lax.axis_index("sp") * rows_dev
    first = jnp.minimum(jnp.maximum(first_row + row - HALF, 0), rows_dev * sp - ROW_SPAN)
    return first - first_row + HALF


def halo_slots(high):
    odd = lax.axis_index("sp") % 2
    return (
        pl.multiple_of((1 - odd) * (high * GRID_W), GRID_W),
        pl.multiple_of(odd * (high * GRID_W), GRID_W),
    )


def project_kernel(bits, load, shared, kinds, have, final, layer, *refs):
    sources, refs = refs[: len(bits)], refs[len(bits) :]
    gain_ref, refs = refs[0], refs[1:]
    if load:
        stored, refs = refs[:3], refs[3:]
        *refs, held_ref, sems = refs
        copies = [
            pltpu.make_async_copy(stored[kind].at[layer], held_ref.at[kind], sems.at[kind])
            for kind in range(3)
        ]
        for copy in copies:
            copy.start()
    elif shared:
        stored, refs = refs[:3], refs[3:]
    else:
        held_ref, refs = refs[0], refs[1:]
    if have:
        (acc_in, sq_in), refs = refs[:2], refs[2:]
    full = gain_ref.shape[1]
    totals = [None, None, None]
    squares = None
    for at, bit in enumerate(bits):
        wide = sources[at][...].astype(F32)
        width = wide.shape[1]
        cols = block_at(bit, width, LANES)
        square = jnp.sum(wide * wide, axis=1, keepdims=True)
        squares = square if squares is None else squares + square
        scaled = (wide * gain_ref[layer : layer + 1, cols]).astype(BF16)
        for kind in kinds:
            if load and at == 0:
                copies[kind].wait()
            held = stored[kind][layer, :, cols] if shared else held_ref[kind, :, cols]
            product = nt_dot(scaled, held)
            totals[kind] = product if totals[kind] is None else totals[kind] + product
    if have:
        squares = squares + sq_in[:, :1]
        for kind in kinds:
            totals[kind] = totals[kind] + acc_in[have.index(kind)]
    if final:
        row_scale = lax.rsqrt(squares * (1.0 / full) + EPS)
        for at, kind in enumerate(kinds):
            scale = row_scale * HEAD_DIM ** (-0.5) if kind == 0 else row_scale
            made = (totals[kind] * scale).astype(BF16)
            for group, out_ref in enumerate(refs):
                width = out_ref.shape[2]
                out_ref[at] = made[:, group * width : (group + 1) * width]
    else:
        acc_out, sq_out = refs
        for at, kind in enumerate(kinds):
            acc_out[at] = totals[kind]
        sq_out[...] = jnp.broadcast_to(squares, sq_out.shape)


def project(parts, bits, weights, carried, kinds, have, final, layer, gain, groups=1):
    tok, width = parts[0].shape
    parts_n = len(parts)
    operands = [*parts, gain]
    specs = [VMEM] * (parts_n + 1)
    load, shared = isinstance(weights, list), isinstance(weights, tuple)
    if load:
        _, channels, full = weights[0].shape
        operands += weights
        specs += [HBM] * 3
    elif shared:
        _, channels, full = weights[0].shape
        operands += weights
        specs += [VMEM] * 3
    else:
        _, channels, full = weights.shape
        operands.append(in_vmem(weights))
        specs.append(VMEM)
    if have:
        operands += map(in_vmem, carried)
        specs += [VMEM] * 2
    if final:
        out_shape = [pltpu.VMEM((len(kinds), tok, channels // groups), BF16)] * groups
    else:
        out_shape = [pltpu.VMEM((len(kinds), tok, channels), F32), pltpu.VMEM((tok, LANES), F32)]
    scratch = []
    if load:
        out_shape.append(pltpu.VMEM((3, channels, full), BF16))
        scratch.append(pltpu.SemaphoreType.DMA((3,)))
    flops = 2 * tok * width * channels * len(kinds) * parts_n
    return call(
        partial(project_kernel, bits, load, shared, kinds, have, final, layer),
        operands,
        specs,
        out_shape,
        cost(flops, parts_n * width * (channels * 6 + tok * 2) + 4 * tok * channels),
        scratch,
    )


def emit_kernel(bits, load, layer, sub, subs, *refs):
    sources, refs = refs[: len(bits)], refs[len(bits) :]
    held_ref, base_ref, out_ref, *rest = refs
    if load:
        stored_ref, (held_ref, sem) = held_ref, rest
        copy = pltpu.make_async_copy(stored_ref.at[layer], held_ref, sem)
        copy.start()
    total = base_ref[...].astype(F32)
    if load:
        copy.wait()
    for at, bit in enumerate(bits):
        rows = block_at(bit, sources[at].shape[1], HEAD_DIM, sub, subs)
        held = held_ref[rows, :] if load else held_ref[layer, rows, :]
        total = total + jnp.dot(sources[at][...], held, preferred_element_type=F32)
    out_ref[...] = total.astype(out_ref.dtype)


def emit(parts, bits, weight, base, out_type, load, layer, sub=0, subs=1):
    tok, width = parts[0].shape
    cols = base.shape[1]
    out_shape = [pltpu.VMEM((tok, cols), out_type)]
    if out_type == BF16 and layer == LAYERS - 1:
        out_shape = [jax.ShapeDtypeStruct((tok, cols), out_type)]
    scratch = []
    if load:
        scratch = [pltpu.VMEM(weight.shape[1:], BF16), pltpu.SemaphoreType.DMA]
    return call(
        partial(emit_kernel, bits, load, layer, sub, subs),
        [*parts, weight, base],
        [VMEM] * len(parts) + [HBM if load else VMEM, VMEM],
        out_shape,
        cost(2 * tok * width * cols * len(bits), 10**6),
        scratch,
    )


def cut_weight(weight):
    _, rows, cols = weight.shape
    half = rows // 2
    slabs = []
    for layer, parts in enumerate(PARTS):
        unit = cols // sum(parts)
        for at, part in enumerate(parts):
            slabs.append((layer, unit * sum(parts[:at]), unit * part))

    def pick(sources, targets):
        here = pl.ds(pl.multiple_of(lax.axis_index("grp") * half, half), half)
        return [
            (sources[0].at[layer, here, pl.ds(first, width)], target)
            for (layer, first, width), target in zip(slabs, targets)
        ]

    shapes = [(half, width) for _, _, width in slabs]
    rider = [weight], shapes, pick, len(slabs)
    cuts = call(lambda *refs: None, [], [], [], cost(10**6, 10**6), rider=rider)
    return [
        [cut for cut, slab in zip(cuts, slabs) if slab[0] == layer] for layer in range(len(PARTS))
    ]


def far_kernel(pieces, own_ref, beside_ref, across_ref, corner_ref, base_ref, *refs):
    near, side, out_ref = refs[:pieces], refs[pieces:-1], refs[-1]
    me = lax.axis_index("tp")
    even = me % 2 == 0
    aligned = me // 2 == lax.axis_index("grp")
    own, beside, across, corner = own_ref[...], beside_ref[...], across_ref[...], corner_ref[...]
    mine = jnp.concatenate([jnp.where(even, own, beside), jnp.where(even, beside, own)], axis=1)
    other = jnp.concatenate(
        [jnp.where(even, across, corner), jnp.where(even, corner, across)], axis=1
    )
    with_near = jnp.where(aligned, mine, other)
    with_side = jnp.where(aligned, other, mine)
    done = 0
    for at in range(pieces):
        cols = slice(done, done + near[at].shape[1])
        done = cols.stop
        total = base_ref[:, cols].astype(F32)
        total = total + jnp.dot(with_near, near[at][...], preferred_element_type=F32)
        total = total + jnp.dot(with_side, side[at][...], preferred_element_type=F32)
        out_ref[:, cols] = total.astype(BF16)


def emit_far(parts, base, near, side):
    tok, cols = base.shape
    operands = [*parts, base, *near, *side]
    return pl.pallas_call(
        partial(far_kernel, len(near)),
        out_shape=pltpu.VMEM((tok, cols), BF16),
        in_specs=[VMEM] * len(operands),
        out_specs=VMEM,
        cost_estimate=cost(2 * tok * cols * 4 * parts[0].shape[1], 10**6),
        compiler_params=PARAMS,
        name="lent",
    )(*map(in_vmem, operands))


def bias_kernel(layer, sp, table_ref, out_ref, *refs):
    *halo_refs, rows_ref = refs
    heads_n, spans = out_ref.shape[:2]
    offsets, cols = table_ref.shape[2:]
    rows_ref[...] = jnp.zeros_like(rows_ref)
    for head in range(heads_n):
        rows_ref[head, :offsets, :cols] = table_ref[layer, head]
    shape = (GRID_W, LANES)
    query_col = lax.broadcasted_iota(jnp.int32, shape, 0)
    lane = lax.broadcasted_iota(jnp.int32, shape, 1)
    key_col = lane % GRID_W
    first_col = jnp.clip(query_col - COL_SPAN // 2, 0, GRID_W - COL_SPAN)
    inside = (key_col >= first_col) & (key_col < first_col + COL_SPAN)
    for head in range(heads_n):
        plain = rows_ref[head]
        after = pltpu.roll(pltpu.roll(plain, GRID_W, axis=1), rows_ref.shape[1] - 1, axis=0)
        at_lane = lax.broadcasted_iota(jnp.int32, plain.shape, 1)
        both = jnp.where(at_lane < GRID_W, plain, after)
        for span in range(spans):
            row = jnp.broadcast_to(both[span : span + 1, :], shape)
            turned = pltpu.roll(row, LANES - (COL_SPAN - 1), axis=1, stride=1, stride_axis=0)
            out_ref[head, span] = jnp.where(inside, turned, NEG)
    for halo_ref in halo_refs:
        for row in range(halo_ref.shape[0]):
            for at in range(halo_ref.shape[2]):
                one = window_at(row, halo_ref.shape[0], sp) + 2 * at
                low = one + jnp.where(one < HALF, HALF - 1, ROW_SPAN - 1) - row
                high = one + jnp.where(one + 1 < HALF, HALF - 1, ROW_SPAN - 1) - row
                for head in range(heads_n):
                    halo_ref[row, head, at] = jnp.where(
                        lane < GRID_W, out_ref[head, low], out_ref[head, high]
                    )


def expand_bias(table, layer, halo_rows):
    _, heads_n, offsets, _ = table.shape
    spans = offsets - 1
    out_shape = [pltpu.VMEM((heads_n, spans, GRID_W, LANES), F32)]
    if halo_rows:
        out_shape.append(pltpu.VMEM((halo_rows, heads_n, HALF // 2, GRID_W, LANES), F32))
    return call(
        partial(bias_kernel, layer, lax.axis_size("sp")),
        [table],
        [VMEM],
        out_shape,
        cost(heads_n * spans * GRID_W * LANES * 40, heads_n * spans * GRID_W * LANES * 4),
        [pltpu.VMEM((heads_n, 2 * ROW_SPAN, LANES), F32)],
    )


def stacked_query(query, lane, heads_in):
    if heads_in == 1:
        return query
    zero = jnp.zeros_like(query)
    return jnp.concatenate(
        [jnp.where(lane // HEAD_DIM == head, query, zero) for head in range(heads_in)], axis=0
    )


def own_kernel(rows_dev, head0, query_ref, pair_ref, bias_ref, mixed_ref, peak_ref):
    channels = query_ref.shape[2]
    group = min(LANES, channels)
    heads_in = group // HEAD_DIM
    tok = rows_dev * GRID_W
    stack = heads_in * GRID_W
    lane = lax.broadcasted_iota(jnp.int32, (GRID_W, group), 1)
    ones = jnp.ones((tok, LANES), BF16)
    for pair in range(channels // group):
        cols = slice(pair * group, (pair + 1) * group)
        query = jnp.concatenate(
            [
                stacked_query(query_ref[0, row * GRID_W : (row + 1) * GRID_W, cols], lane, heads_in)
                for row in range(rows_dev)
            ],
            axis=0,
        )
        scores = nt_dot(query, pair_ref[0, :, cols])
        values = jnp.concatenate([pair_ref[1, :, cols], ones], axis=1)
        for row in range(rows_dev):
            here = slice(row * stack, (row + 1) * stack)
            pieces = []
            for at in range(tok // LANES):
                offset = (LANES // GRID_W) * at - row + ROW_SPAN - 1
                bias = jnp.concatenate(
                    [bias_ref[head0 + pair * heads_in + head, offset] for head in range(heads_in)],
                    axis=0,
                )
                pieces.append(scores[here, at * LANES : (at + 1) * LANES] + bias)
            peak = pieces[0]
            for piece in pieces[1:]:
                peak = jnp.maximum(peak, piece)
            peak = jnp.max(peak, axis=1, keepdims=True)
            lifted = jnp.concatenate([jnp.exp(piece - peak).astype(BF16) for piece in pieces], axis=1)
            mixed_ref[pair, here, :] = jnp.dot(lifted, values, preferred_element_type=F32)
            peak_ref[pair, here, :] = jnp.broadcast_to(peak, (stack, LANES))


def attend_own(query, pair, bias, rows_dev, head0=0):
    _, tok, channels = query.shape
    group = min(LANES, channels)
    pairs, rows = channels // group, tok * (group // HEAD_DIM)
    return call(
        partial(own_kernel, rows_dev, head0),
        [*map(in_vmem, (query, pair, bias))],
        [VMEM] * 3,
        [
            pltpu.VMEM((pairs, rows, group + LANES), F32),
            pltpu.VMEM((pairs, rows, LANES), F32),
        ],
        cost(pairs * rows * tok * 800, bias.size * 4, pairs * rows * tok),
    )


def halo_kernel(
    rows_dev, sp, head0, query_ref, even_ref, odd_ref, bias_ref, mixed_ref, peak_ref, out_ref, keys, values
):
    channels = query_ref.shape[2]
    group = min(LANES, channels)
    heads_in = group // HEAD_DIM
    span = HALF * GRID_W
    stack = heads_in * GRID_W
    even_slot, odd_slot = halo_slots(HALF)
    for scratch, kind in ((keys, 0), (values, 1)):
        scratch[pl.ds(even_slot, span), :] = even_ref[kind]
        scratch[pl.ds(odd_slot, span), :] = odd_ref[kind]
    lane = lax.broadcasted_iota(jnp.int32, (GRID_W, group), 1)
    ones = jnp.ones((span, LANES), BF16)
    for row in range(rows_dev):
        first = pl.multiple_of(window_at(row, rows_dev, sp) * GRID_W, GRID_W)
        here = slice(row * stack, (row + 1) * stack)
        for pair in range(channels // group):
            cols = slice(pair * group, (pair + 1) * group)
            query = stacked_query(query_ref[0, row * GRID_W : (row + 1) * GRID_W, cols], lane, heads_in)
            scores = nt_dot(query, keys[pl.ds(first, span), cols])
            pieces = []
            for at in range(span // LANES):
                bias = jnp.concatenate(
                    [bias_ref[row, head0 + pair * heads_in + head, at] for head in range(heads_in)],
                    axis=0,
                )
                pieces.append(scores[:, at * LANES : (at + 1) * LANES] + bias)
            peak = pieces[0]
            for piece in pieces[1:]:
                peak = jnp.maximum(peak, piece)
            before = peak_ref[pair, here, :]
            peak = jnp.maximum(jnp.max(peak, axis=1, keepdims=True), before)
            lifted = jnp.concatenate([jnp.exp(piece - peak).astype(BF16) for piece in pieces], axis=1)
            wide = jnp.concatenate([values[pl.ds(first, span), cols], ones], axis=1)
            mixed = jnp.dot(lifted, wide, preferred_element_type=F32)
            fade = jnp.exp(before - peak)
            top = mixed_ref[pair, here, :group] * fade[:, :group] + mixed[:, :group]
            weight = mixed_ref[pair, here, group:] * fade + mixed[:, group:]
            result, total = top[:GRID_W], weight[:GRID_W, :group]
            for head in range(1, heads_in):
                mine = lane // HEAD_DIM == head
                below = slice(head * GRID_W, (head + 1) * GRID_W)
                result = jnp.where(mine, top[below], result)
                total = jnp.where(mine, weight[below, :group], total)
            out_ref[row * GRID_W : (row + 1) * GRID_W, cols] = (result / total).astype(BF16)


def attend_halo(query, even, odd, bias, mixed, peak, rows_dev, head0=0):
    _, tok, channels = query.shape
    scores = tok * (channels // HEAD_DIM) * HALF * GRID_W
    return pl.pallas_call(
        partial(halo_kernel, rows_dev, lax.axis_size("sp"), head0),
        out_shape=pltpu.VMEM((tok, channels), BF16),
        in_specs=[VMEM] * 6,
        out_specs=VMEM,
        scratch_shapes=[pltpu.VMEM((ROW_SPAN * GRID_W, channels), BF16)] * 2,
        cost_estimate=cost(scores * HEAD_DIM * 6, bias.size * 4 + tok * channels * 16, scores),
        compiler_params=PARAMS,
        name="halo",
    )(*map(in_vmem, (query, even, odd, bias, mixed, peak)))


def attend_kernel(
    rows_dev, sp, query_ref, own_ref, even_ref, odd_ref, bias_ref, out_ref, keys, values
):
    channels = query_ref.shape[2]
    group = min(LANES, channels)
    heads_in = group // HEAD_DIM
    span = ROW_SPAN * GRID_W
    even_slot, odd_slot = halo_slots(HALF + rows_dev)
    halo = HALF * GRID_W
    for scratch, kind in ((keys, 0), (values, 1)):
        scratch[HALF * GRID_W : (HALF + rows_dev) * GRID_W, :] = own_ref[kind]
        scratch[pl.ds(even_slot, halo), :] = even_ref[kind]
        scratch[pl.ds(odd_slot, halo), :] = odd_ref[kind]
    lane = lax.broadcasted_iota(jnp.int32, (GRID_W, group), 1)
    ones = jnp.ones((span, group), BF16)
    for row in range(rows_dev):
        window = window_at(row, rows_dev, sp)
        first = pl.multiple_of(window * GRID_W, GRID_W)
        offset = window - row + HALF - 1
        for pair in range(channels // group):
            cols = slice(pair * group, (pair + 1) * group)
            query = query_ref[0, row * GRID_W : (row + 1) * GRID_W, cols]
            query = stacked_query(query, lane, heads_in)
            scores = nt_dot(query, keys[pl.ds(first, span), cols])
            pieces = []
            for at in range(span // LANES):
                bias = jnp.concatenate(
                    [
                        bias_ref[pair * heads_in + head, offset + (LANES // GRID_W) * at]
                        for head in range(heads_in)
                    ],
                    axis=0,
                )
                pieces.append(scores[:, at * LANES : (at + 1) * LANES] + bias)
            peak = pieces[0]
            for piece in pieces[1:]:
                peak = jnp.maximum(peak, piece)
            peak = jnp.max(peak, axis=1, keepdims=True)
            lifted = jnp.concatenate([jnp.exp(piece - peak).astype(BF16) for piece in pieces], axis=1)
            mixed = jnp.dot(lifted, values[pl.ds(first, span), cols], preferred_element_type=F32)
            weight = jnp.dot(lifted, ones, preferred_element_type=F32)
            mixed = mixed / weight
            result = mixed[:GRID_W]
            for head in range(1, heads_in):
                result = jnp.where(
                    lane // HEAD_DIM == head, mixed[head * GRID_W : (head + 1) * GRID_W], result
                )
            out_ref[row * GRID_W : (row + 1) * GRID_W, cols] = result.astype(BF16)


def attend(query, own, even, odd, bias, rows_dev):
    _, tok, channels = query.shape
    padded = (rows_dev + 2 * HALF) * GRID_W
    scores = tok * (channels // HEAD_DIM) * ROW_SPAN * GRID_W
    return pl.pallas_call(
        partial(attend_kernel, rows_dev, lax.axis_size("sp")),
        out_shape=pltpu.VMEM((tok, channels), BF16),
        in_specs=[VMEM] * 5,
        out_specs=VMEM,
        scratch_shapes=[pltpu.VMEM((padded, channels), BF16)] * 2,
        cost_estimate=cost(scores * HEAD_DIM * 6, bias.size * 4 + tok * channels * 16, scores),
        compiler_params=PARAMS,
        name="attend",
    )(query, own, even, odd, bias)


def exchange(block, pairs):
    sp, tp = lax.axis_size("sp"), lax.axis_size("tp")
    partner = {}
    for one, two in pairs:
        partner[one], partner[two] = two, one
    moves = []
    for row in range(sp):
        for col in range(tp):
            if row in partner:
                moves.append((row * tp + col, partner[row] * tp + col))
            elif tp % 2 == 0:
                moves.append((row * tp + col, row * tp + (col ^ 1)))
    return lax.ppermute(block, ("sp", "tp"), moves)


def flip(block, axis, bit):
    count = lax.axis_size(axis)
    return lax.ppermute(block, axis, [(at, at ^ bit) for at in range(count)])


def body(hidden_in, norm_gain, query_weight, key_weight, value_weight, output_weight, offset_bias):
    tok_dev, _ = hidden_in.shape
    rows_dev = tok_dev // GRID_W
    tp = lax.axis_size("tp")
    sp = lax.axis_size("sp")
    is_odd = lax.axis_index("sp") % 2
    split = rows_dev == HALF
    weights = [in_hbm(weight) for weight in (query_weight, key_weight, value_weight)]
    even_pairs = [(at, at + 1) for at in range(0, sp - 1, 2)]
    odd_pairs = [(at, at + 1) for at in range(1, sp - 1, 2)]
    stream = hidden_in
    lend = split and tp == 4 and lax.axis_size("grp") == 2 and len(PARTS) == LAYERS - 1
    lent = None
    near = {}
    shared = query_weight, key_weight, value_weight

    def send(cuts, layer, first, end):
        for at in range(first, end):
            near.setdefault(layer, []).append(flip(cuts[layer][at], "tp", 2))

    for layer in range(LAYERS):
        step = partial(project, layer=layer, gain=norm_gain)
        if lent:
            parts, base, held = carry
            beside = flip(stream, "tp", 1)
            across = emit_far(parts, base, near[layer - 1], side)
            corner = flip(across, "tp", 1)
            carried = step([stream, across], (0, 2), held, None, KEYED, (), False)
            carried = step([beside], (1,), held, carried, KEYED, KEYED, False)
        elif tp == 4:
            across = flip(stream, "tp", 2)
            beside = flip(stream, "tp", 1)
            corner = flip(across, "tp", 1)
            *carried, held = step([stream], (0,), weights, None, ALL, (), False)
            carried = step([beside], (1,), held, carried, ALL, ALL, False)
            if lend:
                cuts = cut_weight(in_hbm(output_weight))
                send(cuts, layer, 0, len(cuts[layer]))
            carried = step([across], (2,), held, carried, ALL, ALL, False)
        groups = query_weight.shape[1] // LANES
        if tp == 4:
            sources = [stream, across, beside, corner]
        if lend and layer == LAYERS - 1 and groups == 2:
            pairs, queries, swaps, attended = [], [], [], []
            pairs = step([corner], (3,), held, carried, KEYED, KEYED, True, groups=groups)
            queries = step(sources, (0, 2, 1, 3), held, None, (0,), (), True, groups=groups)
            for pair in pairs:
                swaps.append(exchange(pair, even_pairs))
                swaps.append(exchange(pair, odd_pairs))
            bias, halo_bias = expand_bias(offset_bias, layer, rows_dev)
            beside, across, corner = [], [], []
            for group in range(groups):
                head0 = group * (LANES // HEAD_DIM)
                mixed, peak = attend_own(queries[group], pairs[group], bias, rows_dev, head0)
                halo = swaps[2 * group : 2 * group + 2]
                done = attend_halo(queries[group], *halo, halo_bias, mixed, peak, rows_dev, head0)
                attended.append(done)
                across.append(flip(done, "tp", 2))
                beside.append(flip(done, "tp", 1))
                corner.append(flip(across[-1], "tp", 1))
            turns = [(attended, 0), (beside, 1), (across, 2), (corner, 3)]
            for group in range(groups):
                for part, bit in turns:
                    final = group == groups - 1 and bit == 3
                    (stream,) = emit(
                        [part[group]],
                        (bit,),
                        output_weight,
                        stream,
                        BF16 if final else F32,
                        False,
                        layer,
                        group,
                        groups,
                    )
            return stream
        if tp == 4:
            old = across
            (pair,) = step([corner], (3,), held, carried, KEYED, KEYED if layer and lend else ALL, True)
            if layer and lend:
                (query,) = step(sources, (0, 2, 1, 3), held, None, (0,), (), True)
            else:
                keep = shared if lend else held
                (query,) = step([corner], (3,), keep, carried, (0,), ALL, True)
        else:
            gathered = lax.all_gather(stream, "tp", axis=1, tiled=True)
            *carried, held = step([gathered], (None,), weights, None, ALL, (), True)
            query, pair = carried[0][:1], carried[0][1:]
        if split:
            to_even = to_odd = pair
        else:
            low, top = pair[:, : HALF * GRID_W], pair[:, (rows_dev - HALF) * GRID_W :]
            to_even = jnp.where(is_odd == 0, top, low)
            to_odd = jnp.where(is_odd == 0, low, top)
        even = exchange(to_even, even_pairs)
        odd = exchange(to_odd, odd_pairs)
        lent = lend and layer < LAYERS - 1
        more = lend and layer < LAYERS - 2
        bias, *halo_bias = expand_bias(offset_bias, layer, rows_dev if split else 0)
        if lent:
            side = []
            for piece in near[layer]:
                side.append(flip(piece, "grp", 1))
        if split:
            mixed, peak = attend_own(query, pair, bias, rows_dev)
            attended = attend_halo(
                query, even, odd, halo_bias[0], mixed, peak, rows_dev
            )
        else:
            attended = attend(query, pair, even, odd, bias, rows_dev)
        step = partial(emit, layer=layer)
        if tp == 4:
            across = flip(attended, "tp", 2)
            beside = flip(attended, "tp", 1)
            corner = flip(across, "tp", 1)
            (partly,) = step([attended], (0,), output_weight, stream, F32, False)
            (partly,) = step([beside], (1,), output_weight, partly, F32, False)
            (partly,) = step([across], (2,), output_weight, partly, F32, False)
            if more:
                send(cuts, layer + 1, 0, len(cuts[layer + 1]))
            (stream,) = step([corner], (3,), output_weight, partly, BF16, False)
            if lent:
                carry = ([attended, beside, across, corner], old, shared)
        else:
            gathered = lax.all_gather(attended, "tp", axis=1, tiled=True)
            (stream,) = step([gathered], (None,), in_hbm(output_weight), stream, BF16, True)
    return stream


def solution(mesh):
    return jax.shard_map(
        body,
        mesh=mesh,
        in_specs=(
            P(("grp", "sp"), "tp"),
            P(),
            P(None, "tp", None),
            P(None, "tp", None),
            P(None, "tp", None),
            P(None, None, "tp"),
            P(None, "tp", None, None),
        ),
        out_specs=P(("grp", "sp"), "tp"),
        check_vma=False,
    )
```
